32 devices in a mesh: sp: 16 (over z, y, core), tp: 2 (over x).
Axes of the slice: x: 2, y: 2, z: 4, core: 2. Of those that a mesh axis runs over, the one named last changes fastest.
Arguments:
- residual: bfloat16 [2048, 2048], P(('sp', 'tp')), may hold values from -6 to 6
- forget_forward: bfloat16 [2048, 1024], P('sp', 'tp'), may hold values from -5.5 to 5.5
- forget_backward: bfloat16 [2048, 1024], P('sp', 'tp'), may hold values from -5.5 to 5.5
- value_written: bfloat16 [2048, 1024], P('sp', 'tp'), may hold values from -6 to 6
- query_logits: bfloat16 [2048, 1024], P('sp', 'tp'), may hold values from -6 to 6
- output_gate_logits: bfloat16 [2048, 1024], P('sp', 'tp'), may hold values from -6 to 6
- forget_minimum: float32 [2, 1024], P(None, 'tp'), may hold values from 0.88 to 1
- extra_log_rate: float32 [2, 2048, 8], P(None, 'sp', 'tp'), may hold values from -0.7 to 0
- head_norm_scale: float32 [128], replicated, may hold values from 0.1 to 1.9
- output_matrix: bfloat16 [1024, 2048], P(None, 'sp'), may hold values from -0.1875 to 0.1875
- prenorm_scale: float32 [2048], replicated, may hold values from 0.1 to 1.9
- gate_up_matrix: bfloat16 [2048, 5632], P('sp', 'tp'), may hold values from -0.125 to 0.125
- value_up_matrix: bfloat16 [2048, 5632], P('sp', 'tp'), may hold values from -0.125 to 0.125
- gate_taps: float32 [3, 5632], P(None, 'tp'), may hold values from -3.5 to 3.5
- value_taps: float32 [3, 5632], P(None, 'tp'), may hold values from -3.5 to 3.5
- down_matrix: bfloat16 [5632, 2048], P('tp', 'sp'), may hold values from -0.078125 to 0.078125
Outputs:
- layer_out: bfloat16 [2048, 2048], P(('sp', 'tp'))
The draws below stay inside these ranges and needn't reach their ends.
All inputs are finite; a program needn't handle non-finite values.
Results may differ from the reference program's by a relative error of at most 0.012.
Values may be sent and summed in bfloat16 or wider, within the bound.
A program may use at most 128 MiB of HBM per device.

```python
import jax
import jax.numpy as jnp
from jax import lax

D = 2048
HEADS = 8
HEAD_WIDTH = 128
HW = 1024
FF = 5632
BLOCK = 64
TOK_DEV = 128
TOKENS = 2048
N_TP = 2


def forget_draw(key):
    noise = jnp.clip(jax.random.normal(jax.random.fold_in(key, 1), (TOKENS, HEADS * HEAD_WIDTH), jnp.float32), -4.0, 4.0)
    shifts = jax.random.uniform(jax.random.fold_in(key, 2), (TOKENS // TOK_DEV, 1, 1), jnp.float32, -1.5, 1.5)
    noise = (noise.reshape(TOKENS // TOK_DEV, TOK_DEV, HEADS * HEAD_WIDTH) + shifts).reshape(TOKENS, HEADS * HEAD_WIDTH)
    return noise.astype(jnp.bfloat16)


def draw_forget_forward(key, part):
    return forget_draw(jax.random.fold_in(key, 11))


def draw_forget_backward(key, part):
    return forget_draw(jax.random.fold_in(key, 12))


def draw_forget_minimum(key, part):
    fast_count = 4
    picks = jax.random.randint(jax.random.fold_in(key, 21), (2, HEADS, 1), 0, 8)
    fast_bound = jax.random.uniform(jax.random.fold_in(key, 22), (2, HEADS, HEAD_WIDTH), jnp.float32, 0.88, 0.92)
    slow_bound = 1.0 - jax.random.uniform(jax.random.fold_in(key, 23), (2, HEADS, HEAD_WIDTH), jnp.float32, 0.5, 1.5) / TOKENS
    forget_floor = jnp.where(picks < fast_count, fast_bound, slow_bound)
    return forget_floor.reshape(2, HEADS * HEAD_WIDTH).astype(jnp.float32)


def draw_extra_log_rate(key, part):
    spots = jax.random.randint(jax.random.fold_in(key, 31), (2, 1, 3), 0, TOKENS)
    places = jnp.arange(TOKENS, dtype=jnp.int32)[None, :, None]
    struck = jnp.any(places == spots, axis=-1)[:, :, None]
    depth = jnp.log(jax.random.uniform(jax.random.fold_in(key, 32), (2, TOKENS, HEADS), jnp.float32, 0.5, 0.8))
    return jnp.where(struck, depth, 0.0).astype(jnp.float32)


def block_levels(own_key, shape, cuts, least, top_value):
    gain = 1.0
    for dim, parts in cuts:
        heights = jax.random.uniform(jax.random.fold_in(jax.random.fold_in(own_key, 6), dim), (parts,), jnp.float32, least / len(cuts), top_value / len(cuts))
        gain = gain * jnp.repeat(jnp.exp(heights), shape[dim] // parts).reshape((-1,) + (1,) * (len(shape) - 1 - dim))
    return gain


def normal_values(rng, extent, scale, bound, cuts=(), kind=jnp.bfloat16):
    result = scale * jax.random.normal(rng, extent, jnp.float32)
    if cuts:
        result = result * block_levels(rng, extent, cuts, -0.22, 0.18)
    return jnp.clip(result, -bound, bound).astype(kind)


def setup_inputs(seed: int = 0) -> dict:
    seeds = jax.random.split(jax.random.key(seed), 17)
    residual = normal_values(seeds[0], (TOKENS, D), 1.0, 6.0, ((0, 32),))
    forget_forward = draw_forget_forward(jax.random.fold_in(seeds[16], 71), 0)
    forget_backward = draw_forget_backward(jax.random.fold_in(seeds[16], 71), 0)
    value_written = normal_values(seeds[3], (TOKENS, HW), 1.0, 6.0, ((0, 16), (1, 2)))
    query_logits = normal_values(seeds[4], (TOKENS, HW), 1.0, 6.0, ((0, 16), (1, 2)))
    output_gate_logits = normal_values(seeds[5], (TOKENS, HW), 1.0, 6.0, ((0, 16), (1, 2)))
    forget_minimum = draw_forget_minimum(jax.random.fold_in(seeds[16], 71), 0)
    extra_log_rate = draw_extra_log_rate(jax.random.fold_in(seeds[16], 71), 0)
    head_norm_scale = jnp.clip(1.0 + 0.18 * jax.random.normal(seeds[8], (HEAD_WIDTH,), jnp.float32), 0.1, 1.9)
    output_matrix = normal_values(seeds[9], (HW, D), HW ** -0.5, 0.1875, ((1, 16),))
    prenorm_scale = jnp.clip(1.0 + 0.18 * jax.random.normal(seeds[10], (D,), jnp.float32), 0.1, 1.9)
    gate_up_matrix = normal_values(seeds[11], (D, FF), D ** -0.5, 0.125, ((0, 16), (1, 2)))
    value_up_matrix = normal_values(seeds[12], (D, FF), D ** -0.5, 0.125, ((0, 16), (1, 2)))
    gate_taps = normal_values(seeds[13], (3, FF), 3 ** -0.5, 3.5, ((1, 2),), jnp.float32)
    value_taps = normal_values(seeds[14], (3, FF), 3 ** -0.5, 3.5, ((1, 2),), jnp.float32)
    down_matrix = normal_values(seeds[15], (FF, D), FF ** -0.5, 0.078125, ((0, 2), (1, 16)))
    return dict(residual=residual, forget_forward=forget_forward, forget_backward=forget_backward, value_written=value_written, query_logits=query_logits, output_gate_logits=output_gate_logits, forget_minimum=forget_minimum, extra_log_rate=extra_log_rate, head_norm_scale=head_norm_scale, output_matrix=output_matrix, prenorm_scale=prenorm_scale, gate_up_matrix=gate_up_matrix, value_up_matrix=value_up_matrix, gate_taps=gate_taps, value_taps=value_taps, down_matrix=down_matrix)


EPSILON = 1e-06

def rms_scale(array):
    return array * lax.rsqrt(lax.optimization_barrier(jnp.mean(array * array, axis=-1, keepdims=True)) + EPSILON)

def forget_factors(forget_logits, forget_floor, extra_decay):
    unbounded_gate = forget_logits.astype(jnp.float32)
    log_forget_gate = jnp.log(forget_floor + (1.0 - forget_floor) * jax.nn.sigmoid(unbounded_gate)) + jnp.repeat(extra_decay, HEAD_WIDTH, axis=1)
    key_in = (1.0 - forget_floor) * jax.nn.sigmoid(-unbounded_gate)
    shape = (unbounded_gate.shape[0], unbounded_gate.shape[1] // HEAD_WIDTH, HEAD_WIDTH)
    return (log_forget_gate.reshape(shape), key_in.reshape(shape))

def block_scan(log_forget_gate, key_in, values, queries):
    length, heads, depth = log_forget_gate.shape
    width = values.shape[2]
    blocks = length // BLOCK
    highest = lax.Precision.HIGHEST
    lower = jnp.tril(jnp.ones((BLOCK, BLOCK), dtype=bool))[:, :, None, None]

    def split(array):
        return array.reshape(blocks, BLOCK, heads, array.shape[2])

    def advance(carry, pieces):
        state, carried = carry
        log_part, key_part, value_part, query_part = pieces
        running = jnp.cumsum(log_part, axis=0)
        block_total = running[-1]
        query_carry = query_part * jnp.exp(carried[None] + running)
        from_state = jnp.einsum('chd,hde->che', query_part * jnp.exp(running), state, precision=highest)
        gaps = jnp.where(lower, running[:, None] - running[None, :], -1e+30)
        scores = jnp.einsum('ihd,jhd,ijhd->hij', query_part, key_part, jnp.exp(gaps), precision=highest)
        inside = jnp.einsum('hij,jhe->ihe', scores, value_part, precision=highest)
        fresh = jnp.einsum('chd,che->hde', key_part * jnp.exp(block_total[None] - running), value_part, precision=highest)
        state = jnp.exp(block_total)[:, :, None] * state + fresh
        return ((state, carried + block_total), (from_state + inside, query_carry))
    start = (jnp.zeros((heads, depth, width), jnp.float32), jnp.zeros((heads, depth), jnp.float32))
    (state, carried), (outputs, query_carry) = lax.scan(advance, start, (split(log_forget_gate), split(key_in), split(values), split(queries)))
    return (state, carried, outputs.reshape(length, heads, width), query_carry.reshape(length, heads, depth))

def reference(residual, forget_forward, forget_backward, value_written, query_logits, output_gate_logits, forget_minimum, extra_log_rate, head_norm_scale, output_matrix, prenorm_scale, gate_up_matrix, value_up_matrix, gate_taps, value_taps, down_matrix):
    length = value_written.shape[0]
    shape = (length, value_written.shape[1] // HEAD_WIDTH, HEAD_WIDTH)
    values = value_written.astype(jnp.float32).reshape(shape)
    queries = jax.nn.silu(query_logits.astype(jnp.float32)).reshape(shape)
    log_decay_forward, key_forward = forget_factors(forget_forward, forget_minimum[0], extra_log_rate[0])
    forward = block_scan(log_decay_forward, key_forward, values, queries)[2]
    log_decay_backward, key_backward = forget_factors(forget_backward, forget_minimum[1], extra_log_rate[1])
    backward = block_scan(log_decay_backward[::-1], key_backward[::-1], values[::-1], queries[::-1])[2][::-1]
    gated = rms_scale(forward + backward) * head_norm_scale * jax.nn.silu(output_gate_logits.astype(jnp.float32)).reshape(shape)
    mixed_in = gated.reshape(length, shape[1] * HEAD_WIDTH).astype(jnp.bfloat16)
    after_mix = residual.astype(jnp.float32) + jnp.dot(mixed_in, output_matrix, preferred_element_type=jnp.float32)
    normed = (rms_scale(after_mix) * prenorm_scale).astype(jnp.bfloat16)
    gate_up = jnp.dot(normed, gate_up_matrix, preferred_element_type=jnp.float32).astype(jnp.bfloat16)
    value_up = jnp.dot(normed, value_up_matrix, preferred_element_type=jnp.float32).astype(jnp.bfloat16)

    def convolve(upward, kernel):
        padded = jnp.pad(upward, ((1, 1), (0, 0)))
        return padded[:length] * kernel[0] + padded[1:length + 1] * kernel[1] + padded[2:] * kernel[2]
    hidden = (jax.nn.silu(convolve(gate_up, gate_taps)) * convolve(value_up, value_taps)).astype(jnp.bfloat16)
    group_width = hidden.shape[1] // N_TP

    def add_group(index, total):
        first = (index * group_width).astype(jnp.int32)
        hidden_part = lax.dynamic_slice_in_dim(hidden, first, group_width, 1)
        weight_part = lax.dynamic_slice_in_dim(down_matrix, first, group_width, 0)
        partial_sum = jnp.dot(hidden_part, weight_part, preferred_element_type=jnp.float32)
        return total + lax.optimization_barrier(partial_sum.astype(jnp.bfloat16)).astype(jnp.float32)
    down = lax.fori_loop(jnp.int32(0), jnp.int32(N_TP), add_group, jnp.zeros((length, down_matrix.shape[1]), jnp.float32))
    return (after_mix + down).astype(jnp.bfloat16)
```

```python
import functools
import math

import jax
import jax.numpy as jnp
from jax import lax
from jax.experimental import pallas as pl
from jax.experimental.pallas import tpu as pltpu
from jax.sharding import PartitionSpec as P

HEAD_WIDTH = 128
EPSILON = 1e-06
MESH = pl.DeviceIdType.MESH
F32 = jnp.float32
BF16 = jnp.bfloat16
DECAY_ROWS = 16
CHUNKS = 4


class Grid:
    def __init__(self, mesh):
        sp, tp = mesh.shape["sp"], mesh.shape["tp"]
        self.sp, self.x = sp, tp
        self.c = math.gcd(sp, 2)
        self.y = math.gcd(sp // self.c, 2)
        self.z = sp // (self.c * self.y)
        self.ids = iter(range(100))

    def size(self, dim):
        return getattr(self, dim)

    def place(self):
        s, t = lax.axis_index("sp"), lax.axis_index("tp")
        return {
            "sp": s,
            "x": t,
            "c": lax.rem(s, self.c),
            "y": lax.rem(s // self.c, self.y),
            "z": s // (self.c * self.y),
        }

    def peer(self, place, dim, index):
        if dim == "sp":
            return {"sp": index, "tp": place["x"]}
        at = dict(place)
        at[dim] = index
        return {"sp": (at["z"] * self.y + at["y"]) * self.c + at["c"], "tp": at["x"]}

    def greet(self, place, dims):
        barrier = pltpu.get_barrier_semaphore()
        count = 0
        for dim in dims:
            n = self.size(dim)
            for k in range(1, n):
                peer = self.peer(place, dim, lax.rem(place[dim] + k, n))
                pl.semaphore_signal(barrier, inc=1, device_id=peer, device_id_type=MESH)
                count += 1
        pl.semaphore_wait(barrier, count)


def exchange_kernel(grid, dims, keep, *refs):
    m = len(dims)
    ins, outs = refs[:m], refs[m : 2 * m]
    send_sem, recv_sem, own_sem = refs[2 * m :]
    place = grid.place()
    copies = []
    grid.greet(place, sorted(set(dims)))
    base = 0
    for i, dim in enumerate(dims):
        n, me = grid.size(dim), place[dim]
        for k in range(1, n):
            to = lax.rem(me + k, n)
            slot = me if keep else k - 1
            copy = pltpu.make_async_remote_copy(
                src_ref=ins[i].at[to],
                dst_ref=outs[i].at[slot],
                send_sem=send_sem.at[base + k - 1],
                recv_sem=recv_sem.at[base + k - 1],
                device_id=grid.peer(place, dim, to),
                device_id_type=MESH,
            )
            copy.start()
            copies.append(copy)
        base += n - 1
    if keep:
        for i, dim in enumerate(dims):
            me = place[dim]
            own = pltpu.make_async_copy(ins[i].at[me], outs[i].at[me], own_sem.at[i])
            own.start()
            copies.append(own)
    for copy in copies:
        copy.wait()


def exchange(grid, items, keep):
    dims = tuple(d for _, d in items)
    total = sum(grid.size(d) - 1 for d in dims)
    shapes = tuple(
        jax.ShapeDtypeStruct(a.shape if keep else (a.shape[0] - 1,) + a.shape[1:], a.dtype)
        for a, _ in items
    )
    return pl.pallas_call(
        functools.partial(exchange_kernel, grid, dims, keep),
        out_shape=shapes,
        in_specs=[pl.BlockSpec(memory_space=pl.ANY)] * len(items),
        out_specs=[pl.BlockSpec(memory_space=pl.ANY)] * len(items),
        scratch_shapes=[
            pltpu.SemaphoreType.DMA((total,)),
            pltpu.SemaphoreType.DMA((total,)),
            pltpu.SemaphoreType.DMA((len(items),)),
        ],
        compiler_params=pltpu.CompilerParams(
            collective_id=next(grid.ids), has_side_effects=True
        ),
    )(*[a for a, _ in items])


def gather_kernel(grid, x_ref, out_ref, send_sem, recv_sem, own_sem):
    place = grid.place()
    z, y, c, x = (place[d] for d in "zycx")
    part = x_ref.shape[1] // (2 * CHUNKS)
    grid.greet(place, ("z", "y", "c", "x"))
    own = pltpu.make_async_copy(x_ref, out_ref.at[z, y, c, x], own_sem)
    own.start()
    used = 0

    def push(dim, src, dst):
        nonlocal used
        n, copies = grid.size(dim), []
        for k in range(1, n):
            copy = pltpu.make_async_remote_copy(
                src_ref=src,
                dst_ref=dst,
                send_sem=send_sem.at[used],
                recv_sem=recv_sem.at[used],
                device_id=grid.peer(place, dim, lax.rem(place[dim] + k, n)),
                device_id_type=MESH,
            )
            copy.start()
            copies.append(copy)
            used += 1
        return copies

    def start(level, t):
        both = pl.ds(2 * t * part, 2 * part)
        first, second = pl.ds(2 * t * part, part), pl.ds((2 * t + 1) * part, part)
        if level == 0:
            return push("z", x_ref.at[:, both], out_ref.at[z, y, c, x, :, both])
        if level == 1:
            a = out_ref.at[:, y, c, x, :, first]
            b = out_ref.at[:, y, c, x, :, second]
            return push("y", a, a) + push("x", b, b)
        if level == 2:
            a = out_ref.at[:, :, c, x, :, first]
            b = out_ref.at[:, y, c, :, :, second]
            return push("x", a, a) + push("y", b, b)
        a = out_ref.at[:, :, c, :, :, both]
        return push("c", a, a)

    flying = {(0, t): start(0, t) for t in range(CHUNKS)}
    own.wait()
    for step in range(CHUNKS + 3):
        for level in range(4):
            t = step - level
            if 0 <= t < CHUNKS:
                for copy in flying[level, t]:
                    copy.wait()
                if level < 3:
                    flying[level + 1, t] = start(level + 1, t)


def gather(grid, array):
    total = CHUNKS * sum(grid.size(d) - 1 for d in "zyyxxc")
    return pl.pallas_call(
        functools.partial(gather_kernel, grid),
        out_shape=jax.ShapeDtypeStruct(
            (grid.z, grid.y, grid.c, grid.x) + array.shape, array.dtype
        ),
        in_specs=[pl.BlockSpec(memory_space=pltpu.VMEM)],
        out_specs=pl.BlockSpec(memory_space=pl.ANY),
        scratch_shapes=[
            pltpu.SemaphoreType.DMA((total,)),
            pltpu.SemaphoreType.DMA((total,)),
            pltpu.SemaphoreType.DMA,
        ],
        compiler_params=pltpu.CompilerParams(
            collective_id=next(grid.ids), has_side_effects=True
        ),
    )(array)


ORDERS = ("cxyz", "cyxz")


def reduce_kernel(grid, a_ref, b_ref, out_ref, *scratch):
    held, got, (send_sem, recv_sem, own_sem) = scratch[:2], scratch[2:10], scratch[10:]
    terms = (a_ref, b_ref)
    place = grid.place()
    rows, part = held[0].shape[-2:]
    grid.greet(place, ("z", "y", "c", "x"))
    used = 0

    def start(level, t):
        nonlocal used
        copies = []
        for color in range(2):
            dim = ORDERS[color][level]
            n, me = grid.size(dim), place[dim]
            for k in range(1, n):
                to = lax.rem(me + k, n)
                if level == 0:
                    src = terms[color].at[to, :, :, :, :, pl.ds(t * part, part)]
                else:
                    before = tuple(place[d] for d in ORDERS[color][1:level])
                    src = held[color].at[(t,) + before + (to,)]
                copy = pltpu.make_async_remote_copy(
                    src_ref=src,
                    dst_ref=got[2 * level + color].at[t, k - 1],
                    send_sem=send_sem.at[used],
                    recv_sem=recv_sem.at[used],
                    device_id=grid.peer(place, dim, to),
                    device_id_type=MESH,
                )
                copy.start()
                copies.append(copy)
                used += 1
        return copies

    def add(level, t):
        for color in range(2):
            order = ORDERS[color]
            here = tuple(place[d] for d in order[1 : level + 1])
            left = [grid.size(d) for d in order[level + 1 :]]
            peers = grid.size(order[level]) - 1
            where = got[2 * level + color]

            def block(i, _, color=color, here=here, left=left, peers=peers, where=where):
                index, rest = [], i
                for n in reversed(left):
                    index.insert(0, lax.rem(rest, n))
                    rest = rest // n
                index = tuple(index)
                total = held[color][(t,) + here + index].astype(F32)
                for k in range(peers):
                    total += where[(t, k) + index].astype(F32)
                if level < 3:
                    held[color][(t,) + here + index] = total.astype(BF16)
                else:
                    first = (color * CHUNKS + t) * part
                    out_ref[:, first : first + part] = total
                return 0

            if left:
                lax.fori_loop(0, math.prod(left), block, 0)
            else:
                block(0, 0)

    flying = {(0, t): start(0, t) for t in range(CHUNKS)}
    for t in range(CHUNKS):
        for color in range(2):
            own = pltpu.make_async_copy(
                terms[color].at[place["c"], :, :, :, :, pl.ds(t * part, part)],
                held[color].at[t],
                own_sem.at[t, color],
            )
            own.start()
            flying[0, t].append(own)
    for step in range(CHUNKS + 3):
        for level in range(4):
            t = step - level
            if 0 <= t < CHUNKS:
                for copy in flying[level, t]:
                    copy.wait()
                add(level, t)
                if level < 3:
                    flying[level + 1, t] = start(level + 1, t)


def reduce_scatter(grid, first, second):
    rows, cols = first.shape[-2:]
    tile = (rows, cols // CHUNKS)

    def sizes(order):
        return tuple(grid.size(d) for d in order)

    scratch = [pltpu.VMEM((CHUNKS,) + sizes(o[1:]) + tile, BF16) for o in ORDERS]
    for level in range(4):
        for o in ORDERS:
            peers = grid.size(o[level]) - 1
            scratch.append(
                pltpu.VMEM((CHUNKS, max(peers, 1)) + sizes(o[level + 1 :]) + tile, BF16)
            )
    total = 2 * CHUNKS * sum(grid.size(d) - 1 for d in "cxyz")
    return pl.pallas_call(
        functools.partial(reduce_kernel, grid),
        out_shape=jax.ShapeDtypeStruct((rows, 2 * cols), F32),
        in_specs=[pl.BlockSpec(memory_space=pl.ANY)] * 2,
        out_specs=pl.BlockSpec(memory_space=pltpu.VMEM),
        scratch_shapes=scratch
        + [
            pltpu.SemaphoreType.DMA((total,)),
            pltpu.SemaphoreType.DMA((total,)),
            pltpu.SemaphoreType.DMA((CHUNKS, 2)),
        ],
        compiler_params=pltpu.CompilerParams(
            collective_id=next(grid.ids), has_side_effects=True, vmem_limit_bytes=64000000
        ),
    )(first, second)


def dot(a, b, dims, precision=None):
    return lax.dot_general(
        a, b, (dims, ((), ())), precision=precision, preferred_element_type=F32
    )


def local_kernel(
    heads, zf_ref, zb_ref, v_ref, q_ref, floor_ref, extra_ref, out_ref, carry_ref, state_ref, decay_ref
):
    length = v_ref.shape[0]
    rows = lax.broadcasted_iota(jnp.int32, (length, length), 0)
    cols = lax.broadcasted_iota(jnp.int32, (length, length), 1)
    middle = length // 2
    for h in range(heads):
        at = slice(h * HEAD_WIDTH, (h + 1) * HEAD_WIDTH)
        values = v_ref[:, at]
        logits = q_ref[:, at].astype(F32)
        queries = logits * jax.nn.sigmoid(logits)
        scores = jnp.zeros((length, length), F32)
        for d, z_ref in enumerate((zf_ref, zb_ref)):
            mask = rows >= cols if d == 0 else rows <= cols
            z = z_ref[:, at].astype(F32)
            floor = floor_ref[d : d + 1, at]
            rest = 1.0 - floor
            logf = jnp.log(floor + rest * jax.nn.sigmoid(z)) + extra_ref[d, :, h : h + 1]
            key = rest * jax.nn.sigmoid(-z)
            running = dot(
                jnp.where(mask, 1.0, 0.0), logf, ((1,), (0,)), lax.Precision.HIGHEST
            )
            last = length - 1 if d == 0 else 0
            total = running[last : last + 1]
            centred = running - running[middle : middle + 1]
            part = dot(
                (queries * jnp.exp(centred)).astype(BF16),
                (key * jnp.exp(-centred)).astype(BF16),
                ((1,), (1,)),
            )
            scores += jnp.where(mask, part, 0.0)
            carry_ref[d, :, at] = (queries * jnp.exp(running)).astype(BF16)
            fresh = (key * jnp.exp(total - running)).astype(BF16)
            state_ref[d, h] = dot(values, fresh, ((0,), (0,))).astype(BF16)
            decay_ref[d, h] = jnp.broadcast_to(
                jnp.exp(total), (DECAY_ROWS, HEAD_WIDTH)
            ).astype(BF16)
        out_ref[:, at] = dot(scores.astype(BF16), values, ((1,), (0,)))


def prefix_kernel(rows, got_ref, out_ref):
    n = got_ref.shape[0]
    forward = lax.axis_index("sp") < n // 2

    def hop(k, carry):
        at = jnp.where(forward, k, n - 1 - k)
        out_ref[at] = carry.astype(BF16)
        block = got_ref[at].astype(F32)
        return block[rows : rows + 1] * carry + block[:rows]

    lax.fori_loop(0, n, hop, jnp.zeros((rows, HEAD_WIDTH), F32))


def finish_kernel(heads, out_ref, carry_ref, enter_ref, gate_ref, scale_ref, gated_ref):
    for h in range(heads):
        at = slice(h * HEAD_WIDTH, (h + 1) * HEAD_WIDTH)
        total = out_ref[:, at]
        for d in range(2):
            total += dot(carry_ref[d, :, at], enter_ref[d, h], ((1,), (1,)))
        mean = jnp.mean(total * total, axis=-1, keepdims=True)
        g = gate_ref[:, at].astype(F32)
        gated_ref[:, at] = (
            total * lax.rsqrt(mean + EPSILON) * scale_ref[...] * (g * jax.nn.sigmoid(g))
        ).astype(BF16)


LANES = 128
PAD_ROWS = 16
SLICES = 4


class Fused:
    def __init__(self, grid, heads, length, depth, units, width):
        self.grid = grid
        self.heads, self.length, self.depth = heads, length, depth
        self.quads = grid.z * grid.y
        self.blocks = units // LANES
        self.base = self.blocks // self.quads
        self.most = -(-self.blocks // self.quads)
        self.unit = self.most * LANES
        self.width = width
        self.rows = length // grid.x
        self.shards = self.quads * grid.x
        self.own = self.shards * self.rows
        self.step = depth // (2 * SLICES)
        self.quarter = width * grid.x // 4

    @staticmethod
    def fits(grid, heads, length, depth, units, width, out_depth):
        return (
            (grid.z, grid.y, grid.c, grid.x) == (4, 2, 2, 2)
            and heads == grid.c * grid.y
            and units % LANES == 0
            and units // LANES >= grid.z * grid.y
            and length % (16 * grid.x) == 0
            and depth == out_depth == grid.sp * LANES
            and depth % (2 * SLICES * LANES) == 0
        )

    def scratch(self):
        g, h2, w = self.grid, HEAD_WIDTH + PAD_ROWS, HEAD_WIDTH
        dma = pltpu.SemaphoreType.DMA
        n = 2 * SLICES
        tall = self.quads * g.x * self.rows
        return dict(
            wup=pltpu.VMEM((self.depth, 2 * self.unit), BF16),
            wdn=pltpu.VMEM((self.unit, self.depth), BF16),
            outm=pltpu.VMEM((g.z, g.y, self.width * g.x, g.c * LANES), BF16),
            local=pltpu.VMEM((self.length, self.width), F32),
            carry=pltpu.VMEM((2, self.length, self.width), BF16),
            stb=pltpu.VMEM((2, 2, 2, h2, w), BF16),
            rc=pltpu.VMEM((2, 2, h2, w), BF16),
            ct=pltpu.VMEM((2, 2, h2, w), BF16),
            ry=pltpu.VMEM((2, h2, w), BF16),
            pt=pltpu.VMEM((2, h2, w), BF16),
            rz=pltpu.VMEM((g.z, h2, w), BF16),
            ce=pltpu.VMEM((2, 2, w, w), BF16),
            yb=pltpu.VMEM((2, w, w), BF16),
            ent=pltpu.VMEM((2, 2, 2, w, w), BF16),
            cb=pltpu.VMEM((2, 2, w, w), BF16),
            gb=pltpu.VMEM((self.rows, self.width), BF16),
            sw=pltpu.VMEM((g.x, self.rows, self.width), BF16),
            after=pltpu.VMEM((self.rows, self.depth), F32),
            tok=pltpu.VMEM((g.z, g.y, g.x, self.rows, self.depth), BF16),
            acc=pltpu.VMEM((tall, 2 * self.unit), F32),
            ed=pltpu.VMEM((2 * self.most, 2 * self.quads, LANES), F32),
            er=pltpu.VMEM((2 * self.most, 2 * self.quads + 16, LANES), F32),
            hid=pltpu.VMEM((tall, self.unit), BF16),
            part=pltpu.VMEM((g.z, g.y, g.x, self.rows, self.depth), BF16),
            r1=pltpu.VMEM((n, g.z, 2, self.rows, self.step), BF16),
            r2=pltpu.VMEM((n, g.z, self.rows, self.step), BF16),
            r3=pltpu.VMEM((n, g.z - 1, self.rows, self.step), BF16),
            loc_s=dma((2,)),
            oz_s=dma((3, 4)), oz_r=dma((3, 4)),
            oy_s=dma((3,)), oy_r=dma((3,)),
            ox_s=dma((1,)), ox_r=dma((1,)),
            oc_s=dma((4,)), oc_r=dma((4,)),
            w_s=dma((self.quads, 6)), w_r=dma((self.quads, 6)),
            f_s=dma((self.quads, 2)), f_r=dma((self.quads, 2)),
            st_s=dma((5,)), st_r=dma((5,)),
            sz_s=dma((3,)), sz_r=dma((3,)),
            az_s=dma((n, 4)), az_r=dma((n, 4)),
            a2_s=dma((n,)), a2_r=dma((n,)),
            a3_s=dma((n,)), a3_r=dma((n,)),
            ed_s=dma((1,)), ed_r=dma((1,)),
            r1_s=dma((n,)), r1_r=dma((n,)),
            r2_s=dma((n,)), r2_r=dma((n,)),
            r3_s=dma((n, 3)), r3_r=dma((n, 3)),
        )


INPUTS = (
    "zf",
    "zb",
    "val",
    "qry",
    "og",
    "floor",
    "extra",
    "hscale",
    "res",
    "pscale",
    "gtaps",
    "vtaps",
    "out_w",
    "gate_w",
    "value_w",
    "down_w",
)


def fused_kernel(f, names, *refs):
    R = dict(zip(INPUTS + ("out",) + tuple(names), refs))
    R = type("Refs", (), R)
    g = f.grid
    s, x = lax.axis_index("sp"), lax.axis_index("tp")
    c, y, z = lax.rem(s, 2), lax.rem(s // 2, 2), s // 4
    q = s // 2
    W, U, Q = HEAD_WIDTH, f.unit, f.quads
    H, D = f.rows, f.depth
    drains = []

    def to(z=z, y=y, c=c, x=x):
        return {"sp": (z * 2 + y) * 2 + c, "tp": x}

    def remote(src, dst, ss, rs, dev):
        return pltpu.make_async_remote_copy(
            src_ref=src, dst_ref=dst, send_sem=ss, recv_sem=rs, device_id=dev, device_id_type=MESH
        )

    def go(cp, cond=None):
        if cond is None:
            cp.start()
        else:
            pl.when(cond)(cp.start)
        drains.append((cond, cp))
        return cp

    def lane(i):
        return pl.ds(pl.multiple_of(i * LANES, LANES), LANES)

    def first_block(j):
        return (f.blocks * j) // Q

    def extra_block(j):
        return first_block(j + 1) - first_block(j) > f.base

    mine = first_block(q)
    has_extra = extra_block(q)
    main, rest = f.base * LANES, (f.most - f.base) * LANES

    def weight_copies(src_s, j, kinds):
        start = first_block(j)
        at = pl.ds(pl.multiple_of(start * LANES, LANES), main)
        at2 = pl.ds(pl.multiple_of((start + f.base) * LANES, LANES), LANES)
        k = pl.ds(pl.multiple_of(src_s * LANES, LANES), LANES)
        out = []
        if "up" in kinds:
            out.append((0, None, R.gate_w.at[:, at], R.wup.at[k, pl.ds(0, main)]))
            out.append((1, None, R.value_w.at[:, at], R.wup.at[k, pl.ds(U, main)]))
            if rest:
                e = extra_block(j)
                out.append((2, e, R.gate_w.at[:, at2], R.wup.at[k, pl.ds(main, LANES)]))
                out.append((3, e, R.value_w.at[:, at2], R.wup.at[k, pl.ds(U + main, LANES)]))
        if "down" in kinds:
            out.append((4, None, R.down_w.at[at, :], R.wdn.at[pl.ds(0, main), k]))
            if rest:
                out.append((5, extra_block(j), R.down_w.at[at2, :], R.wdn.at[pl.ds(main, LANES), k]))
        return out

    def own_weights(kinds):
        for i, cond, src, dst in weight_copies(s, q, kinds):
            cp = pltpu.make_async_copy(src, dst, R.w_r.at[q, i])
            if cond is None:
                cp.start()
            else:
                pl.when(cond)(cp.start)

    def send_weights(k, kinds):
        j = lax.rem(q + k, Q)
        for i, cond, src, dst in weight_copies(s, j, kinds):
            go(remote(src, dst, R.w_s.at[k, i], R.w_r.at[q, i], {"sp": j * 2 + c, "tp": x}), cond)

    def pass_weights(p, kinds):
        ps = p * 2 + c
        for i, cond, _, dst in weight_copies(ps, q, kinds):
            cp = remote(dst, dst, R.w_s.at[0, i], R.w_r.at[p, i], to(c=1 - c))
            if cond is None:
                cp.wait_recv()
            else:
                pl.when(cond)(cp.wait_recv)
        k = pl.ds(pl.multiple_of(ps * LANES, LANES), LANES)
        if "up" in kinds:
            go(remote(R.wup.at[k, :], R.wup.at[k, :], R.f_s.at[p, 0], R.f_r.at[p, 0], to(c=1 - c)))
        if "down" in kinds:
            go(remote(R.wdn.at[:, k], R.wdn.at[:, k], R.f_s.at[p, 1], R.f_r.at[p, 1], to(c=1 - c)))

    def wait_weights(p, kind):
        k = pl.ds(pl.multiple_of((p * 2 + 1 - c) * LANES, LANES), LANES)
        ref = R.wup.at[k, :] if kind == 0 else R.wdn.at[:, k]
        remote(ref, ref, R.f_s.at[p, kind], R.f_r.at[p, kind], to(c=1 - c)).wait_recv()

    mid = (z == 1) | (z == 2)
    t0, t1 = jnp.where(z == 1, 0, 1), jnp.where(z == 2, 3, 2)
    far = jnp.where(z == 1, 0, 3)

    class ZGather:
        def __init__(self, src, dst, ss, rs):
            self.src, self.dst, self.ss, self.rs = src, dst, ss, rs

        def start(self):
            for j, t in enumerate((t0, t1)):
                go(remote(self.src, self.dst(z), self.ss(j), self.rs(z), to(z=t)))

        def arrive(self, shard):
            d = self.dst(shard)
            remote(d, d, self.ss(0), self.rs(shard), to(z=t0)).wait_recv()

        def forward(self):
            for k in range(2):
                shard = jnp.where(z == 1, 2 + k, k)
                d = self.dst(shard)
                cp = remote(d, d, self.ss(2 + k), self.rs(shard), to(z=far))

                @pl.when(mid)
                def _(cp=cp):
                    cp.wait_recv()
                    cp.start()

                drains.append((mid, cp))

        def finish(self):
            @pl.when(mid)
            def _():
                self.arrive(far)

            @pl.when(jnp.logical_not(mid))
            def _():
                for k in range(3):
                    self.arrive(jnp.where(z == 0, 1 + k, k))

    if rest:
        @pl.when(jnp.logical_not(has_extra))
        def _():
            R.wup[:, main:U] = jnp.zeros((D, LANES), BF16)
            R.wup[:, U + main :] = jnp.zeros((D, LANES), BF16)
            R.wdn[main:U, :] = jnp.zeros((LANES, D), BF16)

    edge = jnp.zeros((2 * f.most, 8, LANES), F32)
    R.er[:, 0:8, :] = edge
    R.er[:, 8 + 2 * Q :, :] = edge

    barrier = pltpu.get_barrier_semaphore()
    for k in range(1, Q):
        dev = {"sp": lax.rem(q + k, Q) * 2 + c, "tp": x}
        pl.semaphore_signal(barrier, inc=1, device_id=dev, device_id_type=MESH)
    pl.semaphore_signal(barrier, inc=1, device_id=to(c=1 - c), device_id_type=MESH)
    pl.semaphore_signal(barrier, inc=1, device_id=to(x=1 - x), device_id_type=MESH)
    pl.semaphore_wait(barrier, Q + 1)

    ccol = lane(c)
    O = f.quarter
    starts = (2 * O + x * O, 0, O)
    own_out = []
    for i, (r, size) in enumerate(((starts[0], O), (0, 2 * O))):
        at = pl.ds(pl.multiple_of(r, O), size)
        cp = pltpu.make_async_copy(R.out_w.at[at, :], R.outm.at[z, y, at, ccol], R.loc_s.at[i])
        cp.start()
        own_out.append(cp)
    zg = []
    for i, r in enumerate(starts):
        at = pl.ds(pl.multiple_of(r, O), O)
        zg.append(
            ZGather(
                R.out_w.at[at, :],
                lambda k, at=at: R.outm.at[k, y, at, ccol],
                lambda j, i=i: R.oz_s.at[i, j],
                lambda j, i=i: R.oz_r.at[i, j],
            )
        )
        zg[-1].start()

    def out_y(i):
        at = pl.ds(pl.multiple_of(starts[i], O), O)
        src = R.outm.at[:, y, at, ccol]
        return remote(src, src, R.oy_s.at[i], R.oy_r.at[i], to(y=1 - y))

    def out_x():
        at = pl.ds(pl.multiple_of(starts[0], O), O)
        src = R.outm.at[:, :, at, ccol]
        return remote(src, src, R.ox_s.at[0], R.ox_r.at[0], to(x=1 - x))

    def out_c(i):
        src = R.outm.at[:, :, pl.ds(i * O, O), ccol]
        return remote(src, src, R.oc_s.at[i], R.oc_r.at[i], to(c=1 - c))

    own_weights(("up",))
    send_weights(1, ("up",))

    L = f.length
    rows_i = lax.broadcasted_iota(jnp.int32, (L, L), 0)
    cols_i = lax.broadcasted_iota(jnp.int32, (L, L), 1)
    middle = L // 2
    for h in range(f.heads):
        at = slice(h * W, (h + 1) * W)
        values = R.val[:, at]
        logits = R.qry[:, at].astype(F32)
        queries = logits * jax.nn.sigmoid(logits)
        scores = jnp.zeros((L, L), F32)
        for d, z_ref in enumerate((R.zf, R.zb)):
            mask = rows_i >= cols_i if d == 0 else rows_i <= cols_i
            pre = z_ref[:, at].astype(F32)
            floor = R.floor[d : d + 1, at]
            span = 1.0 - floor
            logf = jnp.log(floor + span * jax.nn.sigmoid(pre)) + R.extra[d, :, h : h + 1]
            key = span * jax.nn.sigmoid(-pre)
            running = dot(jnp.where(mask, 1.0, 0.0), logf, ((1,), (0,)), lax.Precision.HIGHEST)
            last = L - 1 if d == 0 else 0
            total = running[last : last + 1]
            centred = running - running[middle : middle + 1]
            inner = dot(
                (queries * jnp.exp(centred)).astype(BF16),
                (key * jnp.exp(-centred)).astype(BF16),
                ((1,), (1,)),
            )
            scores += jnp.where(mask, inner, 0.0)
            R.carry[d, :, at] = (queries * jnp.exp(running)).astype(BF16)
            fresh = (key * jnp.exp(total - running)).astype(BF16)
            R.stb[h // 2, h % 2, d, :W] = dot(values, fresh, ((0,), (0,))).astype(BF16)
            R.stb[h // 2, h % 2, d, W:] = jnp.broadcast_to(jnp.exp(total), (PAD_ROWS, W)).astype(BF16)
        R.local[:, at] = dot(scores.astype(BF16), values, ((1,), (0,)))

    def state(ref, *at):
        return ref[at + (slice(0, W),)].astype(F32)

    def decay(ref, *at):
        return ref[at + (slice(W, W + 1),)].astype(F32)

    def put(ref, at, value, factor):
        ref[at + (slice(0, W),)] = value.astype(BF16)
        ref[at + (slice(W, W + PAD_ROWS),)] = jnp.broadcast_to(factor, (PAD_ROWS, W)).astype(BF16)

    def hop(i, src, dst, dev):
        return go(remote(src, dst, R.st_s.at[i], R.st_r.at[i], dev))

    step = hop(0, R.stb.at[1 - c], R.rc, to(c=1 - c))
    for o in zg:
        o.forward()
    send_weights(2, ("up",))
    step.wait_recv()
    for hp in range(2):
        for d in range(2):
            ahead = c == d
            so, ao = state(R.stb, c, hp, d), decay(R.stb, c, hp, d)
            sp_, ap = state(R.rc, hp, d), decay(R.rc, hp, d)
            both = jnp.where(ahead, ap, ao) * jnp.where(ahead, so, sp_) + jnp.where(ahead, sp_, so)
            put(R.ct, (hp, d), both, ao * ap)
    step = hop(1, R.ct.at[1 - y], R.ry, to(y=1 - y))
    for cp in own_out:
        cp.wait()
    out_ys = []
    for i, o in enumerate(zg):
        o.finish()
        out_ys.append(go(out_y(i)))
    send_weights(7, ("up",))
    step.wait_recv()
    for d in range(2):
        ahead = y == d
        so, ao = state(R.ct, y, d), decay(R.ct, y, d)
        sp_, ap = state(R.ry, d), decay(R.ry, d)
        both = jnp.where(ahead, ap, ao) * jnp.where(ahead, so, sp_) + jnp.where(ahead, sp_, so)
        put(R.pt, (d,), both, ao * ap)
    hops = []
    for k in range(1, 4):
        zt = lax.rem(z + k, 4)
        src = R.pt.at[jnp.where(zt > z, 0, 1)]
        hops.append(go(remote(src, R.rz.at[z], R.sz_s.at[k - 1], R.sz_r.at[k - 1], to(z=zt))))
    out_ys[0].wait_recv()
    out_xs = go(out_x())
    send_weights(6, ("up",))
    send_weights(3, ("up",))
    for h_ in hops:
        h_.wait_recv()

    def enter(d):
        def one(i, e):
            at = i if d == 0 else 3 - i
            return decay(R.rz, at) * e + state(R.rz, at)

        return lax.fori_loop(0, z if d == 0 else 3 - z, one, jnp.zeros((W, W), F32))

    for d in range(2):
        e = enter(d)
        so, ao = state(R.ct, y, d), decay(R.ct, y, d)
        sp_, ap = state(R.ry, d), decay(R.ry, d)
        R.ce[y, d] = jnp.where(y == d, e, ap * e + sp_).astype(BF16)
        R.yb[d] = jnp.where(y == d, ao * e + so, e).astype(BF16)
    step = hop(2, R.yb, R.ce.at[y], to(y=1 - y))
    out_cs = []
    for i in (1, 2):
        out_ys[i].wait_recv()
        out_cs.append(go(out_c(i - 1)))
    send_weights(5, ("up",))
    send_weights(4, ("up",))
    step.wait_recv()
    for hp in range(2):
        for d in range(2):
            e = R.ce[hp, d].astype(F32)
            so, ao = state(R.stb, c, hp, d), decay(R.stb, c, hp, d)
            sp_, ap = state(R.rc, hp, d), decay(R.rc, hp, d)
            R.ent[c, hp, d] = jnp.where(c == d, e, ap * e + sp_).astype(BF16)
            R.cb[hp, d] = jnp.where(c == d, ao * e + so, e).astype(BF16)
    step = hop(3, R.cb, R.ent.at[c], to(c=1 - c))
    out_xs.wait_recv()
    for i in (2, 3):
        out_cs.append(go(out_c(i)))
    step.wait_recv()

    def finish(half, write):
        at_rows = pl.ds(pl.multiple_of(half * H, H), H)
        for h in range(f.heads):
            at = slice(h * W, (h + 1) * W)
            total = R.local[at_rows, at]
            for d in range(2):
                total += dot(R.carry[d, at_rows, at], R.ent[h // 2, h % 2, d], ((1,), (1,)))
            mean = jnp.mean(total * total, axis=-1, keepdims=True)
            gate = R.og[at_rows, at].astype(F32)
            write(
                at,
                (
                    total * lax.rsqrt(mean + EPSILON) * R.hscale[...] * (gate * jax.nn.sigmoid(gate))
                ).astype(BF16),
            )

    def write_peer(at, value):
        R.gb[:, at] = value

    def write_own(at, value):
        R.sw[x, :, at] = value

    finish(1 - x, write_peer)
    step = hop(4, R.gb, R.sw.at[x], to(x=1 - x))
    finish(x, write_own)
    for o in out_cs:
        o.wait_recv()
    step.wait_recv()
    square = jnp.zeros((H, 1), F32)
    width = g.c * LANES
    for p in range(Q):
        at = slice(p * width, (p + 1) * width)
        total = R.res[:, at].astype(F32)
        for t in range(2):
            total += dot(R.sw[t], R.outm[p // 2, p % 2, t * f.width : (t + 1) * f.width], ((1,), (0,)))
        R.after[:, at] = total
        square += jnp.sum(total * total, axis=-1, keepdims=True)
    scale = lax.rsqrt(square / D + EPSILON)
    for p in range(Q):
        at = slice(p * width, (p + 1) * width)
        R.tok[z, y, x, :, at] = (R.after[:, at] * scale * R.pscale[:, at]).astype(BF16)

    n, S = 2 * SLICES, f.step

    def cols(k):
        return slice(k * S, (k + 1) * S)

    def cds(k):
        return pl.ds(k * S, S)

    ag = []
    for k in range(n):
        ag.append(
            ZGather(
                R.tok.at[z, y, x, :, cds(k)],
                lambda t, k=k: R.tok.at[t, y, x, :, cds(k)],
                lambda j, k=k: R.az_s.at[k, j],
                lambda j, k=k: R.az_r.at[k, j],
            )
        )

    def pair(t):
        return (t, t + SLICES)

    def second(k):
        src = R.tok.at[:, y, x, :, cds(k)]
        dev = to(x=1 - x) if k < SLICES else to(y=1 - y)
        return remote(src, src, R.a2_s.at[k], R.a2_r.at[k], dev)

    def third(k):
        if k < SLICES:
            src, dev = R.tok.at[:, y, :, :, cds(k)], to(y=1 - y)
        else:
            src, dev = R.tok.at[:, :, x, :, cds(k)], to(x=1 - x)
        return remote(src, src, R.a3_s.at[k], R.a3_r.at[k], dev)

    def up(k, first):
        wait_weights(k, 0)
        tall = g.y * g.x * H

        def body(i, _):
            at = pl.ds(pl.multiple_of(i * tall, tall), tall)
            value = dot(R.tok[i, :, :, :, cols(k)].reshape(tall, S), R.wup[cols(k), :], ((1,), (0,)))
            R.acc[at, :] = value if first else R.acc[at, :] + value
            return 0

        lax.fori_loop(0, g.z, body, 0)

    for t in range(SLICES):
        for k in pair(t):
            ag[k].start()
    own_weights(("down",))
    flying = {}
    for t in range(SLICES + 3):
        if t < SLICES:
            for k in pair(t):
                ag[k].forward()
        if 0 <= t - 1 < SLICES:
            for k in pair(t - 1):
                ag[k].finish()
                flying[2, k] = go(second(k))
        if t < SLICES:
            pass_weights(2 * t, ("up",))
            pass_weights(2 * t + 1, ("up",))
            send_weights(2 * t + 1, ("down",))
            if 2 * t + 2 < Q:
                send_weights(2 * t + 2, ("down",))
        if 0 <= t - 2 < SLICES:
            for k in pair(t - 2):
                flying[2, k].wait_recv()
                flying[3, k] = go(third(k))
        if 0 <= t - 3 < SLICES:
            for k in pair(t - 3):
                flying[3, k].wait_recv()
                up(k, k == 0)

    for i in range(Q):
        for e, row in enumerate((i * L, (i + 1) * L - 1)):
            value = R.acc[row : row + 1, :].astype(BF16).astype(F32)
            for b in range(2 * f.most):
                R.ed[b, 2 * i + e : 2 * i + e + 1, :] = value[:, b * LANES : (b + 1) * LANES]
    edges = go(
        remote(R.ed, R.er.at[:, pl.ds(8, 2 * Q), :], R.ed_s.at[0], R.ed_r.at[0], to(c=1 - c))
    )
    for p in range(Q):
        pass_weights(p, ("down",))
    edges.wait_recv()
    top = lax.broadcasted_iota(jnp.int32, (L, LANES), 0)

    def conv(i, _):
        at = pl.ds(pl.multiple_of(i * L, L), L)
        for b in range(f.most):
            def branch(ref, off):
                col = slice(off + b * LANES, off + (b + 1) * LANES)
                tap = ref[:, pl.ds(pl.multiple_of((mine + b) * LANES, LANES), LANES)]
                value = R.acc[at, col].astype(BF16).astype(F32)
                before = R.er[off // LANES + b, pl.ds(7 + 2 * (i + c), 1), :]
                behind = R.er[off // LANES + b, pl.ds(8 + 2 * (i + c), 1), :]
                above = jnp.where(top == 0, before, pltpu.roll(value, 1, 0))
                below = jnp.where(top == L - 1, behind, pltpu.roll(value, L - 1, 0))
                return above * tap[0:1] + value * tap[1:2] + below * tap[2:3]

            gate = branch(R.gtaps, 0)
            value = branch(R.vtaps, U)
            R.hid[at, b * LANES : (b + 1) * LANES] = (
                gate * jax.nn.sigmoid(gate) * value
            ).astype(BF16)
        return 0

    lax.fori_loop(0, Q, conv, 0)
    for p in range(Q):
        wait_weights(p, 1)

    def down(k):
        tall = g.y * g.x * H

        def body(i, _):
            at = pl.ds(pl.multiple_of(i * tall, tall), tall)
            value = dot(R.hid[at, :], R.wdn[:, cols(k)], ((1,), (0,)))
            R.part[i, :, :, :, cols(k)] = value.astype(BF16).reshape(g.y, g.x, H, S)
            return 0

        lax.fori_loop(0, g.z, body, 0)

    def first_sum(k):
        if k < SLICES:
            src, dev = R.part.at[:, 1 - y, :, :, cds(k)], to(y=1 - y)
        else:
            src, dev = R.part.at[:, :, 1 - x, :, cds(k)], to(x=1 - x)
        return remote(src, R.r1.at[k], R.r1_s.at[k], R.r1_r.at[k], dev)

    def second_sum(k):
        if k < SLICES:
            src, dev = R.part.at[:, y, 1 - x, :, cds(k)], to(x=1 - x)
        else:
            src, dev = R.part.at[:, 1 - y, x, :, cds(k)], to(y=1 - y)
        return remote(src, R.r2.at[k], R.r2_s.at[k], R.r2_r.at[k], dev)

    def add_first(k):
        def body(i, _):
            zi, j = i // 2, lax.rem(i, 2)
            at = (zi, y, j) if k < SLICES else (zi, j, x)
            at = at + (slice(None), cols(k))
            R.part[at] = (R.part[at].astype(F32) + R.r1[k, zi, j].astype(F32)).astype(BF16)
            return 0

        lax.fori_loop(0, 2 * g.z, body, 0)

    def add_second(k):
        def body(i, _):
            at = (i, y, x, slice(None), cols(k))
            R.part[at] = (R.part[at].astype(F32) + R.r2[k, i].astype(F32)).astype(BF16)
            return 0

        lax.fori_loop(0, g.z, body, 0)

    def last_sums(k):
        sums = []
        for j in range(1, 4):
            zt = lax.rem(z + j, 4)
            src = R.part.at[zt, y, x, :, cds(k)]
            sums.append(
                go(remote(src, R.r3.at[k, j - 1], R.r3_s.at[k, j - 1], R.r3_r.at[k, j - 1], to(z=zt)))
            )
        return sums

    for t in range(SLICES):
        for k in pair(t):
            down(k)
            flying[4, k] = go(first_sum(k))
    for t in range(1, SLICES + 3):
        if t - 1 < SLICES:
            for k in pair(t - 1):
                flying[4, k].wait_recv()
                add_first(k)
                flying[5, k] = go(second_sum(k))
        if 0 <= t - 2 < SLICES:
            for k in pair(t - 2):
                flying[5, k].wait_recv()
                add_second(k)
                flying[6, k] = last_sums(k)
        if 0 <= t - 3 < SLICES:
            for k in pair(t - 3):
                total = R.after[:, cols(k)] + R.part[z, y, x, :, cols(k)].astype(F32)
                for j, cp in enumerate(flying[6, k]):
                    cp.wait_recv()
                    total += R.r3[k, j].astype(F32)
                R.out[:, cols(k)] = total.astype(BF16)
    for cond, cp in drains:
        if cond is None:
            cp.wait_send()
        else:
            pl.when(cond)(cp.wait_send)


def fused(grid, f, args):
    scratch = f.scratch()
    vmem = pl.BlockSpec(memory_space=pltpu.VMEM)
    anyw = pl.BlockSpec(memory_space=pl.ANY)
    return pl.pallas_call(
        functools.partial(fused_kernel, f, list(scratch)),
        out_shape=jax.ShapeDtypeStruct((f.rows, f.depth), BF16),
        in_specs=[vmem] * 12 + [anyw] * 4,
        out_specs=vmem,
        scratch_shapes=list(scratch.values()),
        compiler_params=pltpu.CompilerParams(
            collective_id=next(grid.ids), has_side_effects=True, vmem_limit_bytes=60000000
        ),
    )(*args)


def on_device(
    grid,
    residual,
    forget_forward,
    forget_backward,
    value_written,
    query_logits,
    output_gate_logits,
    forget_minimum,
    extra_log_rate,
    head_norm_scale,
    output_matrix,
    prenorm_scale,
    gate_up_matrix,
    value_up_matrix,
    gate_taps,
    value_taps,
    down_matrix,
):
    shape = (
        value_written.shape[1] // HEAD_WIDTH,
        value_written.shape[0],
        gate_up_matrix.shape[0] * grid.sp,
        gate_up_matrix.shape[1],
        value_written.shape[1],
    )
    if Fused.fits(grid, *shape, output_matrix.shape[1] * grid.sp):
        return fused(
            grid,
            Fused(grid, *shape),
            (
                forget_forward,
                forget_backward,
                value_written,
                query_logits,
                output_gate_logits,
                forget_minimum,
                extra_log_rate,
                head_norm_scale[None],
                residual,
                prenorm_scale[None],
                gate_taps,
                value_taps,
                output_matrix,
                gate_up_matrix,
                value_up_matrix,
                down_matrix,
            ),
        )
    sp, tp = grid.sp, grid.x
    length, width = value_written.shape
    heads = width // HEAD_WIDTH
    depth, units = gate_up_matrix.shape
    unit = units // sp
    me = lax.axis_index("sp")

    out_full = lax.all_gather(output_matrix, "sp", axis=1, tiled=True)

    def cut(w):
        return w.reshape(depth, sp, unit).transpose(1, 0, 2)

    up = jnp.concatenate([cut(gate_up_matrix), cut(value_up_matrix)], axis=2)
    down = down_matrix.reshape(sp, unit, down_matrix.shape[1])
    up, down = exchange(grid, [(up, "sp"), (down, "sp")], True)
    up = up.reshape(sp * depth, 2 * unit)
    down = down.transpose(1, 0, 2).reshape(unit, -1)

    local, carry, state, decay = pl.pallas_call(
        functools.partial(local_kernel, heads),
        out_shape=(
            jax.ShapeDtypeStruct((length, width), F32),
            jax.ShapeDtypeStruct((2, length, width), BF16),
            jax.ShapeDtypeStruct((2, heads, HEAD_WIDTH, HEAD_WIDTH), BF16),
            jax.ShapeDtypeStruct((2, heads, DECAY_ROWS, HEAD_WIDTH), BF16),
        ),
    )(forget_forward, forget_backward, value_written, query_logits, forget_minimum, extra_log_rate)

    rows = 2 * heads * HEAD_WIDTH // sp
    decays = jnp.repeat(
        decay.reshape(2 * heads, DECAY_ROWS, HEAD_WIDTH), sp // (2 * heads), axis=0
    )
    message = jnp.concatenate([state.reshape(sp, rows, HEAD_WIDTH), decays], axis=1)
    (got,) = exchange(grid, [(message, "sp")], True)
    prefix = pl.pallas_call(
        functools.partial(prefix_kernel, rows),
        out_shape=jax.ShapeDtypeStruct((sp, rows, HEAD_WIDTH), BF16),
    )(got)
    (entering,) = exchange(grid, [(prefix, "sp")], True)
    gated = pl.pallas_call(
        functools.partial(finish_kernel, heads),
        out_shape=jax.ShapeDtypeStruct((length, width), BF16),
    )(
        local,
        carry,
        entering.reshape(2, heads, HEAD_WIDTH, HEAD_WIDTH),
        output_gate_logits,
        head_norm_scale[None],
    )
    (swapped,) = exchange(grid, [(gated.reshape(tp, length // tp, width), "x")], True)
    token_rows = swapped.transpose(1, 0, 2).reshape(length // tp, tp * width)
    mixed = jnp.dot(token_rows, out_full, preferred_element_type=F32)
    own_after = residual.astype(F32) + mixed
    mean = jnp.mean(own_after * own_after, axis=-1, keepdims=True)
    normed = (own_after * lax.rsqrt(mean + EPSILON) * prenorm_scale).astype(BF16)
    everyone = gather(grid, normed)
    tokens = everyone.reshape(-1, normed.shape[1])
    upward = jnp.dot(tokens, up, preferred_element_type=F32).astype(BF16)
    padded = jnp.pad(upward, ((1, 1), (0, 0)))
    taps = jnp.concatenate(
        [
            lax.dynamic_slice_in_dim(gate_taps, me * unit, unit, 1),
            lax.dynamic_slice_in_dim(value_taps, me * unit, unit, 1),
        ],
        axis=1,
    )
    count = tokens.shape[0]
    conv = padded[:count] * taps[0] + padded[1 : count + 1] * taps[1] + padded[2:] * taps[2]
    hidden = (jax.nn.silu(conv[:, :unit]) * conv[:, unit:]).astype(BF16)
    parts = hidden.reshape(everyone.shape[:-1] + (unit,))
    half = down.shape[1] // 2

    def project(order, weights):
        moved = parts.transpose(*order, 4, 5)
        product = jnp.dot(moved.reshape(-1, unit), weights, preferred_element_type=F32)
        return product.astype(BF16).reshape(moved.shape[:-1] + (weights.shape[1],))

    down_sum = reduce_scatter(
        grid, project((2, 3, 1, 0), down[:, :half]), project((2, 1, 3, 0), down[:, half:])
    )
    return (own_after + down_sum).astype(BF16)


def solution(mesh):
    return jax.shard_map(
        functools.partial(on_device, Grid(mesh)),
        mesh=mesh,
        in_specs=(
            P(("sp", "tp"), None),
            P("sp", "tp"),
            P("sp", "tp"),
            P("sp", "tp"),
            P("sp", "tp"),
            P("sp", "tp"),
            P(None, "tp"),
            P(None, "sp", "tp"),
            P(),
            P(None, "sp"),
            P(),
            P("sp", "tp"),
            P("sp", "tp"),
            P(None, "tp"),
            P(None, "tp"),
            P("tp", "sp"),
        ),
        out_specs=P(("sp", "tp"), None),
        check_vma=False,
    )
```

```python
import functools
import math

import jax
import jax.numpy as jnp
from jax import lax
from jax.experimental import pallas as pl
from jax.experimental.pallas import tpu as pltpu
from jax.sharding import PartitionSpec as P

HEAD_WIDTH = 128
EPSILON = 1e-06
MESH = pl.DeviceIdType.MESH
F32 = jnp.float32
BF16 = jnp.bfloat16
DECAY_ROWS = 16
CHUNKS = 4


class Grid:
    def __init__(self, mesh):
        sp, tp = mesh.shape["sp"], mesh.shape["tp"]
        self.sp, self.x = sp, tp
        self.c = math.gcd(sp, 2)
        self.y = math.gcd(sp // self.c, 2)
        self.z = sp // (self.c * self.y)
        self.ids = iter(range(100))

    def size(self, dim):
        return getattr(self, dim)

    def place(self):
        s, t = lax.axis_index("sp"), lax.axis_index("tp")
        return {
            "sp": s,
            "x": t,
            "c": lax.rem(s, self.c),
            "y": lax.rem(s // self.c, self.y),
            "z": s // (self.c * self.y),
        }

    def peer(self, place, dim, index):
        if dim == "sp":
            return {"sp": index, "tp": place["x"]}
        at = dict(place)
        at[dim] = index
        return {"sp": (at["z"] * self.y + at["y"]) * self.c + at["c"], "tp": at["x"]}

    def greet(self, place, dims):
        barrier = pltpu.get_barrier_semaphore()
        count = 0
        for dim in dims:
            n = self.size(dim)
            for k in range(1, n):
                peer = self.peer(place, dim, lax.rem(place[dim] + k, n))
                pl.semaphore_signal(barrier, inc=1, device_id=peer, device_id_type=MESH)
                count += 1
        pl.semaphore_wait(barrier, count)


def exchange_kernel(grid, dims, keep, *refs):
    m = len(dims)
    ins, outs = refs[:m], refs[m : 2 * m]
    send_sem, recv_sem, own_sem = refs[2 * m :]
    place = grid.place()
    copies = []
    grid.greet(place, sorted(set(dims)))
    base = 0
    for i, dim in enumerate(dims):
        n, me = grid.size(dim), place[dim]
        for k in range(1, n):
            to = lax.rem(me + k, n)
            slot = me if keep else k - 1
            copy = pltpu.make_async_remote_copy(
                src_ref=ins[i].at[to],
                dst_ref=outs[i].at[slot],
                send_sem=send_sem.at[base + k - 1],
                recv_sem=recv_sem.at[base + k - 1],
                device_id=grid.peer(place, dim, to),
                device_id_type=MESH,
            )
            copy.start()
            copies.append(copy)
        base += n - 1
    if keep:
        for i, dim in enumerate(dims):
            me = place[dim]
            own = pltpu.make_async_copy(ins[i].at[me], outs[i].at[me], own_sem.at[i])
            own.start()
            copies.append(own)
    for copy in copies:
        copy.wait()


def exchange(grid, items, keep):
    dims = tuple(d for _, d in items)
    total = sum(grid.size(d) - 1 for d in dims)
    shapes = tuple(
        jax.ShapeDtypeStruct(a.shape if keep else (a.shape[0] - 1,) + a.shape[1:], a.dtype)
        for a, _ in items
    )
    return pl.pallas_call(
        functools.partial(exchange_kernel, grid, dims, keep),
        out_shape=shapes,
        in_specs=[pl.BlockSpec(memory_space=pl.ANY)] * len(items),
        out_specs=[pl.BlockSpec(memory_space=pl.ANY)] * len(items),
        scratch_shapes=[
            pltpu.SemaphoreType.DMA((total,)),
            pltpu.SemaphoreType.DMA((total,)),
            pltpu.SemaphoreType.DMA((len(items),)),
        ],
        compiler_params=pltpu.CompilerParams(
            collective_id=next(grid.ids), has_side_effects=True
        ),
    )(*[a for a, _ in items])


def gather_kernel(grid, x_ref, out_ref, send_sem, recv_sem, own_sem):
    place = grid.place()
    z, y, c, x = (place[d] for d in "zycx")
    part = x_ref.shape[1] // (2 * CHUNKS)
    grid.greet(place, ("z", "y", "c", "x"))
    own = pltpu.make_async_copy(x_ref, out_ref.at[z, y, c, x], own_sem)
    own.start()
    used = 0

    def push(dim, src, dst):
        nonlocal used
        n, copies = grid.size(dim), []
        for k in range(1, n):
            copy = pltpu.make_async_remote_copy(
                src_ref=src,
                dst_ref=dst,
                send_sem=send_sem.at[used],
                recv_sem=recv_sem.at[used],
                device_id=grid.peer(place, dim, lax.rem(place[dim] + k, n)),
                device_id_type=MESH,
            )
            copy.start()
            copies.append(copy)
            used += 1
        return copies

    def start(level, t):
        both = pl.ds(2 * t * part, 2 * part)
        first, second = pl.ds(2 * t * part, part), pl.ds((2 * t + 1) * part, part)
        if level == 0:
            return push("z", x_ref.at[:, both], out_ref.at[z, y, c, x, :, both])
        if level == 1:
            a = out_ref.at[:, y, c, x, :, first]
            b = out_ref.at[:, y, c, x, :, second]
            return push("y", a, a) + push("x", b, b)
        if level == 2:
            a = out_ref.at[:, :, c, x, :, first]
            b = out_ref.at[:, y, c, :, :, second]
            return push("x", a, a) + push("y", b, b)
        a = out_ref.at[:, :, c, :, :, both]
        return push("c", a, a)

    flying = {(0, t): start(0, t) for t in range(CHUNKS)}
    own.wait()
    for step in range(CHUNKS + 3):
        for level in range(4):
            t = step - level
            if 0 <= t < CHUNKS:
                for copy in flying[level, t]:
                    copy.wait()
                if level < 3:
                    flying[level + 1, t] = start(level + 1, t)


def gather(grid, array):
    total = CHUNKS * sum(grid.size(d) - 1 for d in "zyyxxc")
    return pl.pallas_call(
        functools.partial(gather_kernel, grid),
        out_shape=jax.ShapeDtypeStruct(
            (grid.z, grid.y, grid.c, grid.x) + array.shape, array.dtype
        ),
        in_specs=[pl.BlockSpec(memory_space=pltpu.VMEM)],
        out_specs=pl.BlockSpec(memory_space=pl.ANY),
        scratch_shapes=[
            pltpu.SemaphoreType.DMA((total,)),
            pltpu.SemaphoreType.DMA((total,)),
            pltpu.SemaphoreType.DMA,
        ],
        compiler_params=pltpu.CompilerParams(
            collective_id=next(grid.ids), has_side_effects=True
        ),
    )(array)


ORDERS = ("cxyz", "cyxz")


def reduce_kernel(grid, a_ref, b_ref, out_ref, *scratch):
    held, got, (send_sem, recv_sem, own_sem) = scratch[:2], scratch[2:10], scratch[10:]
    terms = (a_ref, b_ref)
    place = grid.place()
    rows, part = held[0].shape[-2:]
    grid.greet(place, ("z", "y", "c", "x"))
    used = 0

    def start(level, t):
        nonlocal used
        copies = []
        for color in range(2):
            dim = ORDERS[color][level]
            n, me = grid.size(dim), place[dim]
            for k in range(1, n):
                to = lax.rem(me + k, n)
                if level == 0:
                    src = terms[color].at[to, :, :, :, :, pl.ds(t * part, part)]
                else:
                    before = tuple(place[d] for d in ORDERS[color][1:level])
                    src = held[color].at[(t,) + before + (to,)]
                copy = pltpu.make_async_remote_copy(
                    src_ref=src,
                    dst_ref=got[2 * level + color].at[t, k - 1],
                    send_sem=send_sem.at[used],
                    recv_sem=recv_sem.at[used],
                    device_id=grid.peer(place, dim, to),
                    device_id_type=MESH,
                )
                copy.start()
                copies.append(copy)
                used += 1
        return copies

    def add(level, t):
        for color in range(2):
            order = ORDERS[color]
            here = tuple(place[d] for d in order[1 : level + 1])
            left = [grid.size(d) for d in order[level + 1 :]]
            peers = grid.size(order[level]) - 1
            where = got[2 * level + color]

            def block(i, _, color=color, here=here, left=left, peers=peers, where=where):
                index, rest = [], i
                for n in reversed(left):
                    index.insert(0, lax.rem(rest, n))
                    rest = rest // n
                index = tuple(index)
                total = held[color][(t,) + here + index].astype(F32)
                for k in range(peers):
                    total += where[(t, k) + index].astype(F32)
                if level < 3:
                    held[color][(t,) + here + index] = total.astype(BF16)
                else:
                    first = (color * CHUNKS + t) * part
                    out_ref[:, first : first + part] = total
                return 0

            if left:
                lax.fori_loop(0, math.prod(left), block, 0)
            else:
                block(0, 0)

    flying = {(0, t): start(0, t) for t in range(CHUNKS)}
    for t in range(CHUNKS):
        for color in range(2):
            own = pltpu.make_async_copy(
                terms[color].at[place["c"], :, :, :, :, pl.ds(t * part, part)],
                held[color].at[t],
                own_sem.at[t, color],
            )
            own.start()
            flying[0, t].append(own)
    for step in range(CHUNKS + 3):
        for level in range(4):
            t = step - level
            if 0 <= t < CHUNKS:
                for copy in flying[level, t]:
                    copy.wait()
                add(level, t)
                if level < 3:
                    flying[level + 1, t] = start(level + 1, t)


def reduce_scatter(grid, first, second):
    rows, cols = first.shape[-2:]
    tile = (rows, cols // CHUNKS)

    def sizes(order):
        return tuple(grid.size(d) for d in order)

    scratch = [pltpu.VMEM((CHUNKS,) + sizes(o[1:]) + tile, BF16) for o in ORDERS]
    for level in range(4):
        for o in ORDERS:
            peers = grid.size(o[level]) - 1
            scratch.append(
                pltpu.VMEM((CHUNKS, max(peers, 1)) + sizes(o[level + 1 :]) + tile, BF16)
            )
    total = 2 * CHUNKS * sum(grid.size(d) - 1 for d in "cxyz")
    return pl.pallas_call(
        functools.partial(reduce_kernel, grid),
        out_shape=jax.ShapeDtypeStruct((rows, 2 * cols), F32),
        in_specs=[pl.BlockSpec(memory_space=pl.ANY)] * 2,
        out_specs=pl.BlockSpec(memory_space=pltpu.VMEM),
        scratch_shapes=scratch
        + [
            pltpu.SemaphoreType.DMA((total,)),
            pltpu.SemaphoreType.DMA((total,)),
            pltpu.SemaphoreType.DMA((CHUNKS, 2)),
        ],
        compiler_params=pltpu.CompilerParams(
            collective_id=next(grid.ids), has_side_effects=True, vmem_limit_bytes=64000000
        ),
    )(first, second)


def dot(a, b, dims, precision=None):
    return lax.dot_general(
        a, b, (dims, ((), ())), precision=precision, preferred_element_type=F32
    )


def local_kernel(
    heads, zf_ref, zb_ref, v_ref, q_ref, floor_ref, extra_ref, out_ref, carry_ref, state_ref, decay_ref
):
    length = v_ref.shape[0]
    rows = lax.broadcasted_iota(jnp.int32, (length, length), 0)
    cols = lax.broadcasted_iota(jnp.int32, (length, length), 1)
    middle = length // 2
    for h in range(heads):
        at = slice(h * HEAD_WIDTH, (h + 1) * HEAD_WIDTH)
        values = v_ref[:, at]
        logits = q_ref[:, at].astype(F32)
        queries = logits * jax.nn.sigmoid(logits)
        scores = jnp.zeros((length, length), F32)
        for d, z_ref in enumerate((zf_ref, zb_ref)):
            mask = rows >= cols if d == 0 else rows <= cols
            z = z_ref[:, at].astype(F32)
            floor = floor_ref[d : d + 1, at]
            rest = 1.0 - floor
            logf = jnp.log(floor + rest * jax.nn.sigmoid(z)) + extra_ref[d, :, h : h + 1]
            key = rest * jax.nn.sigmoid(-z)
            running = dot(
                jnp.where(mask, 1.0, 0.0), logf, ((1,), (0,)), lax.Precision.HIGHEST
            )
            last = length - 1 if d == 0 else 0
            total = running[last : last + 1]
            centred = running - running[middle : middle + 1]
            part = dot(
                (queries * jnp.exp(centred)).astype(BF16),
                (key * jnp.exp(-centred)).astype(BF16),
                ((1,), (1,)),
            )
            scores += jnp.where(mask, part, 0.0)
            carry_ref[d, :, at] = (queries * jnp.exp(running)).astype(BF16)
            fresh = (key * jnp.exp(total - running)).astype(BF16)
            state_ref[d, h] = dot(values, fresh, ((0,), (0,))).astype(BF16)
            decay_ref[d, h] = jnp.broadcast_to(
                jnp.exp(total), (DECAY_ROWS, HEAD_WIDTH)
            ).astype(BF16)
        out_ref[:, at] = dot(scores.astype(BF16), values, ((1,), (0,)))


def prefix_kernel(rows, got_ref, out_ref):
    n = got_ref.shape[0]
    forward = lax.axis_index("sp") < n // 2

    def hop(k, carry):
        at = jnp.where(forward, k, n - 1 - k)
        out_ref[at] = carry.astype(BF16)
        block = got_ref[at].astype(F32)
        return block[rows : rows + 1] * carry + block[:rows]

    lax.fori_loop(0, n, hop, jnp.zeros((rows, HEAD_WIDTH), F32))


def finish_kernel(heads, out_ref, carry_ref, enter_ref, gate_ref, scale_ref, gated_ref):
    for h in range(heads):
        at = slice(h * HEAD_WIDTH, (h + 1) * HEAD_WIDTH)
        total = out_ref[:, at]
        for d in range(2):
            total += dot(carry_ref[d, :, at], enter_ref[d, h], ((1,), (1,)))
        mean = jnp.mean(total * total, axis=-1, keepdims=True)
        g = gate_ref[:, at].astype(F32)
        gated_ref[:, at] = (
            total * lax.rsqrt(mean + EPSILON) * scale_ref[...] * (g * jax.nn.sigmoid(g))
        ).astype(BF16)


LANES = 128
PAD_ROWS = 16
GATHER_WIDTHS = (2, 2, 2, 2)
REDUCE_WIDTHS = (3, 2, 2, 1)
OUT_PIECES = 4


class Fused:
    def __init__(self, grid, heads, length, depth, units, width):
        self.grid = grid
        self.heads, self.length, self.depth = heads, length, depth
        self.quads = grid.z * grid.y
        self.blocks = units // LANES
        self.base = self.blocks // self.quads
        self.most = -(-self.blocks // self.quads)
        self.unit = self.most * LANES
        self.width = width
        self.rows = length // grid.x
        self.shards = self.quads * grid.x
        self.own = self.shards * self.rows
        self.gather = self.split(GATHER_WIDTHS)
        self.reduce = self.split(REDUCE_WIDTHS)
        self.piece = width // OUT_PIECES

    def split(self, widths):
        unit = self.depth // 2 // sum(widths)
        out = []
        for color in range(2):
            first = color * (self.depth // 2)
            for w in widths:
                out.append((first, w * unit))
                first += w * unit
        return out

    @staticmethod
    def fits(grid, heads, length, depth, units, width, out_depth):
        return (
            (grid.z, grid.y, grid.c, grid.x) == (4, 2, 2, 2)
            and heads == grid.c * grid.y
            and units % LANES == 0
            and units // LANES >= grid.z * grid.y
            and length % (16 * grid.x) == 0
            and depth == out_depth == grid.sp * LANES
            and depth % (2 * LANES * sum(GATHER_WIDTHS)) == 0
            and depth % (2 * LANES * sum(REDUCE_WIDTHS)) == 0
            and width % (16 * OUT_PIECES) == 0
        )

    def scratch(self):
        g, h2, w = self.grid, HEAD_WIDTH + PAD_ROWS, HEAD_WIDTH
        dma = pltpu.SemaphoreType.DMA
        n, m = len(self.gather), len(self.reduce)
        tall = self.quads * g.x * self.rows
        return dict(
            wup=pltpu.VMEM((self.depth, 2 * self.unit), BF16),
            wdn=pltpu.VMEM((self.unit, self.depth), BF16),
            outm=pltpu.VMEM((g.z, g.y, self.width, g.c * LANES), BF16),
            local=pltpu.VMEM((self.length, self.width), F32),
            carry=pltpu.VMEM((2, self.length, self.width), BF16),
            stb=pltpu.VMEM((2, 2, 2, h2, w), BF16),
            rc=pltpu.VMEM((2, 2, h2, w), BF16),
            ct=pltpu.VMEM((2, 2, h2, w), BF16),
            ry=pltpu.VMEM((2, h2, w), BF16),
            pt=pltpu.VMEM((2, h2, w), BF16),
            rz=pltpu.VMEM((g.z, h2, w), BF16),
            ce=pltpu.VMEM((2, 2, w, w), BF16),
            yb=pltpu.VMEM((2, w, w), BF16),
            ent=pltpu.VMEM((2, 2, 2, w, w), BF16),
            cb=pltpu.VMEM((2, 2, w, w), BF16),
            gb=pltpu.VMEM((self.length, self.width), BF16),
            xb=pltpu.VMEM((self.rows, self.depth), BF16),
            xr=pltpu.VMEM((self.rows, self.depth), BF16),
            after=pltpu.VMEM((self.rows, self.depth), F32),
            tok=pltpu.VMEM((g.z, g.y, g.x, self.rows, self.depth), BF16),
            acc=pltpu.VMEM((tall, 2 * self.unit), F32),
            ed=pltpu.VMEM((2 * self.most, 2 * self.quads, LANES), F32),
            er=pltpu.VMEM((2 * self.most, 2 * self.quads + 16, LANES), F32),
            hid=pltpu.VMEM((tall, self.unit), BF16),
            part=pltpu.VMEM((g.z, g.y, g.x, self.rows, self.depth), BF16),
            r1=pltpu.VMEM((g.z, 2, self.rows, self.depth), BF16),
            r2=pltpu.VMEM((g.z, self.rows, self.depth), BF16),
            r3=pltpu.VMEM((g.z - 1, self.rows, self.depth), BF16),
            loc_s=dma((1,)),
            oz_s=dma((OUT_PIECES, 4)), oz_r=dma((OUT_PIECES, 4)),
            oy_s=dma((OUT_PIECES,)), oy_r=dma((OUT_PIECES,)),
            oc_s=dma((OUT_PIECES,)), oc_r=dma((OUT_PIECES,)),
            xs_s=dma((4,)), xs_r=dma((4,)),
            su=pltpu.VMEM((g.z - 1, LANES, 2 * self.unit), BF16),
            sd=pltpu.VMEM((g.z - 1, self.unit, LANES), BF16),
            sy_s=dma((g.z, 6)), sy_r=dma((g.z, 6)),
            w_s=dma((self.quads, 6)), w_r=dma((self.quads, 6)),
            f_s=dma((self.quads, 2)), f_r=dma((self.quads, 2)),
            st_s=dma((4,)), st_r=dma((4,)),
            sz_s=dma((3,)), sz_r=dma((3,)),
            az_s=dma((n, 4)), az_r=dma((n, 4)),
            a2_s=dma((n,)), a2_r=dma((n,)),
            a3_s=dma((n,)), a3_r=dma((n,)),
            ed_s=dma((1,)), ed_r=dma((1,)),
            r1_s=dma((m,)), r1_r=dma((m,)),
            r2_s=dma((m,)), r2_r=dma((m,)),
            r3_s=dma((m, 3)), r3_r=dma((m, 3)),
        )


NEAR = [(0, 0), (0, 1)]
STRAIGHT = [(1, 0), (3, 0), (2, 0)]
CROSS = [(1, 1), (3, 1), (2, 1)]
INPUTS = (
    "zf",
    "zb",
    "val",
    "qry",
    "og",
    "floor",
    "extra",
    "hscale",
    "res",
    "pscale",
    "gtaps",
    "vtaps",
    "out_w",
    "gate_w",
    "value_w",
    "down_w",
)


def fused_kernel(f, names, *refs):
    R = dict(zip(INPUTS + ("out",) + tuple(names), refs))
    R = type("Refs", (), R)
    g = f.grid
    s, x = lax.axis_index("sp"), lax.axis_index("tp")
    c, y, z = lax.rem(s, 2), lax.rem(s // 2, 2), s // 4
    q = s // 2
    W, U, Q = HEAD_WIDTH, f.unit, f.quads
    H, D = f.rows, f.depth
    drains = []

    def to(z=z, y=y, c=c, x=x):
        return {"sp": (z * 2 + y) * 2 + c, "tp": x}

    def remote(src, dst, ss, rs, dev):
        return pltpu.make_async_remote_copy(
            src_ref=src, dst_ref=dst, send_sem=ss, recv_sem=rs, device_id=dev, device_id_type=MESH
        )

    def go(cp, cond=None):
        if cond is None:
            cp.start()
        else:
            pl.when(cond)(cp.start)
        drains.append((cond, cp))
        return cp

    def lane(i):
        return pl.ds(pl.multiple_of(i * LANES, LANES), LANES)

    def first_block(j):
        return (f.blocks * j) // Q

    def extra_block(j):
        return first_block(j + 1) - first_block(j) > f.base

    mine = first_block(q)
    has_extra = extra_block(q)
    main, rest = f.base * LANES, (f.most - f.base) * LANES

    def weight_copies(src_s, j, kinds, stage=None):
        start = first_block(j)
        at = pl.ds(pl.multiple_of(start * LANES, LANES), main)
        at2 = pl.ds(pl.multiple_of((start + f.base) * LANES, LANES), LANES)
        k = pl.ds(pl.multiple_of(src_s * LANES, LANES), LANES)
        wide = R.wup.at[k, :] if stage is None else R.su.at[stage]
        tall = R.wdn.at[:, k] if stage is None else R.sd.at[stage]
        out = []
        if "up" in kinds:
            out.append((0, None, R.gate_w.at[:, at], wide.at[:, pl.ds(0, main)]))
            out.append((1, None, R.value_w.at[:, at], wide.at[:, pl.ds(U, main)]))
            if rest:
                e = extra_block(j)
                out.append((2, e, R.gate_w.at[:, at2], wide.at[:, pl.ds(main, LANES)]))
                out.append((3, e, R.value_w.at[:, at2], wide.at[:, pl.ds(U + main, LANES)]))
        if "down" in kinds:
            out.append((4, None, R.down_w.at[at, :], tall.at[pl.ds(0, main), :]))
            if rest:
                out.append((5, extra_block(j), R.down_w.at[at2, :], tall.at[pl.ds(main, LANES), :]))
        return out

    def own_weights(kinds):
        for i, cond, src, dst in weight_copies(s, q, kinds):
            cp = pltpu.make_async_copy(src, dst, R.w_r.at[q, i])
            if cond is None:
                cp.start()
            else:
                pl.when(cond)(cp.start)

    def kin(dz, dy, sign=1):
        return lax.rem(z + sign * dz + 4, 4) * 2 + (1 - y if dy else y)

    def send_weights(classes, kinds):
        for dz, dy in classes:
            j = kin(dz, dy)
            for i, cond, src, dst in weight_copies(s, j, kinds):
                go(
                    remote(src, dst, R.w_s.at[2 * dz + dy, i], R.w_r.at[q, i], {"sp": j * 2 + c, "tp": x}),
                    cond,
                )

    def lend_weights(distances, kinds):
        for dz in distances:
            j = kin(dz, 1)
            for i, cond, src, dst in weight_copies(s, j, kinds, dz - 1):
                go(remote(src, dst, R.sy_s.at[dz, i], R.sy_r.at[dz, i], to(y=1 - y)), cond)

    def arrived(copies, sems):
        for i, cond, _, dst in copies:
            cp = remote(dst, dst, R.w_s.at[0, i], sems.at[i], to(y=1 - y))
            if cond is None:
                cp.wait_recv()
            else:
                pl.when(cond)(cp.wait_recv)

    def relay_weights(distances, kinds):
        peer = z * 2 + 1 - y
        k = lane(peer * 2 + c)
        for dz in distances:
            j = kin(dz, 0)
            arrived(weight_copies(s, j, kinds, dz - 1), R.sy_r.at[dz])
            dev = {"sp": j * 2 + c, "tp": x}
            if "up" in kinds:
                go(remote(R.su.at[dz - 1], R.wup.at[k, :], R.w_s.at[2 * dz + 1, 0], R.w_r.at[peer, 0], dev))
            if "down" in kinds:
                go(remote(R.sd.at[dz - 1], R.wdn.at[:, k], R.w_s.at[2 * dz + 1, 4], R.w_r.at[peer, 4], dev))

    def pass_weights(classes, kinds):
        for dz, dy in classes:
            p = kin(dz, dy, -1)
            ps = p * 2 + c
            k = lane(ps)
            if dz and dy:
                whole = []
                if "up" in kinds:
                    whole.append((0, None, None, R.wup.at[k, :]))
                if "down" in kinds:
                    whole.append((4, None, None, R.wdn.at[:, k]))
                arrived(whole, R.w_r.at[p])
            else:
                arrived(weight_copies(ps, q, kinds), R.w_r.at[p])
            if "up" in kinds:
                go(remote(R.wup.at[k, :], R.wup.at[k, :], R.f_s.at[p, 0], R.f_r.at[p, 0], to(c=1 - c)))
            if "down" in kinds:
                go(remote(R.wdn.at[:, k], R.wdn.at[:, k], R.f_s.at[p, 1], R.f_r.at[p, 1], to(c=1 - c)))

    def wait_weights(p, kind):
        k = pl.ds(pl.multiple_of((p * 2 + 1 - c) * LANES, LANES), LANES)
        ref = R.wup.at[k, :] if kind == 0 else R.wdn.at[:, k]
        remote(ref, ref, R.f_s.at[p, kind], R.f_r.at[p, kind], to(c=1 - c)).wait_recv()

    mid = (z == 1) | (z == 2)
    t0, t1 = jnp.where(z == 1, 0, 1), jnp.where(z == 2, 3, 2)
    far = jnp.where(z == 1, 0, 3)

    class ZGather:
        def __init__(self, src, dst, ss, rs):
            self.src, self.dst, self.ss, self.rs = src, dst, ss, rs

        def start(self):
            for j, t in enumerate((t0, t1)):
                go(remote(self.src, self.dst(z), self.ss(j), self.rs(z), to(z=t)))

        def arrive(self, shard):
            d = self.dst(shard)
            remote(d, d, self.ss(0), self.rs(shard), to(z=t0)).wait_recv()

        def forward(self):
            for k in range(2):
                shard = jnp.where(z == 1, 2 + k, k)
                d = self.dst(shard)
                cp = remote(d, d, self.ss(2 + k), self.rs(shard), to(z=far))

                @pl.when(mid)
                def _(cp=cp):
                    cp.wait_recv()
                    cp.start()

                drains.append((mid, cp))

        def finish(self):
            @pl.when(mid)
            def _():
                self.arrive(far)

            @pl.when(jnp.logical_not(mid))
            def _():
                for k in range(3):
                    self.arrive(jnp.where(z == 0, 1 + k, k))

    if rest:
        @pl.when(jnp.logical_not(has_extra))
        def _():
            R.wup[:, main:U] = jnp.zeros((D, LANES), BF16)
            R.wup[:, U + main :] = jnp.zeros((D, LANES), BF16)
            R.wdn[main:U, :] = jnp.zeros((LANES, D), BF16)

        for dz in range(1, g.z):
            @pl.when(jnp.logical_not(extra_block(kin(dz, 0))))
            def _(i=dz - 1):
                R.su[i, :, main:U] = jnp.zeros((LANES, LANES), BF16)
                R.su[i, :, U + main :] = jnp.zeros((LANES, LANES), BF16)
                R.sd[i, main:U, :] = jnp.zeros((LANES, LANES), BF16)

    edge = jnp.zeros((2 * f.most, 8, LANES), F32)
    R.er[:, 0:8, :] = edge
    R.er[:, 8 + 2 * Q :, :] = edge

    barrier = pltpu.get_barrier_semaphore()
    for k in range(1, Q):
        dev = {"sp": lax.rem(q + k, Q) * 2 + c, "tp": x}
        pl.semaphore_signal(barrier, inc=1, device_id=dev, device_id_type=MESH)
    pl.semaphore_signal(barrier, inc=1, device_id=to(c=1 - c), device_id_type=MESH)
    pl.semaphore_signal(barrier, inc=1, device_id=to(x=1 - x), device_id_type=MESH)
    pl.semaphore_wait(barrier, Q + 1)

    ccol = lane(c)
    O = f.piece
    own_out = pltpu.make_async_copy(
        R.out_w.at[pl.ds(pl.multiple_of(x * f.width, 16), f.width), :],
        R.outm.at[z, y, :, ccol],
        R.loc_s.at[0],
    )
    own_out.start()
    zg = []
    for i in range(OUT_PIECES):
        zg.append(
            ZGather(
                R.out_w.at[pl.ds(pl.multiple_of(x * f.width + i * O, 16), O), :],
                lambda k, i=i: R.outm.at[k, y, pl.ds(i * O, O), ccol],
                lambda j, i=i: R.oz_s.at[i, j],
                lambda j, i=i: R.oz_r.at[i, j],
            )
        )
        zg[-1].start()

    def out_y(i):
        src = R.outm.at[:, y, pl.ds(i * O, O), ccol]
        return remote(src, src, R.oy_s.at[i], R.oy_r.at[i], to(y=1 - y))

    def out_c(i):
        src = R.outm.at[:, :, pl.ds(i * O, O), ccol]
        return remote(src, src, R.oc_s.at[i], R.oc_r.at[i], to(c=1 - c))

    own_weights(("up",))
    send_weights([(0, 1)], ("up",))
    lend_weights([1], ("up",))

    L = f.length
    rows_i = lax.broadcasted_iota(jnp.int32, (L, L), 0)
    cols_i = lax.broadcasted_iota(jnp.int32, (L, L), 1)
    middle = L // 2
    for h in range(f.heads):
        at = slice(h * W, (h + 1) * W)
        values = R.val[:, at]
        logits = R.qry[:, at].astype(F32)
        queries = logits * jax.nn.sigmoid(logits)
        scores = jnp.zeros((L, L), F32)
        for d, z_ref in enumerate((R.zf, R.zb)):
            mask = rows_i >= cols_i if d == 0 else rows_i <= cols_i
            pre = z_ref[:, at].astype(F32)
            floor = R.floor[d : d + 1, at]
            span = 1.0 - floor
            logf = jnp.log(floor + span * jax.nn.sigmoid(pre)) + R.extra[d, :, h : h + 1]
            key = span * jax.nn.sigmoid(-pre)
            running = dot(jnp.where(mask, 1.0, 0.0), logf, ((1,), (0,)), lax.Precision.HIGHEST)
            last = L - 1 if d == 0 else 0
            total = running[last : last + 1]
            centred = running - running[middle : middle + 1]
            inner = dot(
                (queries * jnp.exp(centred)).astype(BF16),
                (key * jnp.exp(-centred)).astype(BF16),
                ((1,), (1,)),
            )
            scores += jnp.where(mask, inner, 0.0)
            R.carry[d, :, at] = (queries * jnp.exp(running)).astype(BF16)
            fresh = (key * jnp.exp(total - running)).astype(BF16)
            R.stb[h // 2, h % 2, d, :W] = dot(values, fresh, ((0,), (0,))).astype(BF16)
            R.stb[h // 2, h % 2, d, W:] = jnp.broadcast_to(jnp.exp(total), (PAD_ROWS, W)).astype(BF16)
        R.local[:, at] = dot(scores.astype(BF16), values, ((1,), (0,)))

    def state(ref, *at):
        return ref[at + (slice(0, W),)].astype(F32)

    def decay(ref, *at):
        return ref[at + (slice(W, W + 1),)].astype(F32)

    def put(ref, at, value, factor):
        ref[at + (slice(0, W),)] = value.astype(BF16)
        ref[at + (slice(W, W + PAD_ROWS),)] = jnp.broadcast_to(factor, (PAD_ROWS, W)).astype(BF16)

    def hop(i, src, dst, dev):
        return go(remote(src, dst, R.st_s.at[i], R.st_r.at[i], dev))

    out_ys, out_cs = {}, {}

    def out_second(i):
        zg[i].finish()
        out_ys[i] = go(out_y(i))

    def out_third(i):
        out_ys[i].wait_recv()
        out_cs[i] = go(out_c(i))

    step = hop(0, R.stb.at[1 - c], R.rc, to(c=1 - c))
    step.wait_recv()
    for hp in range(2):
        for d in range(2):
            ahead = c == d
            so, ao = state(R.stb, c, hp, d), decay(R.stb, c, hp, d)
            sp_, ap = state(R.rc, hp, d), decay(R.rc, hp, d)
            both = jnp.where(ahead, ap, ao) * jnp.where(ahead, so, sp_) + jnp.where(ahead, sp_, so)
            put(R.ct, (hp, d), both, ao * ap)
    step = hop(1, R.ct.at[1 - y], R.ry, to(y=1 - y))
    zg[0].forward()
    own_out.wait()
    step.wait_recv()
    for d in range(2):
        ahead = y == d
        so, ao = state(R.ct, y, d), decay(R.ct, y, d)
        sp_, ap = state(R.ry, d), decay(R.ry, d)
        both = jnp.where(ahead, ap, ao) * jnp.where(ahead, so, sp_) + jnp.where(ahead, sp_, so)
        put(R.pt, (d,), both, ao * ap)
    hops = []
    for k in range(1, 4):
        zt = lax.rem(z + k, 4)
        src = R.pt.at[jnp.where(zt > z, 0, 1)]
        hops.append(go(remote(src, R.rz.at[z], R.sz_s.at[k - 1], R.sz_r.at[k - 1], to(z=zt))))
    zg[1].forward()
    out_second(0)
    zg[2].forward()
    zg[3].forward()
    send_weights(STRAIGHT[:1], ("up",))
    for h_ in hops:
        h_.wait_recv()

    def enter(d):
        def one(i, e):
            at = i if d == 0 else 3 - i
            return decay(R.rz, at) * e + state(R.rz, at)

        return lax.fori_loop(0, z if d == 0 else 3 - z, one, jnp.zeros((W, W), F32))

    for d in range(2):
        e = enter(d)
        so, ao = state(R.ct, y, d), decay(R.ct, y, d)
        sp_, ap = state(R.ry, d), decay(R.ry, d)
        R.ce[y, d] = jnp.where(y == d, e, ap * e + sp_).astype(BF16)
        R.yb[d] = jnp.where(y == d, ao * e + so, e).astype(BF16)
    step = hop(2, R.yb, R.ce.at[y], to(y=1 - y))
    out_second(1)
    out_second(2)
    send_weights(STRAIGHT[1:2], ("up",))
    step.wait_recv()
    for hp in range(2):
        for d in range(2):
            e = R.ce[hp, d].astype(F32)
            so, ao = state(R.stb, c, hp, d), decay(R.stb, c, hp, d)
            sp_, ap = state(R.rc, hp, d), decay(R.rc, hp, d)
            R.ent[c, hp, d] = jnp.where(c == d, e, ap * e + sp_).astype(BF16)
            R.cb[hp, d] = jnp.where(c == d, ao * e + so, e).astype(BF16)
    step = hop(3, R.cb, R.ent.at[c], to(c=1 - c))
    out_second(3)
    out_third(0)
    lend_weights([3, 2], ("up",))
    send_weights(STRAIGHT[2:], ("up",))
    lend_weights([1, 3, 2], ("down",))
    send_weights([(0, 1)], ("down",))
    step.wait_recv()

    for first, half in enumerate((1 - x, x)):
        at_rows = pl.ds(pl.multiple_of(half * H, H), H)
        for h in range(f.heads):
            at = slice(h * W, (h + 1) * W)
            total = R.local[at_rows, at]
            for d in range(2):
                total += dot(R.carry[d, at_rows, at], R.ent[h // 2, h % 2, d], ((1,), (1,)))
            mean = jnp.mean(total * total, axis=-1, keepdims=True)
            gate = R.og[at_rows, at].astype(F32)
            R.gb[first * H : (first + 1) * H, at] = (
                total * lax.rsqrt(mean + EPSILON) * R.hscale[...] * (gate * jax.nn.sigmoid(gate))
            ).astype(BF16)
    for i in range(1, OUT_PIECES):
        out_third(i)
    for i in range(OUT_PIECES):
        out_cs[i].wait_recv()

    width = g.c * LANES
    swaps = []
    for p in range(Q):
        at = slice(p * width, (p + 1) * width)
        total = dot(R.gb[...], R.outm[p // 2, p % 2], ((1,), (0,)))
        R.xb[:, at] = total[:H].astype(BF16)
        R.after[:, at] = R.res[:, at].astype(F32) + total[H:]
        if p % 2:
            i = p // 2
            two = pl.ds(2 * i * width, 2 * width)
            swaps.append(
                go(remote(R.xb.at[:, two], R.xr.at[:, two], R.xs_s.at[i], R.xs_r.at[i], to(x=1 - x)))
            )
    square = jnp.zeros((H, 1), F32)
    for i, swap in enumerate(swaps):
        at = slice(2 * i * width, 2 * (i + 1) * width)
        swap.wait_recv()
        total = R.after[:, at] + R.xr[:, at].astype(F32)
        R.after[:, at] = total
        square += jnp.sum(total * total, axis=-1, keepdims=True)
    scale = lax.rsqrt(square / D + EPSILON)
    for p in range(Q):
        at = slice(p * width, (p + 1) * width)
        R.tok[z, y, x, :, at] = (R.after[:, at] * scale * R.pscale[:, at]).astype(BF16)

    n = len(f.gather)
    G = n // 2

    def cols(k):
        return slice(f.gather[k][0], sum(f.gather[k]))

    def cds(k):
        return pl.ds(*f.gather[k])

    ag = []
    for k in range(n):
        ag.append(
            ZGather(
                R.tok.at[z, y, x, :, cds(k)],
                lambda t, k=k: R.tok.at[t, y, x, :, cds(k)],
                lambda j, k=k: R.az_s.at[k, j],
                lambda j, k=k: R.az_r.at[k, j],
            )
        )

    def pair(t):
        return (t, t + G)

    def second(k):
        src = R.tok.at[:, y, x, :, cds(k)]
        dev = to(x=1 - x) if k < G else to(y=1 - y)
        return remote(src, src, R.a2_s.at[k], R.a2_r.at[k], dev)

    def third(k):
        if k < G:
            src, dev = R.tok.at[:, y, :, :, cds(k)], to(y=1 - y)
        else:
            src, dev = R.tok.at[:, :, x, :, cds(k)], to(x=1 - x)
        return remote(src, src, R.a3_s.at[k], R.a3_r.at[k], dev)

    def up(t, first):
        tall = g.y * g.x * H

        def body(i, _):
            at = pl.ds(pl.multiple_of(i * tall, tall), tall)
            value = 0.0
            for k in pair(t):
                rows = R.tok[i, :, :, :, cols(k)].reshape(tall, f.gather[k][1])
                value += dot(rows, R.wup[cols(k), :], ((1,), (0,)))
            R.acc[at, :] = value if first else R.acc[at, :] + value
            return 0

        lax.fori_loop(0, g.z, body, 0)

    for t in range(G):
        for k in pair(t):
            ag[k].start()
    own_weights(("down",))
    pass_weights(NEAR + STRAIGHT, ("up",))
    flying = {}
    for t in range(G + 2):
        if t < G:
            for k in pair(t):
                ag[k].forward()
            if t == G - 1:
                relay_weights([1, 3, 2], ("up",))
                send_weights(STRAIGHT, ("down",))
                relay_weights([1, 3, 2], ("down",))
        if 0 <= t - 1 < G:
            for k in pair(t - 1):
                ag[k].finish()
                flying[2, k] = go(second(k))
        if 0 <= t - 2 < G:
            for k in pair(t - 2):
                flying[2, k].wait_recv()
                flying[3, k] = go(third(k))
    pass_weights(CROSS, ("up",))
    for p in range(Q):
        wait_weights(p, 0)
    for t in range(G):
        for k in pair(t):
            flying[3, k].wait_recv()
        up(t, t == 0)

    for i in range(Q):
        for e, row in enumerate((i * L, (i + 1) * L - 1)):
            value = R.acc[row : row + 1, :].astype(BF16).astype(F32)
            for b in range(2 * f.most):
                R.ed[b, 2 * i + e : 2 * i + e + 1, :] = value[:, b * LANES : (b + 1) * LANES]
    edges = go(
        remote(R.ed, R.er.at[:, pl.ds(8, 2 * Q), :], R.ed_s.at[0], R.ed_r.at[0], to(c=1 - c))
    )
    pass_weights(NEAR + STRAIGHT + CROSS, ("down",))
    edges.wait_recv()
    top = lax.broadcasted_iota(jnp.int32, (L, LANES), 0)

    def conv(i, _):
        at = pl.ds(pl.multiple_of(i * L, L), L)
        for b in range(f.most):
            def branch(ref, off):
                col = slice(off + b * LANES, off + (b + 1) * LANES)
                tap = ref[:, pl.ds(pl.multiple_of((mine + b) * LANES, LANES), LANES)]
                value = R.acc[at, col].astype(BF16).astype(F32)
                before = R.er[off // LANES + b, pl.ds(7 + 2 * (i + c), 1), :]
                behind = R.er[off // LANES + b, pl.ds(8 + 2 * (i + c), 1), :]
                above = jnp.where(top == 0, before, pltpu.roll(value, 1, 0))
                below = jnp.where(top == L - 1, behind, pltpu.roll(value, L - 1, 0))
                return above * tap[0:1] + value * tap[1:2] + below * tap[2:3]

            gate = branch(R.gtaps, 0)
            value = branch(R.vtaps, U)
            R.hid[at, b * LANES : (b + 1) * LANES] = (
                gate * jax.nn.sigmoid(gate) * value
            ).astype(BF16)
        return 0

    lax.fori_loop(0, Q, conv, 0)
    for p in range(Q):
        wait_weights(p, 1)

    n = len(f.reduce)
    G = n // 2

    def cols(k):
        return slice(f.reduce[k][0], sum(f.reduce[k]))

    def cds(k):
        return pl.ds(*f.reduce[k])

    def pair(t):
        return (t, t + G)

    def down(k):
        tall = g.y * g.x * H

        def body(i, _):
            at = pl.ds(pl.multiple_of(i * tall, tall), tall)
            value = dot(R.hid[at, :], R.wdn[:, cols(k)], ((1,), (0,)))
            R.part[i, :, :, :, cols(k)] = value.astype(BF16).reshape(g.y, g.x, H, f.reduce[k][1])
            return 0

        lax.fori_loop(0, g.z, body, 0)

    def first_sum(k):
        if k < G:
            src, dev = R.part.at[:, 1 - y, :, :, cds(k)], to(y=1 - y)
        else:
            src, dev = R.part.at[:, :, 1 - x, :, cds(k)], to(x=1 - x)
        return remote(src, R.r1.at[:, :, :, cds(k)], R.r1_s.at[k], R.r1_r.at[k], dev)

    def second_sum(k):
        if k < G:
            src, dev = R.part.at[:, y, 1 - x, :, cds(k)], to(x=1 - x)
        else:
            src, dev = R.part.at[:, 1 - y, x, :, cds(k)], to(y=1 - y)
        return remote(src, R.r2.at[:, :, cds(k)], R.r2_s.at[k], R.r2_r.at[k], dev)

    def add_first(k):
        def body(i, _):
            zi, j = i // 2, lax.rem(i, 2)
            at = (zi, y, j) if k < G else (zi, j, x)
            at = at + (slice(None), cols(k))
            R.part[at] = (R.part[at].astype(F32) + R.r1[zi, j, :, cols(k)].astype(F32)).astype(BF16)
            return 0

        lax.fori_loop(0, 2 * g.z, body, 0)

    def add_second(k):
        def body(i, _):
            at = (i, y, x, slice(None), cols(k))
            R.part[at] = (R.part[at].astype(F32) + R.r2[i, :, cols(k)].astype(F32)).astype(BF16)
            return 0

        lax.fori_loop(0, g.z, body, 0)

    def last_sums(k):
        sums = []
        for j in range(1, 4):
            zt = lax.rem(z + j, 4)
            src = R.part.at[zt, y, x, :, cds(k)]
            sums.append(
                go(remote(src, R.r3.at[j - 1, :, cds(k)], R.r3_s.at[k, j - 1], R.r3_r.at[k, j - 1], to(z=zt)))
            )
        return sums

    def stage1(t):
        for k in pair(t):
            flying[4, k] = go(first_sum(k))

    def stage2(t):
        for k in pair(t):
            flying[4, k].wait_recv()
            add_first(k)
            flying[5, k] = go(second_sum(k))

    def stage3(t):
        for k in pair(t):
            flying[5, k].wait_recv()
            add_second(k)
            flying[6, k] = last_sums(k)

    def stage4(t):
        for k in pair(t):
            total = R.after[:, cols(k)] + R.part[z, y, x, :, cols(k)].astype(F32)
            for j, cp in enumerate(flying[6, k]):
                cp.wait_recv()
                total += R.r3[j, :, cols(k)].astype(F32)
            R.out[:, cols(k)] = total.astype(BF16)

    for t in range(G):
        for k in pair(t):
            down(k)
            if t < 2:
                flying[4, k] = go(first_sum(k))
    for t in range(G + 2):
        if t < G:
            stage2(t)
        if t + 2 < G:
            stage1(t + 2)
        if 0 <= t - 1 < G:
            stage3(t - 1)
        if 0 <= t - 2 < G:
            stage4(t - 2)
    for cond, cp in drains:
        if cond is None:
            cp.wait_send()
        else:
            pl.when(cond)(cp.wait_send)


def fused(grid, f, args):
    scratch = f.scratch()
    vmem = pl.BlockSpec(memory_space=pltpu.VMEM)
    anyw = pl.BlockSpec(memory_space=pl.ANY)
    return pl.pallas_call(
        functools.partial(fused_kernel, f, list(scratch)),
        out_shape=jax.ShapeDtypeStruct((f.rows, f.depth), BF16),
        in_specs=[vmem] * 12 + [anyw] * 4,
        out_specs=vmem,
        scratch_shapes=list(scratch.values()),
        compiler_params=pltpu.CompilerParams(
            collective_id=next(grid.ids), has_side_effects=True, vmem_limit_bytes=60000000
        ),
    )(*args)


def on_device(
    grid,
    residual,
    forget_forward,
    forget_backward,
    value_written,
    query_logits,
    output_gate_logits,
    forget_minimum,
    extra_log_rate,
    head_norm_scale,
    output_matrix,
    prenorm_scale,
    gate_up_matrix,
    value_up_matrix,
    gate_taps,
    value_taps,
    down_matrix,
):
    shape = (
        value_written.shape[1] // HEAD_WIDTH,
        value_written.shape[0],
        gate_up_matrix.shape[0] * grid.sp,
        gate_up_matrix.shape[1],
        value_written.shape[1],
    )
    if Fused.fits(grid, *shape, output_matrix.shape[1] * grid.sp):
        return fused(
            grid,
            Fused(grid, *shape),
            (
                forget_forward,
                forget_backward,
                value_written,
                query_logits,
                output_gate_logits,
                forget_minimum,
                extra_log_rate,
                head_norm_scale[None],
                residual,
                prenorm_scale[None],
                gate_taps,
                value_taps,
                output_matrix,
                gate_up_matrix,
                value_up_matrix,
                down_matrix,
            ),
        )
    sp, tp = grid.sp, grid.x
    length, width = value_written.shape
    heads = width // HEAD_WIDTH
    depth, units = gate_up_matrix.shape
    unit = units // sp
    me = lax.axis_index("sp")

    out_full = lax.all_gather(output_matrix, "sp", axis=1, tiled=True)

    def cut(w):
        return w.reshape(depth, sp, unit).transpose(1, 0, 2)

    up = jnp.concatenate([cut(gate_up_matrix), cut(value_up_matrix)], axis=2)
    down = down_matrix.reshape(sp, unit, down_matrix.shape[1])
    up, down = exchange(grid, [(up, "sp"), (down, "sp")], True)
    up = up.reshape(sp * depth, 2 * unit)
    down = down.transpose(1, 0, 2).reshape(unit, -1)

    local, carry, state, decay = pl.pallas_call(
        functools.partial(local_kernel, heads),
        out_shape=(
            jax.ShapeDtypeStruct((length, width), F32),
            jax.ShapeDtypeStruct((2, length, width), BF16),
            jax.ShapeDtypeStruct((2, heads, HEAD_WIDTH, HEAD_WIDTH), BF16),
            jax.ShapeDtypeStruct((2, heads, DECAY_ROWS, HEAD_WIDTH), BF16),
        ),
    )(forget_forward, forget_backward, value_written, query_logits, forget_minimum, extra_log_rate)

    rows = 2 * heads * HEAD_WIDTH // sp
    decays = jnp.repeat(
        decay.reshape(2 * heads, DECAY_ROWS, HEAD_WIDTH), sp // (2 * heads), axis=0
    )
    message = jnp.concatenate([state.reshape(sp, rows, HEAD_WIDTH), decays], axis=1)
    (got,) = exchange(grid, [(message, "sp")], True)
    prefix = pl.pallas_call(
        functools.partial(prefix_kernel, rows),
        out_shape=jax.ShapeDtypeStruct((sp, rows, HEAD_WIDTH), BF16),
    )(got)
    (entering,) = exchange(grid, [(prefix, "sp")], True)
    gated = pl.pallas_call(
        functools.partial(finish_kernel, heads),
        out_shape=jax.ShapeDtypeStruct((length, width), BF16),
    )(
        local,
        carry,
        entering.reshape(2, heads, HEAD_WIDTH, HEAD_WIDTH),
        output_gate_logits,
        head_norm_scale[None],
    )
    (swapped,) = exchange(grid, [(gated.reshape(tp, length // tp, width), "x")], True)
    token_rows = swapped.transpose(1, 0, 2).reshape(length // tp, tp * width)
    mixed = jnp.dot(token_rows, out_full, preferred_element_type=F32)
    own_after = residual.astype(F32) + mixed
    mean = jnp.mean(own_after * own_after, axis=-1, keepdims=True)
    normed = (own_after * lax.rsqrt(mean + EPSILON) * prenorm_scale).astype(BF16)
    everyone = gather(grid, normed)
    tokens = everyone.reshape(-1, normed.shape[1])
    upward = jnp.dot(tokens, up, preferred_element_type=F32).astype(BF16)
    padded = jnp.pad(upward, ((1, 1), (0, 0)))
    taps = jnp.concatenate(
        [
            lax.dynamic_slice_in_dim(gate_taps, me * unit, unit, 1),
            lax.dynamic_slice_in_dim(value_taps, me * unit, unit, 1),
        ],
        axis=1,
    )
    count = tokens.shape[0]
    conv = padded[:count] * taps[0] + padded[1 : count + 1] * taps[1] + padded[2:] * taps[2]
    hidden = (jax.nn.silu(conv[:, :unit]) * conv[:, unit:]).astype(BF16)
    parts = hidden.reshape(everyone.shape[:-1] + (unit,))
    half = down.shape[1] // 2

    def project(order, weights):
        moved = parts.transpose(*order, 4, 5)
        product = jnp.dot(moved.reshape(-1, unit), weights, preferred_element_type=F32)
        return product.astype(BF16).reshape(moved.shape[:-1] + (weights.shape[1],))

    down_sum = reduce_scatter(
        grid, project((2, 3, 1, 0), down[:, :half]), project((2, 1, 3, 0), down[:, half:])
    )
    return (own_after + down_sum).astype(BF16)


def solution(mesh):
    return jax.shard_map(
        functools.partial(on_device, Grid(mesh)),
        mesh=mesh,
        in_specs=(
            P(("sp", "tp"), None),
            P("sp", "tp"),
            P("sp", "tp"),
            P("sp", "tp"),
            P("sp", "tp"),
            P("sp", "tp"),
            P(None, "tp"),
            P(None, "sp", "tp"),
            P(),
            P(None, "sp"),
            P(),
            P("sp", "tp"),
            P("sp", "tp"),
            P(None, "tp"),
            P(None, "tp"),
            P("tp", "sp"),
        ),
        out_specs=P(("sp", "tp"), None),
        check_vma=False,
    )
```

```python
import functools
import math

import jax
import jax.numpy as jnp
from jax import lax
from jax.experimental import pallas as pl
from jax.experimental.pallas import tpu as pltpu
from jax.sharding import PartitionSpec as P

HEAD_WIDTH = 128
EPSILON = 1e-06
MESH = pl.DeviceIdType.MESH
F32 = jnp.float32
BF16 = jnp.bfloat16
DECAY_ROWS = 16
CHUNKS = 4


class Grid:
    def __init__(self, mesh):
        sp, tp = mesh.shape["sp"], mesh.shape["tp"]
        self.sp, self.x = sp, tp
        self.c = math.gcd(sp, 2)
        self.y = math.gcd(sp // self.c, 2)
        self.z = sp // (self.c * self.y)
        self.ids = iter(range(100))

    def size(self, dim):
        return getattr(self, dim)

    def place(self):
        s, t = lax.axis_index("sp"), lax.axis_index("tp")
        return {
            "sp": s,
            "x": t,
            "c": lax.rem(s, self.c),
            "y": lax.rem(s // self.c, self.y),
            "z": s // (self.c * self.y),
        }

    def peer(self, place, dim, index):
        if dim == "sp":
            return {"sp": index, "tp": place["x"]}
        at = dict(place)
        at[dim] = index
        return {"sp": (at["z"] * self.y + at["y"]) * self.c + at["c"], "tp": at["x"]}

    def greet(self, place, dims):
        barrier = pltpu.get_barrier_semaphore()
        count = 0
        for dim in dims:
            n = self.size(dim)
            for k in range(1, n):
                peer = self.peer(place, dim, lax.rem(place[dim] + k, n))
                pl.semaphore_signal(barrier, inc=1, device_id=peer, device_id_type=MESH)
                count += 1
        pl.semaphore_wait(barrier, count)


def exchange_kernel(grid, dims, keep, *refs):
    m = len(dims)
    ins, outs = refs[:m], refs[m : 2 * m]
    send_sem, recv_sem, own_sem = refs[2 * m :]
    place = grid.place()
    copies = []
    grid.greet(place, sorted(set(dims)))
    base = 0
    for i, dim in enumerate(dims):
        n, me = grid.size(dim), place[dim]
        for k in range(1, n):
            to = lax.rem(me + k, n)
            slot = me if keep else k - 1
            copy = pltpu.make_async_remote_copy(
                src_ref=ins[i].at[to],
                dst_ref=outs[i].at[slot],
                send_sem=send_sem.at[base + k - 1],
                recv_sem=recv_sem.at[base + k - 1],
                device_id=grid.peer(place, dim, to),
                device_id_type=MESH,
            )
            copy.start()
            copies.append(copy)
        base += n - 1
    if keep:
        for i, dim in enumerate(dims):
            me = place[dim]
            own = pltpu.make_async_copy(ins[i].at[me], outs[i].at[me], own_sem.at[i])
            own.start()
            copies.append(own)
    for copy in copies:
        copy.wait()


def exchange(grid, items, keep):
    dims = tuple(d for _, d in items)
    total = sum(grid.size(d) - 1 for d in dims)
    shapes = tuple(
        jax.ShapeDtypeStruct(a.shape if keep else (a.shape[0] - 1,) + a.shape[1:], a.dtype)
        for a, _ in items
    )
    return pl.pallas_call(
        functools.partial(exchange_kernel, grid, dims, keep),
        out_shape=shapes,
        in_specs=[pl.BlockSpec(memory_space=pl.ANY)] * len(items),
        out_specs=[pl.BlockSpec(memory_space=pl.ANY)] * len(items),
        scratch_shapes=[
            pltpu.SemaphoreType.DMA((total,)),
            pltpu.SemaphoreType.DMA((total,)),
            pltpu.SemaphoreType.DMA((len(items),)),
        ],
        compiler_params=pltpu.CompilerParams(
            collective_id=next(grid.ids), has_side_effects=True
        ),
    )(*[a for a, _ in items])


def gather_kernel(grid, x_ref, out_ref, send_sem, recv_sem, own_sem):
    place = grid.place()
    z, y, c, x = (place[d] for d in "zycx")
    part = x_ref.shape[1] // (2 * CHUNKS)
    grid.greet(place, ("z", "y", "c", "x"))
    own = pltpu.make_async_copy(x_ref, out_ref.at[z, y, c, x], own_sem)
    own.start()
    used = 0

    def push(dim, src, dst):
        nonlocal used
        n, copies = grid.size(dim), []
        for k in range(1, n):
            copy = pltpu.make_async_remote_copy(
                src_ref=src,
                dst_ref=dst,
                send_sem=send_sem.at[used],
                recv_sem=recv_sem.at[used],
                device_id=grid.peer(place, dim, lax.rem(place[dim] + k, n)),
                device_id_type=MESH,
            )
            copy.start()
            copies.append(copy)
            used += 1
        return copies

    def start(level, t):
        both = pl.ds(2 * t * part, 2 * part)
        first, second = pl.ds(2 * t * part, part), pl.ds((2 * t + 1) * part, part)
        if level == 0:
            return push("z", x_ref.at[:, both], out_ref.at[z, y, c, x, :, both])
        if level == 1:
            a = out_ref.at[:, y, c, x, :, first]
            b = out_ref.at[:, y, c, x, :, second]
            return push("y", a, a) + push("x", b, b)
        if level == 2:
            a = out_ref.at[:, :, c, x, :, first]
            b = out_ref.at[:, y, c, :, :, second]
            return push("x", a, a) + push("y", b, b)
        a = out_ref.at[:, :, c, :, :, both]
        return push("c", a, a)

    flying = {(0, t): start(0, t) for t in range(CHUNKS)}
    own.wait()
    for step in range(CHUNKS + 3):
        for level in range(4):
            t = step - level
            if 0 <= t < CHUNKS:
                for copy in flying[level, t]:
                    copy.wait()
                if level < 3:
                    flying[level + 1, t] = start(level + 1, t)


def gather(grid, array):
    total = CHUNKS * sum(grid.size(d) - 1 for d in "zyyxxc")
    return pl.pallas_call(
        functools.partial(gather_kernel, grid),
        out_shape=jax.ShapeDtypeStruct(
            (grid.z, grid.y, grid.c, grid.x) + array.shape, array.dtype
        ),
        in_specs=[pl.BlockSpec(memory_space=pltpu.VMEM)],
        out_specs=pl.BlockSpec(memory_space=pl.ANY),
        scratch_shapes=[
            pltpu.SemaphoreType.DMA((total,)),
            pltpu.SemaphoreType.DMA((total,)),
            pltpu.SemaphoreType.DMA,
        ],
        compiler_params=pltpu.CompilerParams(
            collective_id=next(grid.ids), has_side_effects=True
        ),
    )(array)


ORDERS = ("cxyz", "cyxz")


def reduce_kernel(grid, a_ref, b_ref, out_ref, *scratch):
    held, got, (send_sem, recv_sem, own_sem) = scratch[:2], scratch[2:10], scratch[10:]
    terms = (a_ref, b_ref)
    place = grid.place()
    rows, part = held[0].shape[-2:]
    grid.greet(place, ("z", "y", "c", "x"))
    used = 0

    def start(level, t):
        nonlocal used
        copies = []
        for color in range(2):
            dim = ORDERS[color][level]
            n, me = grid.size(dim), place[dim]
            for k in range(1, n):
                to = lax.rem(me + k, n)
                if level == 0:
                    src = terms[color].at[to, :, :, :, :, pl.ds(t * part, part)]
                else:
                    before = tuple(place[d] for d in ORDERS[color][1:level])
                    src = held[color].at[(t,) + before + (to,)]
                copy = pltpu.make_async_remote_copy(
                    src_ref=src,
                    dst_ref=got[2 * level + color].at[t, k - 1],
                    send_sem=send_sem.at[used],
                    recv_sem=recv_sem.at[used],
                    device_id=grid.peer(place, dim, to),
                    device_id_type=MESH,
                )
                copy.start()
                copies.append(copy)
                used += 1
        return copies

    def add(level, t):
        for color in range(2):
            order = ORDERS[color]
            here = tuple(place[d] for d in order[1 : level + 1])
            left = [grid.size(d) for d in order[level + 1 :]]
            peers = grid.size(order[level]) - 1
            where = got[2 * level + color]

            def block(i, _, color=color, here=here, left=left, peers=peers, where=where):
                index, rest = [], i
                for n in reversed(left):
                    index.insert(0, lax.rem(rest, n))
                    rest = rest // n
                index = tuple(index)
                total = held[color][(t,) + here + index].astype(F32)
                for k in range(peers):
                    total += where[(t, k) + index].astype(F32)
                if level < 3:
                    held[color][(t,) + here + index] = total.astype(BF16)
                else:
                    first = (color * CHUNKS + t) * part
                    out_ref[:, first : first + part] = total
                return 0

            if left:
                lax.fori_loop(0, math.prod(left), block, 0)
            else:
                block(0, 0)

    flying = {(0, t): start(0, t) for t in range(CHUNKS)}
    for t in range(CHUNKS):
        for color in range(2):
            own = pltpu.make_async_copy(
                terms[color].at[place["c"], :, :, :, :, pl.ds(t * part, part)],
                held[color].at[t],
                own_sem.at[t, color],
            )
            own.start()
            flying[0, t].append(own)
    for step in range(CHUNKS + 3):
        for level in range(4):
            t = step - level
            if 0 <= t < CHUNKS:
                for copy in flying[level, t]:
                    copy.wait()
                add(level, t)
                if level < 3:
                    flying[level + 1, t] = start(level + 1, t)


def reduce_scatter(grid, first, second):
    rows, cols = first.shape[-2:]
    tile = (rows, cols // CHUNKS)

    def sizes(order):
        return tuple(grid.size(d) for d in order)

    scratch = [pltpu.VMEM((CHUNKS,) + sizes(o[1:]) + tile, BF16) for o in ORDERS]
    for level in range(4):
        for o in ORDERS:
            peers = grid.size(o[level]) - 1
            scratch.append(
                pltpu.VMEM((CHUNKS, max(peers, 1)) + sizes(o[level + 1 :]) + tile, BF16)
            )
    total = 2 * CHUNKS * sum(grid.size(d) - 1 for d in "cxyz")
    return pl.pallas_call(
        functools.partial(reduce_kernel, grid),
        out_shape=jax.ShapeDtypeStruct((rows, 2 * cols), F32),
        in_specs=[pl.BlockSpec(memory_space=pl.ANY)] * 2,
        out_specs=pl.BlockSpec(memory_space=pltpu.VMEM),
        scratch_shapes=scratch
        + [
            pltpu.SemaphoreType.DMA((total,)),
            pltpu.SemaphoreType.DMA((total,)),
            pltpu.SemaphoreType.DMA((CHUNKS, 2)),
        ],
        compiler_params=pltpu.CompilerParams(
            collective_id=next(grid.ids), has_side_effects=True, vmem_limit_bytes=64000000
        ),
    )(first, second)


def dot(a, b, dims, precision=None):
    return lax.dot_general(
        a, b, (dims, ((), ())), precision=precision, preferred_element_type=F32
    )


def local_kernel(
    heads, zf_ref, zb_ref, v_ref, q_ref, floor_ref, extra_ref, out_ref, carry_ref, state_ref, decay_ref
):
    length = v_ref.shape[0]
    rows = lax.broadcasted_iota(jnp.int32, (length, length), 0)
    cols = lax.broadcasted_iota(jnp.int32, (length, length), 1)
    middle = length // 2
    for h in range(heads):
        at = slice(h * HEAD_WIDTH, (h + 1) * HEAD_WIDTH)
        values = v_ref[:, at]
        logits = q_ref[:, at].astype(F32)
        queries = logits * jax.nn.sigmoid(logits)
        scores = jnp.zeros((length, length), F32)
        for d, z_ref in enumerate((zf_ref, zb_ref)):
            mask = rows >= cols if d == 0 else rows <= cols
            z = z_ref[:, at].astype(F32)
            floor = floor_ref[d : d + 1, at]
            rest = 1.0 - floor
            logf = jnp.log(floor + rest * jax.nn.sigmoid(z)) + extra_ref[d, :, h : h + 1]
            key = rest * jax.nn.sigmoid(-z)
            running = dot(
                jnp.where(mask, 1.0, 0.0), logf, ((1,), (0,)), lax.Precision.HIGHEST
            )
            last = length - 1 if d == 0 else 0
            total = running[last : last + 1]
            centred = running - running[middle : middle + 1]
            part = dot(
                (queries * jnp.exp(centred)).astype(BF16),
                (key * jnp.exp(-centred)).astype(BF16),
                ((1,), (1,)),
            )
            scores += jnp.where(mask, part, 0.0)
            carry_ref[d, :, at] = (queries * jnp.exp(running)).astype(BF16)
            fresh = (key * jnp.exp(total - running)).astype(BF16)
            state_ref[d, h] = dot(values, fresh, ((0,), (0,))).astype(BF16)
            decay_ref[d, h] = jnp.broadcast_to(
                jnp.exp(total), (DECAY_ROWS, HEAD_WIDTH)
            ).astype(BF16)
        out_ref[:, at] = dot(scores.astype(BF16), values, ((1,), (0,)))


def prefix_kernel(rows, got_ref, out_ref):
    n = got_ref.shape[0]
    forward = lax.axis_index("sp") < n // 2

    def hop(k, carry):
        at = jnp.where(forward, k, n - 1 - k)
        out_ref[at] = carry.astype(BF16)
        block = got_ref[at].astype(F32)
        return block[rows : rows + 1] * carry + block[:rows]

    lax.fori_loop(0, n, hop, jnp.zeros((rows, HEAD_WIDTH), F32))


def finish_kernel(heads, out_ref, carry_ref, enter_ref, gate_ref, scale_ref, gated_ref):
    for h in range(heads):
        at = slice(h * HEAD_WIDTH, (h + 1) * HEAD_WIDTH)
        total = out_ref[:, at]
        for d in range(2):
            total += dot(carry_ref[d, :, at], enter_ref[d, h], ((1,), (1,)))
        mean = jnp.mean(total * total, axis=-1, keepdims=True)
        g = gate_ref[:, at].astype(F32)
        gated_ref[:, at] = (
            total * lax.rsqrt(mean + EPSILON) * scale_ref[...] * (g * jax.nn.sigmoid(g))
        ).astype(BF16)


LANES = 128
PAD_ROWS = 16
GATHER_WIDTHS = ((1, 1, 2, 1, 1), (1, 2, 3, 2, 2))
REDUCE_WIDTHS = ((1, 2, 2, 1, 1), (1, 2, 2, 1, 1))
SIDE = 1
LEND = 2
OUT_PIECES = 4


class Fused:
    def __init__(self, grid, heads, length, depth, units, width):
        self.grid = grid
        self.heads, self.length, self.depth = heads, length, depth
        self.quads = grid.z * grid.y
        self.blocks = units // LANES
        self.base = self.blocks // self.quads
        self.most = -(-self.blocks // self.quads)
        self.unit = self.most * LANES
        self.width = width
        self.rows = length // grid.x
        self.shards = self.quads * grid.x
        self.own = self.shards * self.rows
        self.gather = self.split(GATHER_WIDTHS)
        self.reduce = self.split(REDUCE_WIDTHS, 2 * SIDE)
        self.side = (depth - sum(self.reduce[-1])) // 2
        self.piece = width // OUT_PIECES

    def split(self, widths, spare=0):
        unit = self.depth // (sum(map(sum, widths)) + spare)
        out, first = [], 0
        for color in widths:
            for w in color:
                out.append((first, w * unit))
                first += w * unit
        return out

    @staticmethod
    def fits(grid, heads, length, depth, units, width, out_depth):
        return (
            (grid.z, grid.y, grid.c, grid.x) == (4, 2, 2, 2)
            and heads == grid.c * grid.y
            and units % LANES == 0
            and units // LANES >= grid.z * grid.y
            and length % (16 * grid.x) == 0
            and depth == out_depth == grid.sp * LANES
            and depth % (LANES * sum(map(sum, GATHER_WIDTHS))) == 0
            and depth % (LANES * (sum(map(sum, REDUCE_WIDTHS)) + 2 * SIDE)) == 0
            and width % (16 * OUT_PIECES) == 0
        )

    def scratch(self):
        g, h2, w = self.grid, HEAD_WIDTH + PAD_ROWS, HEAD_WIDTH
        dma = pltpu.SemaphoreType.DMA
        n, m = len(self.gather), len(self.reduce)
        tall = self.quads * g.x * self.rows
        return dict(
            wup=pltpu.VMEM((self.depth, 2 * self.unit), BF16),
            wdn=pltpu.VMEM((self.unit, self.depth), BF16),
            outm=pltpu.VMEM((g.z, g.y, self.width, g.c * LANES), BF16),
            local=pltpu.VMEM((self.length, self.width), F32),
            carry=pltpu.VMEM((2, self.length, self.width), BF16),
            stb=pltpu.VMEM((2, 2, 2, h2, w), BF16),
            rc=pltpu.VMEM((2, 2, h2, w), BF16),
            ct=pltpu.VMEM((2, 2, h2, w), BF16),
            ry=pltpu.VMEM((2, h2, w), BF16),
            pt=pltpu.VMEM((2, h2, w), BF16),
            rz=pltpu.VMEM((g.z, h2, w), BF16),
            ce=pltpu.VMEM((2, 2, w, w), BF16),
            yb=pltpu.VMEM((2, w, w), BF16),
            ent=pltpu.VMEM((2, 2, 2, w, w), BF16),
            cb=pltpu.VMEM((2, 2, w, w), BF16),
            gb=pltpu.VMEM((self.length, self.width), BF16),
            xb=pltpu.VMEM((self.rows, self.depth), BF16),
            xr=pltpu.VMEM((self.rows, self.depth), BF16),
            after=pltpu.VMEM((self.rows, self.depth), F32),
            tok=pltpu.VMEM((g.z, g.y, g.x, self.rows, self.depth), BF16),
            acc=pltpu.VMEM((tall, 2 * self.unit), F32),
            ed=pltpu.VMEM((2 * self.most, 2 * self.quads, LANES), F32),
            er=pltpu.VMEM((2 * self.most, 2 * self.quads + 16, LANES), F32),
            hid=pltpu.VMEM((tall, self.unit), BF16),
            part=pltpu.VMEM((g.z, g.y, g.x, self.rows, self.depth), BF16),
            r1=pltpu.VMEM((g.z, 2, self.rows, self.depth), BF16),
            r2=pltpu.VMEM((g.z, self.rows, self.depth), BF16),
            r3=pltpu.VMEM((g.z - 1, self.rows, self.depth), BF16),
            c1=pltpu.VMEM((g.z - 1, g.y, g.x, self.rows, 2 * self.side), BF16),
            c2=pltpu.VMEM((2, 2, self.rows, self.side), BF16),
            c3=pltpu.VMEM((2, self.rows, self.side), BF16),
            c1_s=dma((1,)), c1_r=dma((1,)),
            c2_s=dma((2,)), c2_r=dma((2,)),
            c3_s=dma((2,)), c3_r=dma((2,)),
            zf=pltpu.VMEM((self.length, self.width), BF16),
            zb=pltpu.VMEM((self.length, self.width), BF16),
            val=pltpu.VMEM((self.length, self.width), BF16),
            qry=pltpu.VMEM((self.length, self.width), BF16),
            og=pltpu.VMEM((self.length, self.width), BF16),
            res=pltpu.VMEM((self.rows, self.depth), BF16),
            in_s=dma((6,)),
            loc_s=dma((1,)),
            oz_s=dma((OUT_PIECES, 4)), oz_r=dma((OUT_PIECES, 4)),
            oy_s=dma((OUT_PIECES,)), oy_r=dma((OUT_PIECES,)),
            oc_s=dma((OUT_PIECES,)), oc_r=dma((OUT_PIECES,)),
            xs_s=dma((4,)), xs_r=dma((4,)),
            su=pltpu.VMEM((g.z - 1, LANES, 2 * self.unit), BF16),
            sd=pltpu.VMEM((g.z - 1, self.unit, LANES), BF16),
            sy_s=dma((g.z - 1, 2)), sy_r=dma((g.z - 1, 2)),
            w_s=dma((self.quads, 2)), w_r=dma((self.quads, 2)),
            f_s=dma((self.quads, 2)), f_r=dma((self.quads, 2)),
            st_s=dma((4,)), st_r=dma((4,)),
            sz_s=dma((1,)), sz_r=dma((1,)),
            az_s=dma((n, 4)), az_r=dma((n, 4)),
            ao_s=dma((2,)), ao_r=dma((2,)),
            at_s=dma((2, 2)), at_r=dma((2, 2)),
            a2_s=dma((n,)), a2_r=dma((n,)),
            a3_s=dma((n,)), a3_r=dma((n,)),
            ed_s=dma((1,)), ed_r=dma((1,)),
            r1_s=dma((m,)), r1_r=dma((m,)),
            r2_s=dma((m,)), r2_r=dma((m,)),
            r3_s=dma((m,)), r3_r=dma((m,)),
        )


NEAR = [(0, 0), (0, 1)]
STRAIGHT = [(1, 0), (3, 0), (2, 0)]
CROSS = [(1, 1), (3, 1), (2, 1)]
INPUTS = (
    "zf_in",
    "zb_in",
    "val_in",
    "qry_in",
    "og_in",
    "floor",
    "extra",
    "hscale",
    "res_in",
    "pscale",
    "gtaps",
    "vtaps",
    "out_w",
    "gate_w",
    "value_w",
    "down_w",
)


def fused_kernel(f, names, *refs):
    R = dict(zip(INPUTS + ("out",) + tuple(names), refs))
    R = type("Refs", (), R)
    g = f.grid
    s, x = lax.axis_index("sp"), lax.axis_index("tp")
    c, y, z = lax.rem(s, 2), lax.rem(s // 2, 2), s // 4
    q = s // 2
    W, U, Q = HEAD_WIDTH, f.unit, f.quads
    H, D = f.rows, f.depth
    drains = []

    def to(z=z, y=y, c=c, x=x):
        return {"sp": (z * 2 + y) * 2 + c, "tp": x}

    def remote(src, dst, ss, rs, dev):
        return pltpu.make_async_remote_copy(
            src_ref=src, dst_ref=dst, send_sem=ss, recv_sem=rs, device_id=dev, device_id_type=MESH
        )

    def go(cp, start=True):
        if start:
            cp.start()
        drains.append((None, cp))
        return cp

    def lane(i):
        return pl.ds(pl.multiple_of(i * LANES, LANES), LANES)

    def first_block(j):
        return (f.blocks * j) // Q

    def extra_block(j):
        return first_block(j + 1) - first_block(j) > f.base

    mine = first_block(q)
    has_extra = extra_block(q)
    main, rest = f.base * LANES, (f.most - f.base) * LANES

    def spots(src_s, stage):
        if stage is None:
            k = lane(src_s)
            return R.wup.at[k, :], R.wdn.at[:, k]
        return R.su.at[stage], R.sd.at[stage]

    def weight_copies(src_s, j, kind, stage=None):
        start = first_block(j)
        at = pl.ds(pl.multiple_of(start * LANES, LANES), main)
        at2 = pl.ds(pl.multiple_of((start + f.base) * LANES, LANES), LANES)
        dst = spots(src_s, stage)[kind]
        e = extra_block(j)
        if kind:
            out = [(None, R.down_w.at[at, :], dst.at[pl.ds(0, main), :])]
            if rest:
                out.append((e, R.down_w.at[at2, :], dst.at[pl.ds(main, LANES), :]))
            return out
        out = [
            (None, R.gate_w.at[:, at], dst.at[:, pl.ds(0, main)]),
            (None, R.value_w.at[:, at], dst.at[:, pl.ds(U, main)]),
        ]
        if rest:
            out.append((e, R.gate_w.at[:, at2], dst.at[:, pl.ds(main, LANES)]))
            out.append((e, R.value_w.at[:, at2], dst.at[:, pl.ds(U + main, LANES)]))
        return out

    def when(cond, act):
        if cond is None:
            act()
        else:
            pl.when(cond)(act)

    def totals(dst, kind, extra):
        less = dst.at[pl.ds(0, main), :] if kind else dst.at[:, pl.ds(0, 2 * main)]
        if not rest:
            return [(None, dst)]
        return [(extra, dst), (jnp.logical_not(extra), less)]

    def arrived(dst, kind, extra, sem):
        for cond, ref in totals(dst, kind, extra):
            when(cond, remote(ref, ref, R.w_s.at[0, kind], sem, to(y=1 - y)).wait_recv)

    def sent(dst, kind, extra, sem):
        for cond, ref in totals(dst, kind, extra):
            drains.append((cond, remote(ref, ref, sem, R.w_r.at[0, kind], to(y=1 - y))))

    def own_weights(kind):
        for cond, src, dst in weight_copies(s, q, kind):
            when(cond, pltpu.make_async_copy(src, dst, R.w_r.at[q, kind]).start)

    def kin(dz, dy, sign=1):
        return lax.rem(z + sign * dz + 4, 4) * 2 + (1 - y if dy else y)

    def send_weights(classes, kind):
        for dz, dy in classes:
            j = kin(dz, dy)
            sem = R.w_s.at[2 * dz + dy, kind]
            for cond, src, dst in weight_copies(s, j, kind):
                when(cond, remote(src, dst, sem, R.w_r.at[q, kind], {"sp": j * 2 + c, "tp": x}).start)
            sent(spots(s, None)[kind], kind, extra_block(j), sem)

    def lend_weights(distances, kind):
        for dz in distances:
            j = kin(dz, 1)
            sem = R.sy_s.at[dz - 1, kind]
            for cond, src, dst in weight_copies(s, j, kind, dz - 1):
                when(cond, remote(src, dst, sem, R.sy_r.at[dz - 1, kind], to(y=1 - y)).start)
            sent(spots(s, None)[kind], kind, extra_block(j), sem)

    def relay_weights(distances, kind):
        peer = z * 2 + 1 - y
        goal = spots(peer * 2 + c, None)[kind]
        for dz in distances:
            j = kin(dz, 0)
            extra = extra_block(j)
            held = spots(None, dz - 1)[kind]
            arrived(held, kind, extra, R.sy_r.at[dz - 1, kind])
            dev = {"sp": j * 2 + c, "tp": x}
            sem = R.w_s.at[2 * dz + 1, kind]
            if kind:
                parts = [pl.ds(0, main)]
                pick = lambda ref, part: ref.at[part, :]
            else:
                parts = [pl.ds(0, main), pl.ds(U, main)]
                pick = lambda ref, part: ref.at[:, part]
            few = [
                remote(pick(held, part), pick(goal, part), sem, R.w_r.at[peer, kind], dev)
                for part in parts
            ]
            full = remote(held, goal, sem, R.w_r.at[peer, kind], dev)
            if rest:
                pl.when(extra)(full.start)
                for cp in few:
                    pl.when(jnp.logical_not(extra))(cp.start)
            else:
                full.start()
            sent(held, kind, extra, sem)

    def pass_weights(classes, kind):
        for dz, dy in classes:
            p = kin(dz, dy, -1)
            ref = spots(p * 2 + c, None)[kind]
            arrived(ref, kind, has_extra, R.w_r.at[p, kind])
            go(remote(ref, ref, R.f_s.at[p, kind], R.f_r.at[p, kind], to(c=1 - c)))

    def wait_weights(p, kind):
        k = pl.ds(pl.multiple_of((p * 2 + 1 - c) * LANES, LANES), LANES)
        ref = R.wup.at[k, :] if kind == 0 else R.wdn.at[:, k]
        remote(ref, ref, R.f_s.at[p, kind], R.f_r.at[p, kind], to(c=1 - c)).wait_recv()

    mid = (z == 1) | (z == 2)
    t0, t1 = jnp.where(z == 1, 0, 1), jnp.where(z == 2, 3, 2)
    far = jnp.where(z == 1, 0, 3)

    class ZGather:
        def __init__(self, src, dst, ss, rs):
            self.src, self.dst, self.ss, self.rs = src, dst, ss, rs

        def start(self):
            for j, t in enumerate((t0, t1)):
                go(remote(self.src, self.dst(z), self.ss(j), self.rs(z), to(z=t)))

        def arrive(self, shard):
            d = self.dst(shard)
            remote(d, d, self.ss(0), self.rs(shard), to(z=t0)).wait_recv()

        def forward(self):
            for k in range(2):
                shard = jnp.where(z == 1, 2 + k, k)
                d = self.dst(shard)
                cp = remote(d, d, self.ss(2 + k), self.rs(shard), to(z=far))

                @pl.when(mid)
                def _(cp=cp):
                    cp.wait_recv()
                    cp.start()

                drains.append((mid, cp))

        def finish(self):
            @pl.when(mid)
            def _():
                self.arrive(far)

            @pl.when(jnp.logical_not(mid))
            def _():
                for k in range(3):
                    self.arrive(jnp.where(z == 0, 1 + k, k))

    loads = [
        pltpu.make_async_copy(src, dst, R.in_s.at[i])
        for i, (src, dst) in enumerate(
            (
                (R.zf_in, R.zf),
                (R.zb_in, R.zb),
                (R.val_in, R.val),
                (R.qry_in, R.qry),
                (R.og_in, R.og),
                (R.res_in, R.res),
            )
        )
    ]
    for cp in loads:
        cp.start()
    if rest:
        @pl.when(jnp.logical_not(has_extra))
        def _():
            R.wup[:, main:U] = jnp.zeros((D, LANES), BF16)
            R.wup[:, U + main :] = jnp.zeros((D, LANES), BF16)
            R.wdn[main:U, :] = jnp.zeros((LANES, D), BF16)

    edge = jnp.zeros((2 * f.most, 8, LANES), F32)
    R.er[:, 0:8, :] = edge
    R.er[:, 8 + 2 * Q :, :] = edge

    barrier = pltpu.get_barrier_semaphore()
    for k in range(1, Q):
        dev = {"sp": lax.rem(q + k, Q) * 2 + c, "tp": x}
        pl.semaphore_signal(barrier, inc=1, device_id=dev, device_id_type=MESH)
    pl.semaphore_signal(barrier, inc=1, device_id=to(c=1 - c), device_id_type=MESH)
    pl.semaphore_signal(barrier, inc=1, device_id=to(x=1 - x), device_id_type=MESH)
    pl.semaphore_wait(barrier, Q + 1)

    ccol = lane(c)
    O = f.piece
    own_out = pltpu.make_async_copy(
        R.out_w.at[pl.ds(pl.multiple_of(x * f.width, 16), f.width), :],
        R.outm.at[z, y, :, ccol],
        R.loc_s.at[0],
    )
    own_out.start()
    zg = []
    for i in range(OUT_PIECES):
        zg.append(
            ZGather(
                R.out_w.at[pl.ds(pl.multiple_of(x * f.width + i * O, 16), O), :],
                lambda k, i=i: R.outm.at[k, y, pl.ds(i * O, O), ccol],
                lambda j, i=i: R.oz_s.at[i, j],
                lambda j, i=i: R.oz_r.at[i, j],
            )
        )
        zg[-1].start()

    def out_y(i):
        src = R.outm.at[:, y, pl.ds(i * O, O), ccol]
        return remote(src, src, R.oy_s.at[i], R.oy_r.at[i], to(y=1 - y))

    def out_c(i):
        src = R.outm.at[:, :, pl.ds(i * O, O), ccol]
        return remote(src, src, R.oc_s.at[i], R.oc_r.at[i], to(c=1 - c))

    own_weights(0)
    send_weights([(0, 1)], 0)

    for cp in loads:
        cp.wait()
    L = f.length
    rows_i = lax.broadcasted_iota(jnp.int32, (L, L), 0)
    cols_i = lax.broadcasted_iota(jnp.int32, (L, L), 1)
    middle = L // 2
    extra = [jnp.transpose(R.extra[d]) for d in range(2)]
    for h in range(f.heads):
        at = slice(h * W, (h + 1) * W)
        values = R.val[:, at]
        logits = R.qry[:, at].astype(F32)
        queries = logits * jax.nn.sigmoid(logits)
        scores = jnp.zeros((L, L), F32)
        for d, z_ref in enumerate((R.zf, R.zb)):
            mask = rows_i >= cols_i if d == 0 else rows_i <= cols_i
            pre = z_ref[:, at].astype(F32)
            floor = R.floor[d : d + 1, at]
            span = 1.0 - floor
            logf = jnp.log(floor + span * jax.nn.sigmoid(pre)) + extra[d][:, h : h + 1]
            key = span * jax.nn.sigmoid(-pre)
            running = dot(jnp.where(mask, 1.0, 0.0), logf, ((1,), (0,)), lax.Precision.HIGHEST)
            last = L - 1 if d == 0 else 0
            total = running[last : last + 1]
            centred = running - running[middle : middle + 1]
            inner = dot(
                (queries * jnp.exp(centred)).astype(BF16),
                (key * jnp.exp(-centred)).astype(BF16),
                ((1,), (1,)),
            )
            scores += jnp.where(mask, inner, 0.0)
            R.carry[d, :, at] = (queries * jnp.exp(running)).astype(BF16)
            fresh = (key * jnp.exp(total - running)).astype(BF16)
            R.stb[h // 2, h % 2, d, :W] = dot(values, fresh, ((0,), (0,))).astype(BF16)
            R.stb[h // 2, h % 2, d, W:] = jnp.broadcast_to(jnp.exp(total), (PAD_ROWS, W)).astype(BF16)
        R.local[:, at] = dot(scores.astype(BF16), values, ((1,), (0,)))

    def state(ref, *at):
        return ref[at + (slice(0, W),)].astype(F32)

    def decay(ref, *at):
        return ref[at + (slice(W, W + 1),)].astype(F32)

    def put(ref, at, value, factor):
        ref[at + (slice(0, W),)] = value.astype(BF16)
        ref[at + (slice(W, W + PAD_ROWS),)] = jnp.broadcast_to(factor, (PAD_ROWS, W)).astype(BF16)

    def hop(i, src, dst, dev):
        return go(remote(src, dst, R.st_s.at[i], R.st_r.at[i], dev))

    out_ys, out_cs = {}, {}

    def out_second(i):
        zg[i].finish()
        out_ys[i] = go(out_y(i))

    def out_third(i):
        out_ys[i].wait_recv()
        out_cs[i] = go(out_c(i))

    step = hop(0, R.stb.at[1 - c], R.rc, to(c=1 - c))
    step.wait_recv()
    for hp in range(2):
        for d in range(2):
            ahead = c == d
            so, ao = state(R.stb, c, hp, d), decay(R.stb, c, hp, d)
            sp_, ap = state(R.rc, hp, d), decay(R.rc, hp, d)
            both = jnp.where(ahead, ap, ao) * jnp.where(ahead, so, sp_) + jnp.where(ahead, sp_, so)
            put(R.ct, (hp, d), both, ao * ap)
    step = hop(1, R.ct.at[1 - y], R.ry, to(y=1 - y))
    zg[0].forward()
    own_out.wait()
    step.wait_recv()
    for d in range(2):
        ahead = y == d
        so, ao = state(R.ct, y, d), decay(R.ct, y, d)
        sp_, ap = state(R.ry, d), decay(R.ry, d)
        both = jnp.where(ahead, ap, ao) * jnp.where(ahead, so, sp_) + jnp.where(ahead, sp_, so)
        put(R.pt, (d,), both, ao * ap)
    hops = []
    for k in range(1, 4):
        zt = lax.rem(z + k, 4)
        src = R.pt.at[jnp.where(zt > z, 0, 1)]
        remote(src, R.rz.at[z], R.sz_s.at[0], R.sz_r.at[0], to(z=zt)).start()
    three = R.rz.at[pl.ds(0, 3)]
    hops = [go(remote(three, three, R.sz_s.at[0], R.sz_r.at[0], to(y=1 - y)), False)]
    zg[1].forward()
    out_second(0)
    zg[2].forward()
    out_second(1)
    zg[3].forward()
    send_weights(STRAIGHT, 0)
    for h_ in hops:
        h_.wait_recv()

    def enter(d):
        def one(i, e):
            at = i if d == 0 else 3 - i
            return decay(R.rz, at) * e + state(R.rz, at)

        return lax.fori_loop(0, z if d == 0 else 3 - z, one, jnp.zeros((W, W), F32))

    for d in range(2):
        e = enter(d)
        so, ao = state(R.ct, y, d), decay(R.ct, y, d)
        sp_, ap = state(R.ry, d), decay(R.ry, d)
        R.ce[y, d] = jnp.where(y == d, e, ap * e + sp_).astype(BF16)
        R.yb[d] = jnp.where(y == d, ao * e + so, e).astype(BF16)
    step = hop(2, R.yb, R.ce.at[y], to(y=1 - y))
    out_second(2)
    out_second(3)
    step.wait_recv()
    for hp in range(2):
        for d in range(2):
            e = R.ce[hp, d].astype(F32)
            so, ao = state(R.stb, c, hp, d), decay(R.stb, c, hp, d)
            sp_, ap = state(R.rc, hp, d), decay(R.rc, hp, d)
            R.ent[c, hp, d] = jnp.where(c == d, e, ap * e + sp_).astype(BF16)
            R.cb[hp, d] = jnp.where(c == d, ao * e + so, e).astype(BF16)
    step = hop(3, R.cb, R.ent.at[c], to(c=1 - c))
    out_third(0)
    lend_weights([1, 3, 2], 0)
    step.wait_recv()

    for first, half in enumerate((1 - x, x)):
        at_rows = pl.ds(pl.multiple_of(half * H, H), H)
        for h in range(f.heads):
            at = slice(h * W, (h + 1) * W)
            total = R.local[at_rows, at]
            for d in range(2):
                total += dot(R.carry[d, at_rows, at], R.ent[h // 2, h % 2, d], ((1,), (1,)))
            mean = jnp.mean(total * total, axis=-1, keepdims=True)
            gate = R.og[at_rows, at].astype(F32)
            R.gb[first * H : (first + 1) * H, at] = (
                total * lax.rsqrt(mean + EPSILON) * R.hscale[...] * (gate * jax.nn.sigmoid(gate))
            ).astype(BF16)
    for i in range(1, OUT_PIECES):
        out_third(i)
    for i in range(OUT_PIECES):
        out_cs[i].wait_recv()

    width = g.c * LANES
    swaps = []
    for p in range(Q):
        at = slice(p * width, (p + 1) * width)
        total = dot(R.gb[...], R.outm[p // 2, p % 2], ((1,), (0,)))
        R.xb[:, at] = total[:H].astype(BF16)
        R.after[:, at] = R.res[:, at].astype(F32) + total[H:]
        if p % 2:
            i = p // 2
            two = pl.ds(2 * i * width, 2 * width)
            swaps.append(
                go(remote(R.xb.at[:, two], R.xr.at[:, two], R.xs_s.at[i], R.xs_r.at[i], to(x=1 - x)))
            )
    square = jnp.zeros((H, 1), F32)
    for i, swap in enumerate(swaps):
        at = slice(2 * i * width, 2 * (i + 1) * width)
        swap.wait_recv()
        if i == 1:
            relay_weights([1], 0)
        total = R.after[:, at] + R.xr[:, at].astype(F32)
        R.after[:, at] = total
        square += jnp.sum(total * total, axis=-1, keepdims=True)
    scale = lax.rsqrt(square / D + EPSILON)
    for p in range(Q):
        at = slice(p * width, (p + 1) * width)
        R.tok[z, y, x, :, at] = (R.after[:, at] * scale * R.pscale[:, at]).astype(BF16)

    n = len(f.gather)
    G = n // 2

    def cols(k):
        return slice(f.gather[k][0], sum(f.gather[k]))

    def cds(k):
        return pl.ds(*f.gather[k])

    ag = []
    for k in range(n):
        ag.append(
            ZGather(
                R.tok.at[z, y, x, :, cds(k)],
                lambda t, k=k: R.tok.at[t, y, x, :, cds(k)],
                lambda j, k=k: R.az_s.at[k, j],
                lambda j, k=k: R.az_r.at[k, j],
            )
        )

    def pair(t):
        return (t, t + G)

    spans = ((0, f.gather[G][0]), (f.gather[G][0], D - f.gather[G][0]))

    def second_own(color):
        src = R.tok.at[z, y, x, :, pl.ds(*spans[color])]
        dev = to(y=1 - y) if color else to(x=1 - x)
        return remote(src, src, R.ao_s.at[color], R.ao_r.at[color], dev)

    def second(k):
        dev = to(x=1 - x) if k < G else to(y=1 - y)
        half = z // 2
        for zs in (pl.ds(4 * half + 1 - z, 1), pl.ds(2 * (1 - half), 2)):
            src = R.tok.at[zs, y, x, :, cds(k)]
            remote(src, src, R.a2_s.at[k], R.a2_r.at[k], dev).start()
        all3 = R.tok.at[pl.ds(0, 3), y, x, :, cds(k)]
        return go(remote(all3, all3, R.a2_s.at[k], R.a2_r.at[k], dev), False)

    def third_own(color, piece):
        first, size = spans[color]
        at = pl.ds(first + piece * (size // 2), size // 2)
        if color:
            src, dev = R.tok.at[z, :, x, :, at], to(x=1 - x)
        else:
            src, dev = R.tok.at[z, y, :, :, at], to(y=1 - y)
        return remote(src, src, R.at_s.at[color, piece], R.at_r.at[color, piece], dev)

    def third(k):
        half = z // 2

        def shards(zs):
            if k < G:
                return R.tok.at[zs, y, :, :, cds(k)]
            return R.tok.at[zs, :, x, :, cds(k)]

        dev = to(y=1 - y) if k < G else to(x=1 - x)
        for zs in (pl.ds(4 * half + 1 - z, 1), pl.ds(2 * (1 - half), 2)):
            remote(shards(zs), shards(zs), R.a3_s.at[k], R.a3_r.at[k], dev).start()
        all3 = shards(pl.ds(0, 3))
        return go(remote(all3, all3, R.a3_s.at[k], R.a3_r.at[k], dev), False)

    def up(t, first):
        tall = g.y * g.x * H

        def body(i, _):
            at = pl.ds(pl.multiple_of(i * tall, tall), tall)
            value = 0.0
            for k in pair(t):
                rows = R.tok[i, :, :, :, cols(k)].reshape(tall, f.gather[k][1])
                value += dot(rows, R.wup[cols(k), :], ((1,), (0,)))
            R.acc[at, :] = value if first else R.acc[at, :] + value
            return 0

        lax.fori_loop(0, g.z, body, 0, unroll=True)

    for t in range(G):
        for k in pair(t):
            ag[k].start()
    own_weights(1)
    pass_weights(NEAR + STRAIGHT, 0)
    own_second = [go(second_own(color)) for color in range(2)]
    own_third = []
    flying = {}
    for t in range(G + 3):
        if t < G:
            for k in pair(t):
                ag[k].forward()
            if t == G - 1:
                relay_weights([3, 2], 0)
        if t in (1, 2):
            for color in (1, 0):
                if t == 1:
                    own_second[color].wait_recv()
                own_third.append(go(third_own(color, t - 1)))
        if 0 <= t - 1 < G:
            for k in pair(t - 1):
                ag[k].finish()
                flying[2, k] = second(k)
        if t == LEND:
            lend_weights([1, 3, 2], 1)
            send_weights([(0, 1)], 1)
        if 0 <= t - 3 < G:
            for k in pair(t - 3):
                flying[2, k].wait_recv()
                flying[3, k] = third(k)
        if t == G:
            send_weights(STRAIGHT, 1)
        if t == G + 1:
            relay_weights([1, 3, 2], 1)
    pass_weights(CROSS, 0)
    for p in range(Q):
        wait_weights(p, 0)
    for t in range(G):
        if t == G - 1:
            pass_weights(NEAR + STRAIGHT, 1)
        for cp in own_third if t == 0 else ():
            cp.wait_recv()
        for k in pair(t):
            flying[3, k].wait_recv()
        up(t, t == 0)

    for i in range(Q):
        for e, row in enumerate((i * L, (i + 1) * L - 1)):
            value = R.acc[row : row + 1, :].astype(BF16).astype(F32)
            for b in range(2 * f.most):
                R.ed[b, 2 * i + e : 2 * i + e + 1, :] = value[:, b * LANES : (b + 1) * LANES]
    edges = go(
        remote(R.ed, R.er.at[:, pl.ds(8, 2 * Q), :], R.ed_s.at[0], R.ed_r.at[0], to(c=1 - c))
    )
    pass_weights(CROSS, 1)
    edges.wait_recv()
    top = lax.broadcasted_iota(jnp.int32, (L, LANES), 0)

    def conv(i, _):
        at = pl.ds(pl.multiple_of(i * L, L), L)
        for b in range(f.most):
            def branch(ref, off):
                col = slice(off + b * LANES, off + (b + 1) * LANES)
                tap = ref[:, pl.ds(pl.multiple_of((mine + b) * LANES, LANES), LANES)]
                value = R.acc[at, col].astype(BF16).astype(F32)
                before = R.er[off // LANES + b, pl.ds(7 + 2 * (i + c), 1), :]
                behind = R.er[off // LANES + b, pl.ds(8 + 2 * (i + c), 1), :]
                above = jnp.where(top == 0, before, pltpu.roll(value, 1, 0))
                below = jnp.where(top == L - 1, behind, pltpu.roll(value, L - 1, 0))
                return above * tap[0:1] + value * tap[1:2] + below * tap[2:3]

            gate = branch(R.gtaps, 0)
            value = branch(R.vtaps, U)
            R.hid[at, b * LANES : (b + 1) * LANES] = (
                gate * jax.nn.sigmoid(gate) * value
            ).astype(BF16)
        return 0

    lax.fori_loop(0, Q, conv, 0, unroll=2)
    for p in range(Q):
        wait_weights(p, 1)

    n = len(f.reduce)
    G = n // 2

    def cols(k):
        return slice(f.reduce[k][0], sum(f.reduce[k]))

    def cds(k):
        return pl.ds(*f.reduce[k])

    def pair(t):
        return (t, t + G)

    def down(k):
        tall = g.y * g.x * H

        def body(i, _):
            at = pl.ds(pl.multiple_of(i * tall, tall), tall)
            value = dot(R.hid[at, :], R.wdn[:, k], ((1,), (0,)))
            R.part[i, :, :, :, k] = value.astype(BF16).reshape(g.y, g.x, H, k.stop - k.start)
            return 0

        lax.fori_loop(0, g.z, body, 0, unroll=True)

    def first_sum(k):
        if k < G:
            src, dev = R.part.at[:, 1 - y, :, :, cds(k)], to(y=1 - y)
        else:
            src, dev = R.part.at[:, :, 1 - x, :, cds(k)], to(x=1 - x)
        return remote(src, R.r1.at[:, :, :, cds(k)], R.r1_s.at[k], R.r1_r.at[k], dev)

    def second_sum(k):
        if k < G:
            src, dev = R.part.at[:, y, 1 - x, :, cds(k)], to(x=1 - x)
        else:
            src, dev = R.part.at[:, 1 - y, x, :, cds(k)], to(y=1 - y)
        return remote(src, R.r2.at[:, :, cds(k)], R.r2_s.at[k], R.r2_r.at[k], dev)

    def add_first(k):
        def body(i, _):
            zi, j = i // 2, lax.rem(i, 2)
            at = (zi, y, j) if k < G else (zi, j, x)
            at = at + (slice(None), cols(k))
            R.part[at] = (R.part[at].astype(F32) + R.r1[zi, j, :, cols(k)].astype(F32)).astype(BF16)
            return 0

        lax.fori_loop(0, 2 * g.z, body, 0)

    def add_second(k):
        def body(i, _):
            at = (i, y, x, slice(None), cols(k))
            R.part[at] = (R.part[at].astype(F32) + R.r2[i, :, cols(k)].astype(F32)).astype(BF16)
            return 0

        lax.fori_loop(0, g.z, body, 0)

    def last_sums(k):
        for j in range(1, 4):
            zt = lax.rem(z + j, 4)
            src = R.part.at[zt, y, x, :, cds(k)]
            remote(src, R.r3.at[j - 1, :, cds(k)], R.r3_s.at[k], R.r3_r.at[k], to(z=zt)).start()
        all3 = R.r3.at[:, :, cds(k)]
        return go(remote(all3, all3, R.r3_s.at[k], R.r3_r.at[k], to(y=1 - y)), False)

    def stage1(t):
        for k in pair(t):
            flying[4, k] = go(first_sum(k))

    def stage2(t):
        for k in pair(t):
            flying[4, k].wait_recv()
            add_first(k)
            flying[5, k] = go(second_sum(k))

    def stage3(t):
        for k in pair(t):
            flying[5, k].wait_recv()
            add_second(k)
            flying[6, k] = last_sums(k)

    def stage4(t):
        for k in pair(t):
            total = R.after[:, cols(k)] + R.part[z, y, x, :, cols(k)].astype(F32)
            flying[6, k].wait_recv()
            for j in range(3):
                total += R.r3[j, :, cols(k)].astype(F32)
            R.out[:, cols(k)] = total.astype(BF16)

    V = f.side
    both = slice(D - 2 * V, D)
    one, two = slice(D - 2 * V, D - V), slice(D - V, D)

    def ds(at):
        return pl.ds(at.start, at.stop - at.start)

    side = {}

    def side1():
        for j in range(1, 4):
            zt = lax.rem(z + j, 4)
            src = R.part.at[zt, :, :, :, ds(both)]
            remote(src, R.c1.at[j - 1], R.c1_s.at[0], R.c1_r.at[0], to(z=zt)).start()
        side[1] = go(remote(R.c1, R.c1, R.c1_s.at[0], R.c1_r.at[0], to(y=1 - y)), False)

    def side2():
        side[1].wait_recv()
        for i in range(2 * g.y):
            at = (z, i // 2, i % 2, slice(None), both)
            total = R.part[at].astype(F32)
            for j in range(3):
                total += R.c1[j, i // 2, i % 2].astype(F32)
            R.part[at] = total.astype(BF16)
        src = R.part.at[z, :, 1 - x, :, ds(one)]
        side[2, 0] = go(remote(src, R.c2.at[0], R.c2_s.at[0], R.c2_r.at[0], to(x=1 - x)))
        src = R.part.at[z, 1 - y, :, :, ds(two)]
        side[2, 1] = go(remote(src, R.c2.at[1], R.c2_s.at[1], R.c2_r.at[1], to(y=1 - y)))

    def side3():
        side[2, 0].wait_recv()
        for i in range(2):
            at = (z, i, x, slice(None), one)
            R.part[at] = (R.part[at].astype(F32) + R.c2[0, i].astype(F32)).astype(BF16)
        src = R.part.at[z, 1 - y, x, :, ds(one)]
        side[3, 0] = go(remote(src, R.c3.at[0], R.c3_s.at[0], R.c3_r.at[0], to(y=1 - y)))
        side[2, 1].wait_recv()
        for i in range(2):
            at = (z, y, i, slice(None), two)
            R.part[at] = (R.part[at].astype(F32) + R.c2[1, i].astype(F32)).astype(BF16)
        src = R.part.at[z, y, 1 - x, :, ds(two)]
        side[3, 1] = go(remote(src, R.c3.at[1], R.c3_s.at[1], R.c3_r.at[1], to(x=1 - x)))

    def side4():
        for i, at in enumerate((one, two)):
            side[3, i].wait_recv()
            total = R.after[:, at] + R.part[z, y, x, :, at].astype(F32) + R.c3[i].astype(F32)
            R.out[:, at] = total.astype(BF16)

    for t in range(G):
        for k in pair(t):
            down(cols(k))
            if t < 2:
                flying[4, k] = go(first_sum(k))
        if t == 0:
            down(both)
            side1()
    for t in range(G + 2):
        if t < G:
            stage2(t)
        if t + 2 < G:
            stage1(t + 2)
        if t == 1:
            side2()
        if 0 <= t - 1 < G:
            stage3(t - 1)
        if t == 3:
            side3()
        if 0 <= t - 2 < G:
            stage4(t - 2)
        if t == G:
            side4()
    for cond, cp in drains:
        if cond is None:
            cp.wait_send()
        else:
            pl.when(cond)(cp.wait_send)


def fused(grid, f, args):
    scratch = f.scratch()
    vmem = pl.BlockSpec(memory_space=pltpu.VMEM)
    anyw = pl.BlockSpec(memory_space=pl.ANY)
    return pl.pallas_call(
        functools.partial(fused_kernel, f, list(scratch)),
        out_shape=jax.ShapeDtypeStruct((f.rows, f.depth), BF16),
        in_specs=[anyw] * 5 + [vmem] * 3 + [anyw] + [vmem] * 3 + [anyw] * 4,
        out_specs=vmem,
        scratch_shapes=list(scratch.values()),
        compiler_params=pltpu.CompilerParams(
            collective_id=next(grid.ids), has_side_effects=True, vmem_limit_bytes=60000000
        ),
    )(*args)


def on_device(
    grid,
    residual,
    forget_forward,
    forget_backward,
    value_written,
    query_logits,
    output_gate_logits,
    forget_minimum,
    extra_log_rate,
    head_norm_scale,
    output_matrix,
    prenorm_scale,
    gate_up_matrix,
    value_up_matrix,
    gate_taps,
    value_taps,
    down_matrix,
):
    shape = (
        value_written.shape[1] // HEAD_WIDTH,
        value_written.shape[0],
        gate_up_matrix.shape[0] * grid.sp,
        gate_up_matrix.shape[1],
        value_written.shape[1],
    )
    if Fused.fits(grid, *shape, output_matrix.shape[1] * grid.sp):
        return fused(
            grid,
            Fused(grid, *shape),
            (
                forget_forward,
                forget_backward,
                value_written,
                query_logits,
                output_gate_logits,
                forget_minimum,
                extra_log_rate.transpose(0, 2, 1),
                head_norm_scale[None],
                residual,
                prenorm_scale[None],
                gate_taps,
                value_taps,
                output_matrix,
                gate_up_matrix,
                value_up_matrix,
                down_matrix,
            ),
        )
    sp, tp = grid.sp, grid.x
    length, width = value_written.shape
    heads = width // HEAD_WIDTH
    depth, units = gate_up_matrix.shape
    unit = units // sp
    me = lax.axis_index("sp")

    out_full = lax.all_gather(output_matrix, "sp", axis=1, tiled=True)

    def cut(w):
        return w.reshape(depth, sp, unit).transpose(1, 0, 2)

    up = jnp.concatenate([cut(gate_up_matrix), cut(value_up_matrix)], axis=2)
    down = down_matrix.reshape(sp, unit, down_matrix.shape[1])
    up, down = exchange(grid, [(up, "sp"), (down, "sp")], True)
    up = up.reshape(sp * depth, 2 * unit)
    down = down.transpose(1, 0, 2).reshape(unit, -1)

    local, carry, state, decay = pl.pallas_call(
        functools.partial(local_kernel, heads),
        out_shape=(
            jax.ShapeDtypeStruct((length, width), F32),
            jax.ShapeDtypeStruct((2, length, width), BF16),
            jax.ShapeDtypeStruct((2, heads, HEAD_WIDTH, HEAD_WIDTH), BF16),
            jax.ShapeDtypeStruct((2, heads, DECAY_ROWS, HEAD_WIDTH), BF16),
        ),
    )(forget_forward, forget_backward, value_written, query_logits, forget_minimum, extra_log_rate)

    rows = 2 * heads * HEAD_WIDTH // sp
    decays = jnp.repeat(
        decay.reshape(2 * heads, DECAY_ROWS, HEAD_WIDTH), sp // (2 * heads), axis=0
    )
    message = jnp.concatenate([state.reshape(sp, rows, HEAD_WIDTH), decays], axis=1)
    (got,) = exchange(grid, [(message, "sp")], True)
    prefix = pl.pallas_call(
        functools.partial(prefix_kernel, rows),
        out_shape=jax.ShapeDtypeStruct((sp, rows, HEAD_WIDTH), BF16),
    )(got)
    (entering,) = exchange(grid, [(prefix, "sp")], True)
    gated = pl.pallas_call(
        functools.partial(finish_kernel, heads),
        out_shape=jax.ShapeDtypeStruct((length, width), BF16),
    )(
        local,
        carry,
        entering.reshape(2, heads, HEAD_WIDTH, HEAD_WIDTH),
        output_gate_logits,
        head_norm_scale[None],
    )
    (swapped,) = exchange(grid, [(gated.reshape(tp, length // tp, width), "x")], True)
    token_rows = swapped.transpose(1, 0, 2).reshape(length // tp, tp * width)
    mixed = jnp.dot(token_rows, out_full, preferred_element_type=F32)
    own_after = residual.astype(F32) + mixed
    mean = jnp.mean(own_after * own_after, axis=-1, keepdims=True)
    normed = (own_after * lax.rsqrt(mean + EPSILON) * prenorm_scale).astype(BF16)
    everyone = gather(grid, normed)
    tokens = everyone.reshape(-1, normed.shape[1])
    upward = jnp.dot(tokens, up, preferred_element_type=F32).astype(BF16)
    padded = jnp.pad(upward, ((1, 1), (0, 0)))
    taps = jnp.concatenate(
        [
            lax.dynamic_slice_in_dim(gate_taps, me * unit, unit, 1),
            lax.dynamic_slice_in_dim(value_taps, me * unit, unit, 1),
        ],
        axis=1,
    )
    count = tokens.shape[0]
    conv = padded[:count] * taps[0] + padded[1 : count + 1] * taps[1] + padded[2:] * taps[2]
    hidden = (jax.nn.silu(conv[:, :unit]) * conv[:, unit:]).astype(BF16)
    parts = hidden.reshape(everyone.shape[:-1] + (unit,))
    half = down.shape[1] // 2

    def project(order, weights):
        moved = parts.transpose(*order, 4, 5)
        product = jnp.dot(moved.reshape(-1, unit), weights, preferred_element_type=F32)
        return product.astype(BF16).reshape(moved.shape[:-1] + (weights.shape[1],))

    down_sum = reduce_scatter(
        grid, project((2, 3, 1, 0), down[:, :half]), project((2, 1, 3, 0), down[:, half:])
    )
    return (own_after + down_sum).astype(BF16)


def solution(mesh):
    return jax.shard_map(
        functools.partial(on_device, Grid(mesh)),
        mesh=mesh,
        in_specs=(
            P(("sp", "tp"), None),
            P("sp", "tp"),
            P("sp", "tp"),
            P("sp", "tp"),
            P("sp", "tp"),
            P("sp", "tp"),
            P(None, "tp"),
            P(None, "sp", "tp"),
            P(),
            P(None, "sp"),
            P(),
            P("sp", "tp"),
            P("sp", "tp"),
            P(None, "tp"),
            P(None, "tp"),
            P("tp", "sp"),
        ),
        out_specs=P(("sp", "tp"), None),
        check_vma=False,
    )
```

```python
import functools
import math

import jax
import jax.numpy as jnp
from jax import lax
from jax.experimental import pallas as pl
from jax.experimental.pallas import tpu as pltpu
from jax.sharding import PartitionSpec as P

HEAD_WIDTH = 128
EPSILON = 1e-06
MESH = pl.DeviceIdType.MESH
F32 = jnp.float32
BF16 = jnp.bfloat16
DECAY_ROWS = 16
CHUNKS = 4


class Grid:
    def __init__(self, mesh):
        sp, tp = mesh.shape["sp"], mesh.shape["tp"]
        self.sp, self.x = sp, tp
        self.c = math.gcd(sp, 2)
        self.y = math.gcd(sp // self.c, 2)
        self.z = sp // (self.c * self.y)
        self.ids = iter(range(100))

    def size(self, dim):
        return getattr(self, dim)

    def place(self):
        s, t = lax.axis_index("sp"), lax.axis_index("tp")
        return {
            "sp": s,
            "x": t,
            "c": lax.rem(s, self.c),
            "y": lax.rem(s // self.c, self.y),
            "z": s // (self.c * self.y),
        }

    def peer(self, place, dim, index):
        if dim == "sp":
            return {"sp": index, "tp": place["x"]}
        at = dict(place)
        at[dim] = index
        return {"sp": (at["z"] * self.y + at["y"]) * self.c + at["c"], "tp": at["x"]}

    def greet(self, place, dims):
        barrier = pltpu.get_barrier_semaphore()
        count = 0
        for dim in dims:
            n = self.size(dim)
            for k in range(1, n):
                peer = self.peer(place, dim, lax.rem(place[dim] + k, n))
                pl.semaphore_signal(barrier, inc=1, device_id=peer, device_id_type=MESH)
                count += 1
        pl.semaphore_wait(barrier, count)


def exchange_kernel(grid, dims, keep, *refs):
    m = len(dims)
    ins, outs = refs[:m], refs[m : 2 * m]
    send_sem, recv_sem, own_sem = refs[2 * m :]
    place = grid.place()
    copies = []
    grid.greet(place, sorted(set(dims)))
    base = 0
    for i, dim in enumerate(dims):
        n, me = grid.size(dim), place[dim]
        for k in range(1, n):
            to = lax.rem(me + k, n)
            slot = me if keep else k - 1
            copy = pltpu.make_async_remote_copy(
                src_ref=ins[i].at[to],
                dst_ref=outs[i].at[slot],
                send_sem=send_sem.at[base + k - 1],
                recv_sem=recv_sem.at[base + k - 1],
                device_id=grid.peer(place, dim, to),
                device_id_type=MESH,
            )
            copy.start()
            copies.append(copy)
        base += n - 1
    if keep:
        for i, dim in enumerate(dims):
            me = place[dim]
            own = pltpu.make_async_copy(ins[i].at[me], outs[i].at[me], own_sem.at[i])
            own.start()
            copies.append(own)
    for copy in copies:
        copy.wait()


def exchange(grid, items, keep):
    dims = tuple(d for _, d in items)
    total = sum(grid.size(d) - 1 for d in dims)
    shapes = tuple(
        jax.ShapeDtypeStruct(a.shape if keep else (a.shape[0] - 1,) + a.shape[1:], a.dtype)
        for a, _ in items
    )
    return pl.pallas_call(
        functools.partial(exchange_kernel, grid, dims, keep),
        out_shape=shapes,
        in_specs=[pl.BlockSpec(memory_space=pl.ANY)] * len(items),
        out_specs=[pl.BlockSpec(memory_space=pl.ANY)] * len(items),
        scratch_shapes=[
            pltpu.SemaphoreType.DMA((total,)),
            pltpu.SemaphoreType.DMA((total,)),
            pltpu.SemaphoreType.DMA((len(items),)),
        ],
        compiler_params=pltpu.CompilerParams(
            collective_id=next(grid.ids), has_side_effects=True
        ),
    )(*[a for a, _ in items])


def gather_kernel(grid, x_ref, out_ref, send_sem, recv_sem, own_sem):
    place = grid.place()
    z, y, c, x = (place[d] for d in "zycx")
    part = x_ref.shape[1] // (2 * CHUNKS)
    grid.greet(place, ("z", "y", "c", "x"))
    own = pltpu.make_async_copy(x_ref, out_ref.at[z, y, c, x], own_sem)
    own.start()
    used = 0

    def push(dim, src, dst):
        nonlocal used
        n, copies = grid.size(dim), []
        for k in range(1, n):
            copy = pltpu.make_async_remote_copy(
                src_ref=src,
                dst_ref=dst,
                send_sem=send_sem.at[used],
                recv_sem=recv_sem.at[used],
                device_id=grid.peer(place, dim, lax.rem(place[dim] + k, n)),
                device_id_type=MESH,
            )
            copy.start()
            copies.append(copy)
            used += 1
        return copies

    def start(level, t):
        both = pl.ds(2 * t * part, 2 * part)
        first, second = pl.ds(2 * t * part, part), pl.ds((2 * t + 1) * part, part)
        if level == 0:
            return push("z", x_ref.at[:, both], out_ref.at[z, y, c, x, :, both])
        if level == 1:
            a = out_ref.at[:, y, c, x, :, first]
            b = out_ref.at[:, y, c, x, :, second]
            return push("y", a, a) + push("x", b, b)
        if level == 2:
            a = out_ref.at[:, :, c, x, :, first]
            b = out_ref.at[:, y, c, :, :, second]
            return push("x", a, a) + push("y", b, b)
        a = out_ref.at[:, :, c, :, :, both]
        return push("c", a, a)

    flying = {(0, t): start(0, t) for t in range(CHUNKS)}
    own.wait()
    for step in range(CHUNKS + 3):
        for level in range(4):
            t = step - level
            if 0 <= t < CHUNKS:
                for copy in flying[level, t]:
                    copy.wait()
                if level < 3:
                    flying[level + 1, t] = start(level + 1, t)


def gather(grid, array):
    total = CHUNKS * sum(grid.size(d) - 1 for d in "zyyxxc")
    return pl.pallas_call(
        functools.partial(gather_kernel, grid),
        out_shape=jax.ShapeDtypeStruct(
            (grid.z, grid.y, grid.c, grid.x) + array.shape, array.dtype
        ),
        in_specs=[pl.BlockSpec(memory_space=pltpu.VMEM)],
        out_specs=pl.BlockSpec(memory_space=pl.ANY),
        scratch_shapes=[
            pltpu.SemaphoreType.DMA((total,)),
            pltpu.SemaphoreType.DMA((total,)),
            pltpu.SemaphoreType.DMA,
        ],
        compiler_params=pltpu.CompilerParams(
            collective_id=next(grid.ids), has_side_effects=True
        ),
    )(array)


ORDERS = ("cxyz", "cyxz")


def reduce_kernel(grid, a_ref, b_ref, out_ref, *scratch):
    held, got, (send_sem, recv_sem, own_sem) = scratch[:2], scratch[2:10], scratch[10:]
    terms = (a_ref, b_ref)
    place = grid.place()
    rows, part = held[0].shape[-2:]
    grid.greet(place, ("z", "y", "c", "x"))
    used = 0

    def start(level, t):
        nonlocal used
        copies = []
        for color in range(2):
            dim = ORDERS[color][level]
            n, me = grid.size(dim), place[dim]
            for k in range(1, n):
                to = lax.rem(me + k, n)
                if level == 0:
                    src = terms[color].at[to, :, :, :, :, pl.ds(t * part, part)]
                else:
                    before = tuple(place[d] for d in ORDERS[color][1:level])
                    src = held[color].at[(t,) + before + (to,)]
                copy = pltpu.make_async_remote_copy(
                    src_ref=src,
                    dst_ref=got[2 * level + color].at[t, k - 1],
                    send_sem=send_sem.at[used],
                    recv_sem=recv_sem.at[used],
                    device_id=grid.peer(place, dim, to),
                    device_id_type=MESH,
                )
                copy.start()
                copies.append(copy)
                used += 1
        return copies

    def add(level, t):
        for color in range(2):
            order = ORDERS[color]
            here = tuple(place[d] for d in order[1 : level + 1])
            left = [grid.size(d) for d in order[level + 1 :]]
            peers = grid.size(order[level]) - 1
            where = got[2 * level + color]

            def block(i, _, color=color, here=here, left=left, peers=peers, where=where):
                index, rest = [], i
                for n in reversed(left):
                    index.insert(0, lax.rem(rest, n))
                    rest = rest // n
                index = tuple(index)
                total = held[color][(t,) + here + index].astype(F32)
                for k in range(peers):
                    total += where[(t, k) + index].astype(F32)
                if level < 3:
                    held[color][(t,) + here + index] = total.astype(BF16)
                else:
                    first = (color * CHUNKS + t) * part
                    out_ref[:, first : first + part] = total
                return 0

            if left:
                lax.fori_loop(0, math.prod(left), block, 0)
            else:
                block(0, 0)

    flying = {(0, t): start(0, t) for t in range(CHUNKS)}
    for t in range(CHUNKS):
        for color in range(2):
            own = pltpu.make_async_copy(
                terms[color].at[place["c"], :, :, :, :, pl.ds(t * part, part)],
                held[color].at[t],
                own_sem.at[t, color],
            )
            own.start()
            flying[0, t].append(own)
    for step in range(CHUNKS + 3):
        for level in range(4):
            t = step - level
            if 0 <= t < CHUNKS:
                for copy in flying[level, t]:
                    copy.wait()
                add(level, t)
                if level < 3:
                    flying[level + 1, t] = start(level + 1, t)


def reduce_scatter(grid, first, second):
    rows, cols = first.shape[-2:]
    tile = (rows, cols // CHUNKS)

    def sizes(order):
        return tuple(grid.size(d) for d in order)

    scratch = [pltpu.VMEM((CHUNKS,) + sizes(o[1:]) + tile, BF16) for o in ORDERS]
    for level in range(4):
        for o in ORDERS:
            peers = grid.size(o[level]) - 1
            scratch.append(
                pltpu.VMEM((CHUNKS, max(peers, 1)) + sizes(o[level + 1 :]) + tile, BF16)
            )
    total = 2 * CHUNKS * sum(grid.size(d) - 1 for d in "cxyz")
    return pl.pallas_call(
        functools.partial(reduce_kernel, grid),
        out_shape=jax.ShapeDtypeStruct((rows, 2 * cols), F32),
        in_specs=[pl.BlockSpec(memory_space=pl.ANY)] * 2,
        out_specs=pl.BlockSpec(memory_space=pltpu.VMEM),
        scratch_shapes=scratch
        + [
            pltpu.SemaphoreType.DMA((total,)),
            pltpu.SemaphoreType.DMA((total,)),
            pltpu.SemaphoreType.DMA((CHUNKS, 2)),
        ],
        compiler_params=pltpu.CompilerParams(
            collective_id=next(grid.ids), has_side_effects=True, vmem_limit_bytes=64000000
        ),
    )(first, second)


def dot(a, b, dims, precision=None):
    return lax.dot_general(
        a, b, (dims, ((), ())), precision=precision, preferred_element_type=F32
    )


def local_kernel(
    heads, zf_ref, zb_ref, v_ref, q_ref, floor_ref, extra_ref, out_ref, carry_ref, state_ref, decay_ref
):
    length = v_ref.shape[0]
    rows = lax.broadcasted_iota(jnp.int32, (length, length), 0)
    cols = lax.broadcasted_iota(jnp.int32, (length, length), 1)
    middle = length // 2
    for h in range(heads):
        at = slice(h * HEAD_WIDTH, (h + 1) * HEAD_WIDTH)
        values = v_ref[:, at]
        logits = q_ref[:, at].astype(F32)
        queries = logits * jax.nn.sigmoid(logits)
        scores = jnp.zeros((length, length), F32)
        for d, z_ref in enumerate((zf_ref, zb_ref)):
            mask = rows >= cols if d == 0 else rows <= cols
            z = z_ref[:, at].astype(F32)
            floor = floor_ref[d : d + 1, at]
            rest = 1.0 - floor
            logf = jnp.log(floor + rest * jax.nn.sigmoid(z)) + extra_ref[d, :, h : h + 1]
            key = rest * jax.nn.sigmoid(-z)
            running = dot(
                jnp.where(mask, 1.0, 0.0), logf, ((1,), (0,)), lax.Precision.HIGHEST
            )
            last = length - 1 if d == 0 else 0
            total = running[last : last + 1]
            centred = running - running[middle : middle + 1]
            part = dot(
                (queries * jnp.exp(centred)).astype(BF16),
                (key * jnp.exp(-centred)).astype(BF16),
                ((1,), (1,)),
            )
            scores += jnp.where(mask, part, 0.0)
            carry_ref[d, :, at] = (queries * jnp.exp(running)).astype(BF16)
            fresh = (key * jnp.exp(total - running)).astype(BF16)
            state_ref[d, h] = dot(values, fresh, ((0,), (0,))).astype(BF16)
            decay_ref[d, h] = jnp.broadcast_to(
                jnp.exp(total), (DECAY_ROWS, HEAD_WIDTH)
            ).astype(BF16)
        out_ref[:, at] = dot(scores.astype(BF16), values, ((1,), (0,)))


def prefix_kernel(rows, got_ref, out_ref):
    n = got_ref.shape[0]
    forward = lax.axis_index("sp") < n // 2

    def hop(k, carry):
        at = jnp.where(forward, k, n - 1 - k)
        out_ref[at] = carry.astype(BF16)
        block = got_ref[at].astype(F32)
        return block[rows : rows + 1] * carry + block[:rows]

    lax.fori_loop(0, n, hop, jnp.zeros((rows, HEAD_WIDTH), F32))


def finish_kernel(heads, out_ref, carry_ref, enter_ref, gate_ref, scale_ref, gated_ref):
    for h in range(heads):
        at = slice(h * HEAD_WIDTH, (h + 1) * HEAD_WIDTH)
        total = out_ref[:, at]
        for d in range(2):
            total += dot(carry_ref[d, :, at], enter_ref[d, h], ((1,), (1,)))
        mean = jnp.mean(total * total, axis=-1, keepdims=True)
        g = gate_ref[:, at].astype(F32)
        gated_ref[:, at] = (
            total * lax.rsqrt(mean + EPSILON) * scale_ref[...] * (g * jax.nn.sigmoid(g))
        ).astype(BF16)


LANES = 128
PAD_ROWS = 16
GATHER_WIDTHS = ((1, 1, 2, 1, 1), (1, 2, 3, 2, 2))
REDUCE_WIDTHS = ((1, 2, 2, 1, 1), (1, 2, 2, 1, 1))
SIDE = 1
LEND = 2
OUT_PIECES = 4


class Fused:
    def __init__(self, grid, heads, length, depth, units, width):
        self.grid = grid
        self.heads, self.length, self.depth = heads, length, depth
        self.quads = grid.z * grid.y
        self.blocks = units // LANES
        self.base = self.blocks // self.quads
        self.most = -(-self.blocks // self.quads)
        self.unit = self.most * LANES
        self.width = width
        self.rows = length // grid.x
        self.shards = self.quads * grid.x
        self.own = self.shards * self.rows
        self.gather = self.split(GATHER_WIDTHS)
        self.reduce = self.split(REDUCE_WIDTHS, 2 * SIDE)
        self.side = (depth - sum(self.reduce[-1])) // 2
        self.piece = width // OUT_PIECES

    def split(self, widths, spare=0):
        unit = self.depth // (sum(map(sum, widths)) + spare)
        out, first = [], 0
        for color in widths:
            for w in color:
                out.append((first, w * unit))
                first += w * unit
        return out

    @staticmethod
    def fits(grid, heads, length, depth, units, width, out_depth):
        return (
            (grid.z, grid.y, grid.c, grid.x) == (4, 2, 2, 2)
            and heads == grid.c * grid.y
            and units % LANES == 0
            and units // LANES >= grid.z * grid.y
            and length % (16 * grid.x) == 0
            and depth == out_depth == grid.sp * LANES
            and depth % (LANES * sum(map(sum, GATHER_WIDTHS))) == 0
            and depth % (LANES * (sum(map(sum, REDUCE_WIDTHS)) + 2 * SIDE)) == 0
            and width % (16 * OUT_PIECES) == 0
        )

    def scratch(self):
        g, h2, w = self.grid, HEAD_WIDTH + PAD_ROWS, HEAD_WIDTH
        dma = pltpu.SemaphoreType.DMA
        n, m = len(self.gather), len(self.reduce)
        tall = self.quads * g.x * self.rows
        return dict(
            wup=pltpu.VMEM((self.depth, 2 * self.unit), BF16),
            wdn=pltpu.VMEM((self.unit, self.depth), BF16),
            outm=pltpu.VMEM((g.z, g.y, self.width, g.c * LANES), BF16),
            local=pltpu.VMEM((self.length, self.width), F32),
            carry=pltpu.VMEM((2, self.length, self.width), BF16),
            stb=pltpu.VMEM((2, 2, 2, h2, w), BF16),
            rc=pltpu.VMEM((2, 2, h2, w), BF16),
            ct=pltpu.VMEM((2, 2, h2, w), BF16),
            ry=pltpu.VMEM((2, h2, w), BF16),
            pt=pltpu.VMEM((2, h2, w), BF16),
            rz=pltpu.VMEM((g.z, h2, w), BF16),
            ce=pltpu.VMEM((2, 2, w, w), BF16),
            yb=pltpu.VMEM((2, w, w), BF16),
            ent=pltpu.VMEM((2, 2, 2, w, w), BF16),
            cb=pltpu.VMEM((2, 2, w, w), BF16),
            gb=pltpu.VMEM((self.length, self.width), BF16),
            xb=pltpu.VMEM((self.rows, self.depth), BF16),
            xr=pltpu.VMEM((self.rows, self.depth), BF16),
            after=pltpu.VMEM((self.rows, self.depth), F32),
            tok=pltpu.VMEM((g.z, g.y, g.x, self.rows, self.depth), BF16),
            acc=pltpu.VMEM((tall, 2 * self.unit), F32),
            ed=pltpu.VMEM((2 * self.most, 2 * self.quads, LANES), F32),
            er=pltpu.VMEM((2 * self.most, 2 * self.quads + 16, LANES), F32),
            hid=pltpu.VMEM((tall, self.unit), BF16),
            part=pltpu.VMEM((g.z, g.y, g.x, self.rows, self.depth), BF16),
            r1=pltpu.VMEM((g.z, 2, self.rows, self.depth), BF16),
            r2=pltpu.VMEM((g.z, self.rows, self.depth), BF16),
            r3=pltpu.VMEM((g.z - 1, self.rows, self.depth), BF16),
            c1=pltpu.VMEM((g.z - 1, g.y, g.x, self.rows, 2 * self.side), BF16),
            c2=pltpu.VMEM((2, 2, self.rows, self.side), BF16),
            c3=pltpu.VMEM((2, self.rows, self.side), BF16),
            c1_s=dma((1,)), c1_r=dma((1,)),
            c2_s=dma((2,)), c2_r=dma((2,)),
            c3_s=dma((2,)), c3_r=dma((2,)),
            zf=pltpu.VMEM((self.length, self.width), BF16),
            zb=pltpu.VMEM((self.length, self.width), BF16),
            val=pltpu.VMEM((self.length, self.width), BF16),
            qry=pltpu.VMEM((self.length, self.width), BF16),
            og=pltpu.VMEM((self.length, self.width), BF16),
            res=pltpu.VMEM((self.rows, self.depth), BF16),
            in_s=dma((6,)),
            loc_s=dma((1,)),
            oz_s=dma((OUT_PIECES, 2)), oz_r=dma((OUT_PIECES, 2)),
            oy_s=dma((OUT_PIECES,)), oy_r=dma((OUT_PIECES,)),
            oc_s=dma((OUT_PIECES,)), oc_r=dma((OUT_PIECES,)),
            xs_s=dma((4,)), xs_r=dma((4,)),
            su=pltpu.VMEM((g.z - 1, LANES, 2 * self.unit), BF16),
            sd=pltpu.VMEM((g.z - 1, self.unit, LANES), BF16),
            sy_s=dma((g.z - 1, 2)), sy_r=dma((g.z - 1, 2)),
            w_s=dma((self.quads, 2)), w_r=dma((self.quads, 2)),
            f_s=dma((2,)), f_r=dma((2,)),
            st_s=dma((4,)), st_r=dma((4,)),
            sz_s=dma((1,)), sz_r=dma((1,)),
            az_s=dma((n, 2)), az_r=dma((n, 2)),
            ao_s=dma((2,)), ao_r=dma((2,)),
            at_s=dma((2, 2)), at_r=dma((2, 2)),
            a2_s=dma((n,)), a2_r=dma((n,)),
            a3_s=dma((n,)), a3_r=dma((n,)),
            ed_s=dma((1,)), ed_r=dma((1,)),
            r1_s=dma((m,)), r1_r=dma((m,)),
            r2_s=dma((m,)), r2_r=dma((m,)),
            r3_s=dma((m,)), r3_r=dma((m,)),
        )


NEAR = [(0, 0), (0, 1)]
STRAIGHT = [(1, 0), (3, 0), (2, 0)]
CROSS = [(1, 1), (3, 1), (2, 1)]
INPUTS = (
    "zf_in",
    "zb_in",
    "val_in",
    "qry_in",
    "og_in",
    "floor",
    "extra",
    "hscale",
    "res_in",
    "pscale",
    "gtaps",
    "vtaps",
    "out_w",
    "gate_w",
    "value_w",
    "down_w",
)


def fused_kernel(f, names, *refs):
    R = dict(zip(INPUTS + ("out",) + tuple(names), refs))
    R = type("Refs", (), R)
    g = f.grid
    s, x = lax.axis_index("sp"), lax.axis_index("tp")
    c, y, z = lax.rem(s, 2), lax.rem(s // 2, 2), s // 4
    q = s // 2
    W, U, Q = HEAD_WIDTH, f.unit, f.quads
    H, D = f.rows, f.depth
    drains = []

    def to(z=z, y=y, c=c, x=x):
        return {"sp": (z * 2 + y) * 2 + c, "tp": x}

    def remote(src, dst, ss, rs, dev):
        return pltpu.make_async_remote_copy(
            src_ref=src, dst_ref=dst, send_sem=ss, recv_sem=rs, device_id=dev, device_id_type=MESH
        )

    def go(cp, start=True):
        if start:
            cp.start()
        drains.append((None, cp))
        return cp

    def lane(i):
        return pl.ds(pl.multiple_of(i * LANES, LANES), LANES)

    def first_block(j):
        return (f.blocks * j) // Q

    def extra_block(j):
        return first_block(j + 1) - first_block(j) > f.base

    mine = first_block(q)
    has_extra = extra_block(q)
    main, rest = f.base * LANES, (f.most - f.base) * LANES

    def spots(src_s, stage):
        if stage is None:
            k = lane(src_s)
            return R.wup.at[k, :], R.wdn.at[:, k]
        return R.su.at[stage], R.sd.at[stage]

    def weight_copies(src_s, j, kind, stage=None):
        start = first_block(j)
        at = pl.ds(pl.multiple_of(start * LANES, LANES), main)
        at2 = pl.ds(pl.multiple_of((start + f.base) * LANES, LANES), LANES)
        dst = spots(src_s, stage)[kind]
        e = extra_block(j)
        if kind:
            out = [(None, R.down_w.at[at, :], dst.at[pl.ds(0, main), :])]
            if rest:
                out.append((e, R.down_w.at[at2, :], dst.at[pl.ds(main, LANES), :]))
            return out
        out = [
            (None, R.gate_w.at[:, at], dst.at[:, pl.ds(0, main)]),
            (None, R.value_w.at[:, at], dst.at[:, pl.ds(U, main)]),
        ]
        if rest:
            out.append((e, R.gate_w.at[:, at2], dst.at[:, pl.ds(main, LANES)]))
            out.append((e, R.value_w.at[:, at2], dst.at[:, pl.ds(U + main, LANES)]))
        return out

    def when(cond, act):
        if cond is None:
            act()
        else:
            pl.when(cond)(act)

    def totals(dst, kind, extra):
        less = dst.at[pl.ds(0, main), :] if kind else dst.at[:, pl.ds(0, 2 * main)]
        if not rest:
            return [(None, dst)]
        return [(extra, dst), (jnp.logical_not(extra), less)]

    def arrived(dst, kind, extra, sem):
        for cond, ref in totals(dst, kind, extra):
            when(cond, remote(ref, ref, R.w_s.at[0, kind], sem, to(y=1 - y)).wait_recv)

    def sent(dst, kind, extra, sem):
        for cond, ref in totals(dst, kind, extra):
            drains.append((cond, remote(ref, ref, sem, R.w_r.at[0, kind], to(y=1 - y))))

    def own_weights(kind):
        for cond, src, dst in weight_copies(s, q, kind):
            when(cond, pltpu.make_async_copy(src, dst, R.w_r.at[q, kind]).start)

    def kin(dz, dy, sign=1):
        return lax.rem(z + sign * dz + 4, 4) * 2 + (1 - y if dy else y)

    def send_weights(classes, kind):
        for dz, dy in classes:
            j = kin(dz, dy)
            sem = R.w_s.at[2 * dz + dy, kind]
            for cond, src, dst in weight_copies(s, j, kind):
                when(cond, remote(src, dst, sem, R.w_r.at[q, kind], {"sp": j * 2 + c, "tp": x}).start)
            sent(spots(s, None)[kind], kind, extra_block(j), sem)

    def lend_weights(distances, kind):
        for dz in distances:
            j = kin(dz, 1)
            sem = R.sy_s.at[dz - 1, kind]
            for cond, src, dst in weight_copies(s, j, kind, dz - 1):
                when(cond, remote(src, dst, sem, R.sy_r.at[dz - 1, kind], to(y=1 - y)).start)
            sent(spots(s, None)[kind], kind, extra_block(j), sem)

    def relay_weights(distances, kind):
        peer = z * 2 + 1 - y
        goal = spots(peer * 2 + c, None)[kind]
        for dz in distances:
            j = kin(dz, 0)
            extra = extra_block(j)
            held = spots(None, dz - 1)[kind]
            arrived(held, kind, extra, R.sy_r.at[dz - 1, kind])
            dev = {"sp": j * 2 + c, "tp": x}
            sem = R.w_s.at[2 * dz + 1, kind]
            if kind:
                parts = [pl.ds(0, main)]
                pick = lambda ref, part: ref.at[part, :]
            else:
                parts = [pl.ds(0, main), pl.ds(U, main)]
                pick = lambda ref, part: ref.at[:, part]
            few = [
                remote(pick(held, part), pick(goal, part), sem, R.w_r.at[peer, kind], dev)
                for part in parts
            ]
            full = remote(held, goal, sem, R.w_r.at[peer, kind], dev)
            if rest:
                pl.when(extra)(full.start)
                for cp in few:
                    pl.when(jnp.logical_not(extra))(cp.start)
            else:
                full.start()
            sent(held, kind, extra, sem)

    def pass_weights(classes, kind):
        for dz, dy in classes:
            p = kin(dz, dy, -1)
            ref = spots(p * 2 + c, None)[kind]
            arrived(ref, kind, has_extra, R.w_r.at[p, kind])
            remote(ref, ref, R.f_s.at[kind], R.f_r.at[kind], to(c=1 - c)).start()

    def wait_weights(kind):
        count = pl.ds(0, Q * LANES)
        ref = R.wdn.at[:, count] if kind else R.wup.at[count, :]
        go(remote(ref, ref, R.f_s.at[kind], R.f_r.at[kind], to(c=1 - c)), False).wait_recv()

    mid = (z == 1) | (z == 2)
    t0, t1 = jnp.where(z == 1, 0, 1), jnp.where(z == 2, 3, 2)
    far = jnp.where(z == 1, 0, 3)

    class ZGather:
        def __init__(self, src, dst, ss, rs):
            self.src, self.dst, self.ss, self.rs = src, dst, ss, rs
            self.pair = dst(pl.ds(2 * (1 - z // 2), 2))
            self.far = remote(self.pair, self.pair, ss(1), rs(1), to(z=far))

        def start(self):
            for t in (t0, t1):
                slot = jnp.where(t // 2 == z // 2, 0, 1)
                remote(self.src, self.dst(z), self.ss(0), self.rs(slot), to(z=t)).start()
            go(remote(self.pair, self.pair, self.ss(0), self.rs(1), to(z=t0)), False)

        def forward(self):
            @pl.when(mid)
            def _():
                self.far.wait_recv()
                self.far.start()

            drains.append((mid, self.far))

        def finish(self):
            one = self.dst(z)
            remote(one, one, self.ss(0), self.rs(0), to(z=t0)).wait_recv()
            pl.when(jnp.logical_not(mid))(self.far.wait_recv)

    loads = [
        pltpu.make_async_copy(src, dst, R.in_s.at[i])
        for i, (src, dst) in enumerate(
            (
                (R.zf_in, R.zf),
                (R.zb_in, R.zb),
                (R.val_in, R.val),
                (R.qry_in, R.qry),
                (R.og_in, R.og),
                (R.res_in, R.res),
            )
        )
    ]
    for cp in loads:
        cp.start()
    if rest:
        @pl.when(jnp.logical_not(has_extra))
        def _():
            R.wup[:, main:U] = jnp.zeros((D, LANES), BF16)
            R.wup[:, U + main :] = jnp.zeros((D, LANES), BF16)
            R.wdn[main:U, :] = jnp.zeros((LANES, D), BF16)

    edge = jnp.zeros((2 * f.most, 8, LANES), F32)
    R.er[:, 0:8, :] = edge
    R.er[:, 8 + 2 * Q :, :] = edge

    barrier = pltpu.get_barrier_semaphore()
    for k in range(1, Q):
        dev = {"sp": lax.rem(q + k, Q) * 2 + c, "tp": x}
        pl.semaphore_signal(barrier, inc=1, device_id=dev, device_id_type=MESH)
    pl.semaphore_signal(barrier, inc=1, device_id=to(c=1 - c), device_id_type=MESH)
    pl.semaphore_signal(barrier, inc=1, device_id=to(x=1 - x), device_id_type=MESH)
    pl.semaphore_wait(barrier, Q + 1)

    ccol = lane(c)
    O = f.piece
    own_out = pltpu.make_async_copy(
        R.out_w.at[pl.ds(pl.multiple_of(x * f.width, 16), f.width), :],
        R.outm.at[z, y, :, ccol],
        R.loc_s.at[0],
    )
    own_out.start()
    zg = []
    for i in range(OUT_PIECES):
        zg.append(
            ZGather(
                R.out_w.at[pl.ds(pl.multiple_of(x * f.width + i * O, 16), O), :],
                lambda k, i=i: R.outm.at[k, y, pl.ds(i * O, O), ccol],
                lambda j, i=i: R.oz_s.at[i, j],
                lambda j, i=i: R.oz_r.at[i, j],
            )
        )
        zg[-1].start()

    def out_y(i):
        src = R.outm.at[:, y, pl.ds(i * O, O), ccol]
        return remote(src, src, R.oy_s.at[i], R.oy_r.at[i], to(y=1 - y))

    def out_c(i):
        src = R.outm.at[:, :, pl.ds(i * O, O), ccol]
        return remote(src, src, R.oc_s.at[i], R.oc_r.at[i], to(c=1 - c))

    own_weights(0)
    send_weights([(0, 1)], 0)

    for cp in loads:
        cp.wait()
    L = f.length
    rows_i = lax.broadcasted_iota(jnp.int32, (L, L), 0)
    cols_i = lax.broadcasted_iota(jnp.int32, (L, L), 1)
    middle = L // 2
    extra = [jnp.transpose(R.extra[d]) for d in range(2)]
    for h in range(f.heads):
        at = slice(h * W, (h + 1) * W)
        values = R.val[:, at]
        logits = R.qry[:, at].astype(F32)
        queries = logits * jax.nn.sigmoid(logits)
        scores = jnp.zeros((L, L), F32)
        for d, z_ref in enumerate((R.zf, R.zb)):
            mask = rows_i >= cols_i if d == 0 else rows_i <= cols_i
            pre = z_ref[:, at].astype(F32)
            floor = R.floor[d : d + 1, at]
            span = 1.0 - floor
            logf = jnp.log(floor + span * jax.nn.sigmoid(pre)) + extra[d][:, h : h + 1]
            key = span * jax.nn.sigmoid(-pre)
            running = dot(jnp.where(mask, 1.0, 0.0), logf, ((1,), (0,)), lax.Precision.HIGHEST)
            last = L - 1 if d == 0 else 0
            total = running[last : last + 1]
            centred = running - running[middle : middle + 1]
            inner = dot(
                (queries * jnp.exp(centred)).astype(BF16),
                (key * jnp.exp(-centred)).astype(BF16),
                ((1,), (1,)),
            )
            scores += jnp.where(mask, inner, 0.0)
            R.carry[d, :, at] = (queries * jnp.exp(running)).astype(BF16)
            fresh = (key * jnp.exp(total - running)).astype(BF16)
            R.stb[h // 2, h % 2, d, :W] = dot(values, fresh, ((0,), (0,))).astype(BF16)
            R.stb[h // 2, h % 2, d, W:] = jnp.broadcast_to(jnp.exp(total), (PAD_ROWS, W)).astype(BF16)
        R.local[:, at] = dot(scores.astype(BF16), values, ((1,), (0,)))

    def state(ref, *at):
        return ref[at + (slice(0, W),)].astype(F32)

    def decay(ref, *at):
        return ref[at + (slice(W, W + 1),)].astype(F32)

    def put(ref, at, value, factor):
        ref[at + (slice(0, W),)] = value.astype(BF16)
        ref[at + (slice(W, W + PAD_ROWS),)] = jnp.broadcast_to(factor, (PAD_ROWS, W)).astype(BF16)

    def hop(i, src, dst, dev):
        return go(remote(src, dst, R.st_s.at[i], R.st_r.at[i], dev))

    out_ys, out_cs = {}, {}

    def out_second(i):
        zg[i].finish()
        out_ys[i] = go(out_y(i))

    def out_third(i):
        out_ys[i].wait_recv()
        out_cs[i] = go(out_c(i))

    step = hop(0, R.stb.at[1 - c], R.rc, to(c=1 - c))
    step.wait_recv()
    for hp in range(2):
        for d in range(2):
            ahead = c == d
            so, ao = state(R.stb, c, hp, d), decay(R.stb, c, hp, d)
            sp_, ap = state(R.rc, hp, d), decay(R.rc, hp, d)
            both = jnp.where(ahead, ap, ao) * jnp.where(ahead, so, sp_) + jnp.where(ahead, sp_, so)
            put(R.ct, (hp, d), both, ao * ap)
    step = hop(1, R.ct.at[1 - y], R.ry, to(y=1 - y))
    zg[0].forward()
    own_out.wait()
    step.wait_recv()
    for d in range(2):
        ahead = y == d
        so, ao = state(R.ct, y, d), decay(R.ct, y, d)
        sp_, ap = state(R.ry, d), decay(R.ry, d)
        both = jnp.where(ahead, ap, ao) * jnp.where(ahead, so, sp_) + jnp.where(ahead, sp_, so)
        put(R.pt, (d,), both, ao * ap)
    hops = []
    for k in range(1, 4):
        zt = lax.rem(z + k, 4)
        src = R.pt.at[jnp.where(zt > z, 0, 1)]
        remote(src, R.rz.at[z], R.sz_s.at[0], R.sz_r.at[0], to(z=zt)).start()
    three = R.rz.at[pl.ds(0, 3)]
    hops = [go(remote(three, three, R.sz_s.at[0], R.sz_r.at[0], to(y=1 - y)), False)]
    zg[1].forward()
    out_second(0)
    zg[2].forward()
    out_second(1)
    zg[3].forward()
    send_weights(STRAIGHT, 0)
    for h_ in hops:
        h_.wait_recv()

    def enter(d):
        def one(i, e):
            at = i if d == 0 else 3 - i
            return decay(R.rz, at) * e + state(R.rz, at)

        return lax.fori_loop(0, z if d == 0 else 3 - z, one, jnp.zeros((W, W), F32))

    for d in range(2):
        e = enter(d)
        so, ao = state(R.ct, y, d), decay(R.ct, y, d)
        sp_, ap = state(R.ry, d), decay(R.ry, d)
        R.ce[y, d] = jnp.where(y == d, e, ap * e + sp_).astype(BF16)
        R.yb[d] = jnp.where(y == d, ao * e + so, e).astype(BF16)
    step = hop(2, R.yb, R.ce.at[y], to(y=1 - y))
    out_second(2)
    out_second(3)
    step.wait_recv()
    for hp in range(2):
        for d in range(2):
            e = R.ce[hp, d].astype(F32)
            so, ao = state(R.stb, c, hp, d), decay(R.stb, c, hp, d)
            sp_, ap = state(R.rc, hp, d), decay(R.rc, hp, d)
            R.ent[c, hp, d] = jnp.where(c == d, e, ap * e + sp_).astype(BF16)
            R.cb[hp, d] = jnp.where(c == d, ao * e + so, e).astype(BF16)
    step = hop(3, R.cb, R.ent.at[c], to(c=1 - c))
    out_third(0)
    lend_weights([1, 3, 2], 0)
    step.wait_recv()

    for first, half in enumerate((1 - x, x)):
        at_rows = pl.ds(pl.multiple_of(half * H, H), H)
        for h in range(f.heads):
            at = slice(h * W, (h + 1) * W)
            total = R.local[at_rows, at]
            for d in range(2):
                total += dot(R.carry[d, at_rows, at], R.ent[h // 2, h % 2, d], ((1,), (1,)))
            mean = jnp.mean(total * total, axis=-1, keepdims=True)
            gate = R.og[at_rows, at].astype(F32)
            R.gb[first * H : (first + 1) * H, at] = (
                total * lax.rsqrt(mean + EPSILON) * R.hscale[...] * (gate * jax.nn.sigmoid(gate))
            ).astype(BF16)
    for i in range(1, OUT_PIECES):
        out_third(i)
    for i in range(OUT_PIECES):
        out_cs[i].wait_recv()

    width = g.c * LANES
    swaps = []
    for p in range(Q):
        at = slice(p * width, (p + 1) * width)
        total = dot(R.gb[...], R.outm[p // 2, p % 2], ((1,), (0,)))
        R.xb[:, at] = total[:H].astype(BF16)
        R.after[:, at] = R.res[:, at].astype(F32) + total[H:]
        if p % 2:
            i = p // 2
            two = pl.ds(2 * i * width, 2 * width)
            swaps.append(
                go(remote(R.xb.at[:, two], R.xr.at[:, two], R.xs_s.at[i], R.xs_r.at[i], to(x=1 - x)))
            )
    square = jnp.zeros((H, 1), F32)
    for i, swap in enumerate(swaps):
        at = slice(2 * i * width, 2 * (i + 1) * width)
        swap.wait_recv()
        if i == 1:
            relay_weights([1], 0)
        total = R.after[:, at] + R.xr[:, at].astype(F32)
        R.after[:, at] = total
        square += jnp.sum(total * total, axis=-1, keepdims=True)
    scale = lax.rsqrt(square / D + EPSILON)
    for p in range(Q):
        at = slice(p * width, (p + 1) * width)
        R.tok[z, y, x, :, at] = (R.after[:, at] * scale * R.pscale[:, at]).astype(BF16)

    n = len(f.gather)
    G = n // 2

    def cols(k):
        return slice(f.gather[k][0], sum(f.gather[k]))

    def cds(k):
        return pl.ds(*f.gather[k])

    ag = []
    for k in range(n):
        ag.append(
            ZGather(
                R.tok.at[z, y, x, :, cds(k)],
                lambda t, k=k: R.tok.at[t, y, x, :, cds(k)],
                lambda j, k=k: R.az_s.at[k, j],
                lambda j, k=k: R.az_r.at[k, j],
            )
        )

    def pair(t):
        return (t, t + G)

    spans = ((0, f.gather[G][0]), (f.gather[G][0], D - f.gather[G][0]))

    def second_own(color):
        src = R.tok.at[z, y, x, :, pl.ds(*spans[color])]
        dev = to(y=1 - y) if color else to(x=1 - x)
        return remote(src, src, R.ao_s.at[color], R.ao_r.at[color], dev)

    def second(k):
        dev = to(x=1 - x) if k < G else to(y=1 - y)
        half = z // 2
        for zs in (pl.ds(4 * half + 1 - z, 1), pl.ds(2 * (1 - half), 2)):
            src = R.tok.at[zs, y, x, :, cds(k)]
            remote(src, src, R.a2_s.at[k], R.a2_r.at[k], dev).start()
        all3 = R.tok.at[pl.ds(0, 3), y, x, :, cds(k)]
        return go(remote(all3, all3, R.a2_s.at[k], R.a2_r.at[k], dev), False)

    def third_own(color, piece):
        first, size = spans[color]
        less = size // (2 * LANES) * LANES
        at = pl.ds(first + piece * less, size - less if piece else less)
        if color:
            src, dev = R.tok.at[z, :, x, :, at], to(x=1 - x)
        else:
            src, dev = R.tok.at[z, y, :, :, at], to(y=1 - y)
        return remote(src, src, R.at_s.at[color, piece], R.at_r.at[color, piece], dev)

    def third(k):
        half = z // 2

        def shards(zs):
            if k < G:
                return R.tok.at[zs, y, :, :, cds(k)]
            return R.tok.at[zs, :, x, :, cds(k)]

        dev = to(y=1 - y) if k < G else to(x=1 - x)
        for zs in (pl.ds(4 * half + 1 - z, 1), pl.ds(2 * (1 - half), 2)):
            remote(shards(zs), shards(zs), R.a3_s.at[k], R.a3_r.at[k], dev).start()
        all3 = shards(pl.ds(0, 3))
        return go(remote(all3, all3, R.a3_s.at[k], R.a3_r.at[k], dev), False)

    def up(t, first):
        tall = g.y * g.x * H

        def body(i, _):
            at = pl.ds(pl.multiple_of(i * tall, tall), tall)
            value = 0.0
            for k in pair(t):
                rows = R.tok[i, :, :, :, cols(k)].reshape(tall, f.gather[k][1])
                value += dot(rows, R.wup[cols(k), :], ((1,), (0,)))
            R.acc[at, :] = value if first else R.acc[at, :] + value
            return 0

        lax.fori_loop(0, g.z, body, 0, unroll=True)

    for t in range(G):
        for k in pair(t):
            ag[k].start()
    own_weights(1)
    pass_weights(NEAR + STRAIGHT, 0)
    own_second = [go(second_own(color)) for color in range(2)]
    own_third = []
    flying = {}
    for t in range(G + 3):
        if t < G:
            for k in pair(t):
                ag[k].forward()
            if t == G - 2:
                relay_weights([3, 2], 0)
        if t in (1, 2):
            for color in (1, 0):
                if t == 1:
                    own_second[color].wait_recv()
                own_third.append(go(third_own(color, t - 1)))
        if 0 <= t - 1 < G:
            for k in pair(t - 1):
                ag[k].finish()
                flying[2, k] = second(k)
        if t == LEND:
            lend_weights([1, 3, 2], 1)
            send_weights([(0, 1)], 1)
        if 0 <= t - 3 < G:
            for k in pair(t - 3):
                flying[2, k].wait_recv()
                flying[3, k] = third(k)
        if t == G - 1:
            send_weights(STRAIGHT, 1)
        if t == G:
            relay_weights([1, 3, 2], 1)
    pass_weights(CROSS, 0)
    wait_weights(0)
    for t in range(G):
        if t == G - 1:
            pass_weights(NEAR + STRAIGHT, 1)
        for cp in own_third if t == 0 else ():
            cp.wait_recv()
        for k in pair(t):
            flying[3, k].wait_recv()
        up(t, t == 0)

    for i in range(Q):
        for e, row in enumerate((i * L, (i + 1) * L - 1)):
            value = R.acc[row : row + 1, :].astype(BF16).astype(F32)
            for b in range(2 * f.most):
                R.ed[b, 2 * i + e : 2 * i + e + 1, :] = value[:, b * LANES : (b + 1) * LANES]
    edges = go(
        remote(R.ed, R.er.at[:, pl.ds(8, 2 * Q), :], R.ed_s.at[0], R.ed_r.at[0], to(c=1 - c))
    )
    pass_weights(CROSS, 1)
    edges.wait_recv()
    top = lax.broadcasted_iota(jnp.int32, (L, LANES), 0)

    def conv(i, _):
        at = pl.ds(pl.multiple_of(i * L, L), L)
        for b in range(f.most):
            def branch(ref, off):
                col = slice(off + b * LANES, off + (b + 1) * LANES)
                tap = ref[:, pl.ds(pl.multiple_of((mine + b) * LANES, LANES), LANES)]
                value = R.acc[at, col].astype(BF16).astype(F32)
                before = R.er[off // LANES + b, pl.ds(7 + 2 * (i + c), 1), :]
                behind = R.er[off // LANES + b, pl.ds(8 + 2 * (i + c), 1), :]
                above = jnp.where(top == 0, before, pltpu.roll(value, 1, 0))
                below = jnp.where(top == L - 1, behind, pltpu.roll(value, L - 1, 0))
                return above * tap[0:1] + value * tap[1:2] + below * tap[2:3]

            gate = branch(R.gtaps, 0)
            value = branch(R.vtaps, U)
            R.hid[at, b * LANES : (b + 1) * LANES] = (
                gate * jax.nn.sigmoid(gate) * value
            ).astype(BF16)
        return 0

    lax.fori_loop(0, Q, conv, 0, unroll=True)
    wait_weights(1)

    n = len(f.reduce)
    G = n // 2

    def cols(k):
        return slice(f.reduce[k][0], sum(f.reduce[k]))

    def cds(k):
        return pl.ds(*f.reduce[k])

    def pair(t):
        return (t, t + G)

    def down(k):
        tall = g.y * g.x * H

        def body(i, _):
            at = pl.ds(pl.multiple_of(i * tall, tall), tall)
            value = dot(R.hid[at, :], R.wdn[:, k], ((1,), (0,)))
            R.part[i, :, :, :, k] = value.astype(BF16).reshape(g.y, g.x, H, k.stop - k.start)
            return 0

        lax.fori_loop(0, g.z, body, 0, unroll=True)

    def first_sum(k):
        if k < G:
            src, dev = R.part.at[:, 1 - y, :, :, cds(k)], to(y=1 - y)
        else:
            src, dev = R.part.at[:, :, 1 - x, :, cds(k)], to(x=1 - x)
        return remote(src, R.r1.at[:, :, :, cds(k)], R.r1_s.at[k], R.r1_r.at[k], dev)

    def second_sum(k):
        if k < G:
            src, dev = R.part.at[:, y, 1 - x, :, cds(k)], to(x=1 - x)
        else:
            src, dev = R.part.at[:, 1 - y, x, :, cds(k)], to(y=1 - y)
        return remote(src, R.r2.at[:, :, cds(k)], R.r2_s.at[k], R.r2_r.at[k], dev)

    def add_first(k):
        def body(i, _):
            zi, j = i // 2, lax.rem(i, 2)
            at = (zi, y, j) if k < G else (zi, j, x)
            at = at + (slice(None), cols(k))
            R.part[at] = (R.part[at].astype(F32) + R.r1[zi, j, :, cols(k)].astype(F32)).astype(BF16)
            return 0

        lax.fori_loop(0, 2 * g.z, body, 0)

    def add_second(k):
        def body(i, _):
            at = (i, y, x, slice(None), cols(k))
            R.part[at] = (R.part[at].astype(F32) + R.r2[i, :, cols(k)].astype(F32)).astype(BF16)
            return 0

        lax.fori_loop(0, g.z, body, 0)

    def last_sums(k):
        for j in range(1, 4):
            zt = lax.rem(z + j, 4)
            src = R.part.at[zt, y, x, :, cds(k)]
            remote(src, R.r3.at[j - 1, :, cds(k)], R.r3_s.at[k], R.r3_r.at[k], to(z=zt)).start()
        all3 = R.r3.at[:, :, cds(k)]
        return go(remote(all3, all3, R.r3_s.at[k], R.r3_r.at[k], to(y=1 - y)), False)

    def stage1(t):
        for k in pair(t):
            flying[4, k] = go(first_sum(k))

    def stage2(t):
        for k in pair(t):
            flying[4, k].wait_recv()
            add_first(k)
            flying[5, k] = go(second_sum(k))

    def stage3(t):
        for k in pair(t):
            flying[5, k].wait_recv()
            add_second(k)
            flying[6, k] = last_sums(k)

    def stage4(t):
        for k in pair(t):
            total = R.after[:, cols(k)] + R.part[z, y, x, :, cols(k)].astype(F32)
            flying[6, k].wait_recv()
            for j in range(3):
                total += R.r3[j, :, cols(k)].astype(F32)
            R.out[:, cols(k)] = total.astype(BF16)

    V = f.side
    both = slice(D - 2 * V, D)
    one, two = slice(D - 2 * V, D - V), slice(D - V, D)

    def ds(at):
        return pl.ds(at.start, at.stop - at.start)

    side = {}

    def side1():
        for j in range(1, 4):
            zt = lax.rem(z + j, 4)
            src = R.part.at[zt, :, :, :, ds(both)]
            remote(src, R.c1.at[j - 1], R.c1_s.at[0], R.c1_r.at[0], to(z=zt)).start()
        side[1] = go(remote(R.c1, R.c1, R.c1_s.at[0], R.c1_r.at[0], to(y=1 - y)), False)

    def side2():
        side[1].wait_recv()
        for i in range(2 * g.y):
            at = (z, i // 2, i % 2, slice(None), both)
            total = R.part[at].astype(F32)
            for j in range(3):
                total += R.c1[j, i // 2, i % 2].astype(F32)
            R.part[at] = total.astype(BF16)
        src = R.part.at[z, :, 1 - x, :, ds(one)]
        side[2, 0] = go(remote(src, R.c2.at[0], R.c2_s.at[0], R.c2_r.at[0], to(x=1 - x)))
        src = R.part.at[z, 1 - y, :, :, ds(two)]
        side[2, 1] = go(remote(src, R.c2.at[1], R.c2_s.at[1], R.c2_r.at[1], to(y=1 - y)))

    def side3():
        side[2, 0].wait_recv()
        for i in range(2):
            at = (z, i, x, slice(None), one)
            R.part[at] = (R.part[at].astype(F32) + R.c2[0, i].astype(F32)).astype(BF16)
        src = R.part.at[z, 1 - y, x, :, ds(one)]
        side[3, 0] = go(remote(src, R.c3.at[0], R.c3_s.at[0], R.c3_r.at[0], to(y=1 - y)))
        side[2, 1].wait_recv()
        for i in range(2):
            at = (z, y, i, slice(None), two)
            R.part[at] = (R.part[at].astype(F32) + R.c2[1, i].astype(F32)).astype(BF16)
        src = R.part.at[z, y, 1 - x, :, ds(two)]
        side[3, 1] = go(remote(src, R.c3.at[1], R.c3_s.at[1], R.c3_r.at[1], to(x=1 - x)))

    def side4():
        for i, at in enumerate((one, two)):
            side[3, i].wait_recv()
            total = R.after[:, at] + R.part[z, y, x, :, at].astype(F32) + R.c3[i].astype(F32)
            R.out[:, at] = total.astype(BF16)

    for t in range(G):
        for k in pair(t):
            down(cols(k))
            if t < 2:
                flying[4, k] = go(first_sum(k))
        if t == 0:
            down(both)
            side1()
    for t in range(G + 2):
        if t < G:
            stage2(t)
        if t + 2 < G:
            stage1(t + 2)
        if t == 1:
            side2()
        if 0 <= t - 1 < G:
            stage3(t - 1)
        if t == 3:
            side3()
        if 0 <= t - 2 < G:
            stage4(t - 2)
        if t == G:
            side4()
    for cond, cp in drains:
        if cond is None:
            cp.wait_send()
        else:
            pl.when(cond)(cp.wait_send)


def fused(grid, f, args):
    scratch = f.scratch()
    vmem = pl.BlockSpec(memory_space=pltpu.VMEM)
    anyw = pl.BlockSpec(memory_space=pl.ANY)
    return pl.pallas_call(
        functools.partial(fused_kernel, f, list(scratch)),
        out_shape=jax.ShapeDtypeStruct((f.rows, f.depth), BF16),
        in_specs=[anyw] * 5 + [vmem] * 3 + [anyw] + [vmem] * 3 + [anyw] * 4,
        out_specs=vmem,
        scratch_shapes=list(scratch.values()),
        compiler_params=pltpu.CompilerParams(
            collective_id=next(grid.ids), has_side_effects=True, vmem_limit_bytes=60000000
        ),
    )(*args)


def on_device(
    grid,
    residual,
    forget_forward,
    forget_backward,
    value_written,
    query_logits,
    output_gate_logits,
    forget_minimum,
    extra_log_rate,
    head_norm_scale,
    output_matrix,
    prenorm_scale,
    gate_up_matrix,
    value_up_matrix,
    gate_taps,
    value_taps,
    down_matrix,
):
    shape = (
        value_written.shape[1] // HEAD_WIDTH,
        value_written.shape[0],
        gate_up_matrix.shape[0] * grid.sp,
        gate_up_matrix.shape[1],
        value_written.shape[1],
    )
    if Fused.fits(grid, *shape, output_matrix.shape[1] * grid.sp):
        return fused(
            grid,
            Fused(grid, *shape),
            (
                forget_forward,
                forget_backward,
                value_written,
                query_logits,
                output_gate_logits,
                forget_minimum,
                extra_log_rate.transpose(0, 2, 1),
                head_norm_scale[None],
                residual,
                prenorm_scale[None],
                gate_taps,
                value_taps,
                output_matrix,
                gate_up_matrix,
                value_up_matrix,
                down_matrix,
            ),
        )
    sp, tp = grid.sp, grid.x
    length, width = value_written.shape
    heads = width // HEAD_WIDTH
    depth, units = gate_up_matrix.shape
    unit = units // sp
    me = lax.axis_index("sp")

    out_full = lax.all_gather(output_matrix, "sp", axis=1, tiled=True)

    def cut(w):
        return w.reshape(depth, sp, unit).transpose(1, 0, 2)

    up = jnp.concatenate([cut(gate_up_matrix), cut(value_up_matrix)], axis=2)
    down = down_matrix.reshape(sp, unit, down_matrix.shape[1])
    up, down = exchange(grid, [(up, "sp"), (down, "sp")], True)
    up = up.reshape(sp * depth, 2 * unit)
    down = down.transpose(1, 0, 2).reshape(unit, -1)

    local, carry, state, decay = pl.pallas_call(
        functools.partial(local_kernel, heads),
        out_shape=(
            jax.ShapeDtypeStruct((length, width), F32),
            jax.ShapeDtypeStruct((2, length, width), BF16),
            jax.ShapeDtypeStruct((2, heads, HEAD_WIDTH, HEAD_WIDTH), BF16),
            jax.ShapeDtypeStruct((2, heads, DECAY_ROWS, HEAD_WIDTH), BF16),
        ),
    )(forget_forward, forget_backward, value_written, query_logits, forget_minimum, extra_log_rate)

    rows = 2 * heads * HEAD_WIDTH // sp
    decays = jnp.repeat(
        decay.reshape(2 * heads, DECAY_ROWS, HEAD_WIDTH), sp // (2 * heads), axis=0
    )
    message = jnp.concatenate([state.reshape(sp, rows, HEAD_WIDTH), decays], axis=1)
    (got,) = exchange(grid, [(message, "sp")], True)
    prefix = pl.pallas_call(
        functools.partial(prefix_kernel, rows),
        out_shape=jax.ShapeDtypeStruct((sp, rows, HEAD_WIDTH), BF16),
    )(got)
    (entering,) = exchange(grid, [(prefix, "sp")], True)
    gated = pl.pallas_call(
        functools.partial(finish_kernel, heads),
        out_shape=jax.ShapeDtypeStruct((length, width), BF16),
    )(
        local,
        carry,
        entering.reshape(2, heads, HEAD_WIDTH, HEAD_WIDTH),
        output_gate_logits,
        head_norm_scale[None],
    )
    (swapped,) = exchange(grid, [(gated.reshape(tp, length // tp, width), "x")], True)
    token_rows = swapped.transpose(1, 0, 2).reshape(length // tp, tp * width)
    mixed = jnp.dot(token_rows, out_full, preferred_element_type=F32)
    own_after = residual.astype(F32) + mixed
    mean = jnp.mean(own_after * own_after, axis=-1, keepdims=True)
    normed = (own_after * lax.rsqrt(mean + EPSILON) * prenorm_scale).astype(BF16)
    everyone = gather(grid, normed)
    tokens = everyone.reshape(-1, normed.shape[1])
    upward = jnp.dot(tokens, up, preferred_element_type=F32).astype(BF16)
    padded = jnp.pad(upward, ((1, 1), (0, 0)))
    taps = jnp.concatenate(
        [
            lax.dynamic_slice_in_dim(gate_taps, me * unit, unit, 1),
            lax.dynamic_slice_in_dim(value_taps, me * unit, unit, 1),
        ],
        axis=1,
    )
    count = tokens.shape[0]
    conv = padded[:count] * taps[0] + padded[1 : count + 1] * taps[1] + padded[2:] * taps[2]
    hidden = (jax.nn.silu(conv[:, :unit]) * conv[:, unit:]).astype(BF16)
    parts = hidden.reshape(everyone.shape[:-1] + (unit,))
    half = down.shape[1] // 2

    def project(order, weights):
        moved = parts.transpose(*order, 4, 5)
        product = jnp.dot(moved.reshape(-1, unit), weights, preferred_element_type=F32)
        return product.astype(BF16).reshape(moved.shape[:-1] + (weights.shape[1],))

    down_sum = reduce_scatter(
        grid, project((2, 3, 1, 0), down[:, :half]), project((2, 1, 3, 0), down[:, half:])
    )
    return (own_after + down_sum).astype(BF16)


def solution(mesh):
    return jax.shard_map(
        functools.partial(on_device, Grid(mesh)),
        mesh=mesh,
        in_specs=(
            P(("sp", "tp"), None),
            P("sp", "tp"),
            P("sp", "tp"),
            P("sp", "tp"),
            P("sp", "tp"),
            P("sp", "tp"),
            P(None, "tp"),
            P(None, "sp", "tp"),
            P(),
            P(None, "sp"),
            P(),
            P("sp", "tp"),
            P("sp", "tp"),
            P(None, "tp"),
            P(None, "tp"),
            P("tp", "sp"),
        ),
        out_specs=P(("sp", "tp"), None),
        check_vma=False,
    )
```

```python
import functools
import math

import jax
import jax.numpy as jnp
from jax import lax
from jax.experimental import pallas as pl
from jax.experimental.pallas import tpu as pltpu
from jax.sharding import PartitionSpec as P

HEAD_WIDTH = 128
EPSILON = 1e-06
MESH = pl.DeviceIdType.MESH
F32 = jnp.float32
BF16 = jnp.bfloat16
DECAY_ROWS = 16
CHUNKS = 4


class Grid:
    def __init__(self, mesh):
        sp, tp = mesh.shape["sp"], mesh.shape["tp"]
        self.sp, self.x = sp, tp
        self.c = math.gcd(sp, 2)
        self.y = math.gcd(sp // self.c, 2)
        self.z = sp // (self.c * self.y)
        self.ids = iter(range(100))

    def size(self, dim):
        return getattr(self, dim)

    def place(self):
        s, t = lax.axis_index("sp"), lax.axis_index("tp")
        return {
            "sp": s,
            "x": t,
            "c": lax.rem(s, self.c),
            "y": lax.rem(s // self.c, self.y),
            "z": s // (self.c * self.y),
        }

    def peer(self, place, dim, index):
        if dim == "sp":
            return {"sp": index, "tp": place["x"]}
        at = dict(place)
        at[dim] = index
        return {"sp": (at["z"] * self.y + at["y"]) * self.c + at["c"], "tp": at["x"]}

    def greet(self, place, dims):
        barrier = pltpu.get_barrier_semaphore()
        count = 0
        for dim in dims:
            n = self.size(dim)
            for k in range(1, n):
                peer = self.peer(place, dim, lax.rem(place[dim] + k, n))
                pl.semaphore_signal(barrier, inc=1, device_id=peer, device_id_type=MESH)
                count += 1
        pl.semaphore_wait(barrier, count)


def exchange_kernel(grid, dims, keep, *refs):
    m = len(dims)
    ins, outs = refs[:m], refs[m : 2 * m]
    send_sem, recv_sem, own_sem = refs[2 * m :]
    place = grid.place()
    copies = []
    grid.greet(place, sorted(set(dims)))
    base = 0
    for i, dim in enumerate(dims):
        n, me = grid.size(dim), place[dim]
        for k in range(1, n):
            to = lax.rem(me + k, n)
            slot = me if keep else k - 1
            copy = pltpu.make_async_remote_copy(
                src_ref=ins[i].at[to],
                dst_ref=outs[i].at[slot],
                send_sem=send_sem.at[base + k - 1],
                recv_sem=recv_sem.at[base + k - 1],
                device_id=grid.peer(place, dim, to),
                device_id_type=MESH,
            )
            copy.start()
            copies.append(copy)
        base += n - 1
    if keep:
        for i, dim in enumerate(dims):
            me = place[dim]
            own = pltpu.make_async_copy(ins[i].at[me], outs[i].at[me], own_sem.at[i])
            own.start()
            copies.append(own)
    for copy in copies:
        copy.wait()


def exchange(grid, items, keep):
    dims = tuple(d for _, d in items)
    total = sum(grid.size(d) - 1 for d in dims)
    shapes = tuple(
        jax.ShapeDtypeStruct(a.shape if keep else (a.shape[0] - 1,) + a.shape[1:], a.dtype)
        for a, _ in items
    )
    return pl.pallas_call(
        functools.partial(exchange_kernel, grid, dims, keep),
        out_shape=shapes,
        in_specs=[pl.BlockSpec(memory_space=pl.ANY)] * len(items),
        out_specs=[pl.BlockSpec(memory_space=pl.ANY)] * len(items),
        scratch_shapes=[
            pltpu.SemaphoreType.DMA((total,)),
            pltpu.SemaphoreType.DMA((total,)),
            pltpu.SemaphoreType.DMA((len(items),)),
        ],
        compiler_params=pltpu.CompilerParams(
            collective_id=next(grid.ids), has_side_effects=True
        ),
    )(*[a for a, _ in items])


def gather_kernel(grid, x_ref, out_ref, send_sem, recv_sem, own_sem):
    place = grid.place()
    z, y, c, x = (place[d] for d in "zycx")
    part = x_ref.shape[1] // (2 * CHUNKS)
    grid.greet(place, ("z", "y", "c", "x"))
    own = pltpu.make_async_copy(x_ref, out_ref.at[z, y, c, x], own_sem)
    own.start()
    used = 0

    def push(dim, src, dst):
        nonlocal used
        n, copies = grid.size(dim), []
        for k in range(1, n):
            copy = pltpu.make_async_remote_copy(
                src_ref=src,
                dst_ref=dst,
                send_sem=send_sem.at[used],
                recv_sem=recv_sem.at[used],
                device_id=grid.peer(place, dim, lax.rem(place[dim] + k, n)),
                device_id_type=MESH,
            )
            copy.start()
            copies.append(copy)
            used += 1
        return copies

    def start(level, t):
        both = pl.ds(2 * t * part, 2 * part)
        first, second = pl.ds(2 * t * part, part), pl.ds((2 * t + 1) * part, part)
        if level == 0:
            return push("z", x_ref.at[:, both], out_ref.at[z, y, c, x, :, both])
        if level == 1:
            a = out_ref.at[:, y, c, x, :, first]
            b = out_ref.at[:, y, c, x, :, second]
            return push("y", a, a) + push("x", b, b)
        if level == 2:
            a = out_ref.at[:, :, c, x, :, first]
            b = out_ref.at[:, y, c, :, :, second]
            return push("x", a, a) + push("y", b, b)
        a = out_ref.at[:, :, c, :, :, both]
        return push("c", a, a)

    flying = {(0, t): start(0, t) for t in range(CHUNKS)}
    own.wait()
    for step in range(CHUNKS + 3):
        for level in range(4):
            t = step - level
            if 0 <= t < CHUNKS:
                for copy in flying[level, t]:
                    copy.wait()
                if level < 3:
                    flying[level + 1, t] = start(level + 1, t)


def gather(grid, array):
    total = CHUNKS * sum(grid.size(d) - 1 for d in "zyyxxc")
    return pl.pallas_call(
        functools.partial(gather_kernel, grid),
        out_shape=jax.ShapeDtypeStruct(
            (grid.z, grid.y, grid.c, grid.x) + array.shape, array.dtype
        ),
        in_specs=[pl.BlockSpec(memory_space=pltpu.VMEM)],
        out_specs=pl.BlockSpec(memory_space=pl.ANY),
        scratch_shapes=[
            pltpu.SemaphoreType.DMA((total,)),
            pltpu.SemaphoreType.DMA((total,)),
            pltpu.SemaphoreType.DMA,
        ],
        compiler_params=pltpu.CompilerParams(
            collective_id=next(grid.ids), has_side_effects=True
        ),
    )(array)


ORDERS = ("cxyz", "cyxz")


def reduce_kernel(grid, a_ref, b_ref, out_ref, *scratch):
    held, got, (send_sem, recv_sem, own_sem) = scratch[:2], scratch[2:10], scratch[10:]
    terms = (a_ref, b_ref)
    place = grid.place()
    rows, part = held[0].shape[-2:]
    grid.greet(place, ("z", "y", "c", "x"))
    used = 0

    def start(level, t):
        nonlocal used
        copies = []
        for color in range(2):
            dim = ORDERS[color][level]
            n, me = grid.size(dim), place[dim]
            for k in range(1, n):
                to = lax.rem(me + k, n)
                if level == 0:
                    src = terms[color].at[to, :, :, :, :, pl.ds(t * part, part)]
                else:
                    before = tuple(place[d] for d in ORDERS[color][1:level])
                    src = held[color].at[(t,) + before + (to,)]
                copy = pltpu.make_async_remote_copy(
                    src_ref=src,
                    dst_ref=got[2 * level + color].at[t, k - 1],
                    send_sem=send_sem.at[used],
                    recv_sem=recv_sem.at[used],
                    device_id=grid.peer(place, dim, to),
                    device_id_type=MESH,
                )
                copy.start()
                copies.append(copy)
                used += 1
        return copies

    def add(level, t):
        for color in range(2):
            order = ORDERS[color]
            here = tuple(place[d] for d in order[1 : level + 1])
            left = [grid.size(d) for d in order[level + 1 :]]
            peers = grid.size(order[level]) - 1
            where = got[2 * level + color]

            def block(i, _, color=color, here=here, left=left, peers=peers, where=where):
                index, rest = [], i
                for n in reversed(left):
                    index.insert(0, lax.rem(rest, n))
                    rest = rest // n
                index = tuple(index)
                total = held[color][(t,) + here + index].astype(F32)
                for k in range(peers):
                    total += where[(t, k) + index].astype(F32)
                if level < 3:
                    held[color][(t,) + here + index] = total.astype(BF16)
                else:
                    first = (color * CHUNKS + t) * part
                    out_ref[:, first : first + part] = total
                return 0

            if left:
                lax.fori_loop(0, math.prod(left), block, 0)
            else:
                block(0, 0)

    flying = {(0, t): start(0, t) for t in range(CHUNKS)}
    for t in range(CHUNKS):
        for color in range(2):
            own = pltpu.make_async_copy(
                terms[color].at[place["c"], :, :, :, :, pl.ds(t * part, part)],
                held[color].at[t],
                own_sem.at[t, color],
            )
            own.start()
            flying[0, t].append(own)
    for step in range(CHUNKS + 3):
        for level in range(4):
            t = step - level
            if 0 <= t < CHUNKS:
                for copy in flying[level, t]:
                    copy.wait()
                add(level, t)
                if level < 3:
                    flying[level + 1, t] = start(level + 1, t)


def reduce_scatter(grid, first, second):
    rows, cols = first.shape[-2:]
    tile = (rows, cols // CHUNKS)

    def sizes(order):
        return tuple(grid.size(d) for d in order)

    scratch = [pltpu.VMEM((CHUNKS,) + sizes(o[1:]) + tile, BF16) for o in ORDERS]
    for level in range(4):
        for o in ORDERS:
            peers = grid.size(o[level]) - 1
            scratch.append(
                pltpu.VMEM((CHUNKS, max(peers, 1)) + sizes(o[level + 1 :]) + tile, BF16)
            )
    total = 2 * CHUNKS * sum(grid.size(d) - 1 for d in "cxyz")
    return pl.pallas_call(
        functools.partial(reduce_kernel, grid),
        out_shape=jax.ShapeDtypeStruct((rows, 2 * cols), F32),
        in_specs=[pl.BlockSpec(memory_space=pl.ANY)] * 2,
        out_specs=pl.BlockSpec(memory_space=pltpu.VMEM),
        scratch_shapes=scratch
        + [
            pltpu.SemaphoreType.DMA((total,)),
            pltpu.SemaphoreType.DMA((total,)),
            pltpu.SemaphoreType.DMA((CHUNKS, 2)),
        ],
        compiler_params=pltpu.CompilerParams(
            collective_id=next(grid.ids), has_side_effects=True, vmem_limit_bytes=64000000
        ),
    )(first, second)


def dot(a, b, dims, precision=None):
    return lax.dot_general(
        a, b, (dims, ((), ())), precision=precision, preferred_element_type=F32
    )


def local_kernel(
    heads, zf_ref, zb_ref, v_ref, q_ref, floor_ref, extra_ref, out_ref, carry_ref, state_ref, decay_ref
):
    length = v_ref.shape[0]
    rows = lax.broadcasted_iota(jnp.int32, (length, length), 0)
    cols = lax.broadcasted_iota(jnp.int32, (length, length), 1)
    middle = length // 2
    for h in range(heads):
        at = slice(h * HEAD_WIDTH, (h + 1) * HEAD_WIDTH)
        values = v_ref[:, at]
        logits = q_ref[:, at].astype(F32)
        queries = logits * jax.nn.sigmoid(logits)
        scores = jnp.zeros((length, length), F32)
        for d, z_ref in enumerate((zf_ref, zb_ref)):
            mask = rows >= cols if d == 0 else rows <= cols
            z = z_ref[:, at].astype(F32)
            floor = floor_ref[d : d + 1, at]
            rest = 1.0 - floor
            logf = jnp.log(floor + rest * jax.nn.sigmoid(z)) + extra_ref[d, :, h : h + 1]
            key = rest * jax.nn.sigmoid(-z)
            running = dot(
                jnp.where(mask, 1.0, 0.0), logf, ((1,), (0,)), lax.Precision.HIGHEST
            )
            last = length - 1 if d == 0 else 0
            total = running[last : last + 1]
            centred = running - running[middle : middle + 1]
            part = dot(
                (queries * jnp.exp(centred)).astype(BF16),
                (key * jnp.exp(-centred)).astype(BF16),
                ((1,), (1,)),
            )
            scores += jnp.where(mask, part, 0.0)
            carry_ref[d, :, at] = (queries * jnp.exp(running)).astype(BF16)
            fresh = (key * jnp.exp(total - running)).astype(BF16)
            state_ref[d, h] = dot(values, fresh, ((0,), (0,))).astype(BF16)
            decay_ref[d, h] = jnp.broadcast_to(
                jnp.exp(total), (DECAY_ROWS, HEAD_WIDTH)
            ).astype(BF16)
        out_ref[:, at] = dot(scores.astype(BF16), values, ((1,), (0,)))


def prefix_kernel(rows, got_ref, out_ref):
    n = got_ref.shape[0]
    forward = lax.axis_index("sp") < n // 2

    def hop(k, carry):
        at = jnp.where(forward, k, n - 1 - k)
        out_ref[at] = carry.astype(BF16)
        block = got_ref[at].astype(F32)
        return block[rows : rows + 1] * carry + block[:rows]

    lax.fori_loop(0, n, hop, jnp.zeros((rows, HEAD_WIDTH), F32))


def finish_kernel(heads, out_ref, carry_ref, enter_ref, gate_ref, scale_ref, gated_ref):
    for h in range(heads):
        at = slice(h * HEAD_WIDTH, (h + 1) * HEAD_WIDTH)
        total = out_ref[:, at]
        for d in range(2):
            total += dot(carry_ref[d, :, at], enter_ref[d, h], ((1,), (1,)))
        mean = jnp.mean(total * total, axis=-1, keepdims=True)
        g = gate_ref[:, at].astype(F32)
        gated_ref[:, at] = (
            total * lax.rsqrt(mean + EPSILON) * scale_ref[...] * (g * jax.nn.sigmoid(g))
        ).astype(BF16)


LANES = 128
PAD_ROWS = 16
GATHER_WIDTHS = ((1, 1, 2, 1, 1), (1, 2, 3, 2, 2))
REDUCE_WIDTHS = ((2, 2, 2, 1), (2, 2, 2, 1))
SIDE = 1
LEND = 2
OUT_PIECES = 4


class Fused:
    def __init__(self, grid, heads, length, depth, units, width):
        self.grid = grid
        self.heads, self.length, self.depth = heads, length, depth
        self.quads = grid.z * grid.y
        self.blocks = units // LANES
        self.base = self.blocks // self.quads
        self.most = -(-self.blocks // self.quads)
        self.unit = self.most * LANES
        self.width = width
        self.rows = length // grid.x
        self.shards = self.quads * grid.x
        self.own = self.shards * self.rows
        self.gather = self.split(GATHER_WIDTHS)
        self.reduce = self.split(REDUCE_WIDTHS, 2 * SIDE)
        self.side = (depth - sum(self.reduce[-1])) // 2
        self.piece = width // OUT_PIECES

    def split(self, widths, spare=0):
        unit = self.depth // (sum(map(sum, widths)) + spare)
        out, first = [], 0
        for color in widths:
            for w in color:
                out.append((first, w * unit))
                first += w * unit
        return out

    @staticmethod
    def fits(grid, heads, length, depth, units, width, out_depth):
        return (
            (grid.z, grid.y, grid.c, grid.x) == (4, 2, 2, 2)
            and heads == grid.c * grid.y
            and units % LANES == 0
            and units // LANES >= grid.z * grid.y
            and length % (16 * grid.x) == 0
            and depth == out_depth == grid.sp * LANES
            and depth % (LANES * sum(map(sum, GATHER_WIDTHS))) == 0
            and depth % (LANES * (sum(map(sum, REDUCE_WIDTHS)) + 2 * SIDE)) == 0
            and width % (16 * OUT_PIECES) == 0
        )

    def scratch(self):
        g, h2, w = self.grid, HEAD_WIDTH + PAD_ROWS, HEAD_WIDTH
        dma = pltpu.SemaphoreType.DMA
        n, m = len(self.gather), len(self.reduce)
        tall = self.quads * g.x * self.rows
        return dict(
            wup=pltpu.VMEM((self.depth, 2 * self.unit), BF16),
            wdn=pltpu.VMEM((self.unit, self.depth), BF16),
            outm=pltpu.VMEM((g.z, g.y, self.width, g.c * LANES), BF16),
            local=pltpu.VMEM((self.length, self.width), F32),
            carry=pltpu.VMEM((2, self.length, self.width), BF16),
            stb=pltpu.VMEM((2, 2, 2, h2, w), BF16),
            rc=pltpu.VMEM((2, 2, h2, w), BF16),
            ct=pltpu.VMEM((2, 2, h2, w), BF16),
            ry=pltpu.VMEM((2, h2, w), BF16),
            pt=pltpu.VMEM((2, h2, w), BF16),
            rz=pltpu.VMEM((g.z, h2, w), BF16),
            ce=pltpu.VMEM((2, 2, w, w), BF16),
            yb=pltpu.VMEM((2, w, w), BF16),
            ent=pltpu.VMEM((2, 2, 2, w, w), BF16),
            cb=pltpu.VMEM((2, 2, w, w), BF16),
            gb=pltpu.VMEM((self.length, self.width), BF16),
            xb=pltpu.VMEM((self.rows, self.depth), BF16),
            xr=pltpu.VMEM((self.rows, self.depth), BF16),
            after=pltpu.VMEM((self.rows, self.depth), F32),
            tok=pltpu.VMEM((g.z, g.y, g.x, self.rows, self.depth), BF16),
            acc=pltpu.VMEM((tall, 2 * self.unit), F32),
            ed=pltpu.VMEM((2 * self.most, 2 * self.quads, LANES), F32),
            er=pltpu.VMEM((2 * self.most, 2 * self.quads + 16, LANES), F32),
            hid=pltpu.VMEM((tall, self.unit), BF16),
            part=pltpu.VMEM((g.z, g.y, g.x, self.rows, self.depth), BF16),
            r1=pltpu.VMEM((g.z, 2, self.rows, self.depth), BF16),
            r2=pltpu.VMEM((g.z, self.rows, self.depth), BF16),
            r3=pltpu.VMEM((g.z - 1, self.rows, self.depth), BF16),
            c1=pltpu.VMEM((g.z - 1, g.y, g.x, self.rows, 2 * self.side), BF16),
            c2=pltpu.VMEM((2, 2, self.rows, self.side), BF16),
            c3=pltpu.VMEM((2, self.rows, self.side), BF16),
            o1_s=dma((2, 2)), o1_r=dma((2, 2)),
            o2_s=dma((2, 2)), o2_r=dma((2, 2)),
            c1_s=dma((1,)), c1_r=dma((1,)),
            c2_s=dma((2,)), c2_r=dma((2,)),
            c3_s=dma((2,)), c3_r=dma((2,)),
            zf=pltpu.VMEM((self.length, self.width), BF16),
            zb=pltpu.VMEM((self.length, self.width), BF16),
            val=pltpu.VMEM((self.length, self.width), BF16),
            qry=pltpu.VMEM((self.length, self.width), BF16),
            og=pltpu.VMEM((self.length, self.width), BF16),
            res=pltpu.VMEM((self.rows, self.depth), BF16),
            in_s=dma((6,)),
            loc_s=dma((1,)),
            oz_s=dma((OUT_PIECES, 2)), oz_r=dma((OUT_PIECES, 2)),
            oy_s=dma((OUT_PIECES,)), oy_r=dma((OUT_PIECES,)),
            oc_s=dma((OUT_PIECES,)), oc_r=dma((OUT_PIECES,)),
            xs_s=dma((4,)), xs_r=dma((4,)),
            su=pltpu.VMEM((g.z - 1, LANES, 2 * self.unit), BF16),
            sd=pltpu.VMEM((g.z - 1, self.unit, LANES), BF16),
            sy_s=dma((g.z - 1, 2)), sy_r=dma((g.z - 1, 2)),
            w_s=dma((self.quads, 2)), w_r=dma((self.quads, 2)),
            f_s=dma((2,)), f_r=dma((2,)),
            st_s=dma((4,)), st_r=dma((4,)),
            sz_s=dma((1,)), sz_r=dma((1,)),
            az_s=dma((n, 2)), az_r=dma((n, 2)),
            ao_s=dma((2,)), ao_r=dma((2,)),
            at_s=dma((2, 2)), at_r=dma((2, 2)),
            a2_s=dma((n,)), a2_r=dma((n,)),
            a3_s=dma((n,)), a3_r=dma((n,)),
            ed_s=dma((1,)), ed_r=dma((1,)),
            r1_s=dma((m,)), r1_r=dma((m,)),
            r2_s=dma((m,)), r2_r=dma((m,)),
            r3_s=dma((m,)), r3_r=dma((m,)),
        )


NEAR = [(0, 0), (0, 1)]
STRAIGHT = [(1, 0), (3, 0), (2, 0)]
CROSS = [(1, 1), (3, 1), (2, 1)]
INPUTS = (
    "zf_in",
    "zb_in",
    "val_in",
    "qry_in",
    "og_in",
    "floor",
    "extra",
    "hscale",
    "res_in",
    "pscale",
    "gtaps",
    "vtaps",
    "out_w",
    "gate_w",
    "value_w",
    "down_w",
)


def fused_kernel(f, names, *refs):
    R = dict(zip(INPUTS + ("out",) + tuple(names), refs))
    R = type("Refs", (), R)
    g = f.grid
    s, x = lax.axis_index("sp"), lax.axis_index("tp")
    c, y, z = lax.rem(s, 2), lax.rem(s // 2, 2), s // 4
    q = s // 2
    W, U, Q = HEAD_WIDTH, f.unit, f.quads
    H, D = f.rows, f.depth
    drains = []

    def to(z=z, y=y, c=c, x=x):
        return {"sp": (z * 2 + y) * 2 + c, "tp": x}

    def remote(src, dst, ss, rs, dev):
        return pltpu.make_async_remote_copy(
            src_ref=src, dst_ref=dst, send_sem=ss, recv_sem=rs, device_id=dev, device_id_type=MESH
        )

    def go(cp, start=True):
        if start:
            cp.start()
        drains.append((None, cp))
        return cp

    def lane(i):
        return pl.ds(pl.multiple_of(i * LANES, LANES), LANES)

    def first_block(j):
        return (f.blocks * j) // Q

    def extra_block(j):
        return first_block(j + 1) - first_block(j) > f.base

    mine = first_block(q)
    has_extra = extra_block(q)
    main, rest = f.base * LANES, (f.most - f.base) * LANES

    def spots(src_s, stage):
        if stage is None:
            k = lane(src_s)
            return R.wup.at[k, :], R.wdn.at[:, k]
        return R.su.at[stage], R.sd.at[stage]

    def weight_copies(src_s, j, kind, stage=None):
        start = first_block(j)
        at = pl.ds(pl.multiple_of(start * LANES, LANES), main)
        at2 = pl.ds(pl.multiple_of((start + f.base) * LANES, LANES), LANES)
        dst = spots(src_s, stage)[kind]
        e = extra_block(j)
        if kind:
            out = [(None, R.down_w.at[at, :], dst.at[pl.ds(0, main), :])]
            if rest:
                out.append((e, R.down_w.at[at2, :], dst.at[pl.ds(main, LANES), :]))
            return out
        out = [
            (None, R.gate_w.at[:, at], dst.at[:, pl.ds(0, main)]),
            (None, R.value_w.at[:, at], dst.at[:, pl.ds(U, main)]),
        ]
        if rest:
            out.append((e, R.gate_w.at[:, at2], dst.at[:, pl.ds(main, LANES)]))
            out.append((e, R.value_w.at[:, at2], dst.at[:, pl.ds(U + main, LANES)]))
        return out

    def when(cond, act):
        if cond is None:
            act()
        else:
            pl.when(cond)(act)

    def totals(dst, kind, extra):
        less = dst.at[pl.ds(0, main), :] if kind else dst.at[:, pl.ds(0, 2 * main)]
        if not rest:
            return [(None, dst)]
        return [(extra, dst), (jnp.logical_not(extra), less)]

    def arrived(dst, kind, extra, sem):
        for cond, ref in totals(dst, kind, extra):
            when(cond, remote(ref, ref, R.w_s.at[0, kind], sem, to(y=1 - y)).wait_recv)

    def sent(dst, kind, extra, sem):
        for cond, ref in totals(dst, kind, extra):
            drains.append((cond, remote(ref, ref, sem, R.w_r.at[0, kind], to(y=1 - y))))

    def own_weights(kind):
        for cond, src, dst in weight_copies(s, q, kind):
            when(cond, pltpu.make_async_copy(src, dst, R.w_r.at[q, kind]).start)

    def kin(dz, dy, sign=1):
        return lax.rem(z + sign * dz + 4, 4) * 2 + (1 - y if dy else y)

    def send_weights(classes, kind):
        for dz, dy in classes:
            j = kin(dz, dy)
            sem = R.w_s.at[2 * dz + dy, kind]
            for cond, src, dst in weight_copies(s, j, kind):
                when(cond, remote(src, dst, sem, R.w_r.at[q, kind], {"sp": j * 2 + c, "tp": x}).start)
            sent(spots(s, None)[kind], kind, extra_block(j), sem)

    def lend_weights(distances, kind):
        for dz in distances:
            j = kin(dz, 1)
            sem = R.sy_s.at[dz - 1, kind]
            for cond, src, dst in weight_copies(s, j, kind, dz - 1):
                when(cond, remote(src, dst, sem, R.sy_r.at[dz - 1, kind], to(y=1 - y)).start)
            sent(spots(s, None)[kind], kind, extra_block(j), sem)

    def relay_weights(distances, kind):
        peer = z * 2 + 1 - y
        goal = spots(peer * 2 + c, None)[kind]
        for dz in distances:
            j = kin(dz, 0)
            extra = extra_block(j)
            held = spots(None, dz - 1)[kind]
            arrived(held, kind, extra, R.sy_r.at[dz - 1, kind])
            dev = {"sp": j * 2 + c, "tp": x}
            sem = R.w_s.at[2 * dz + 1, kind]
            if kind:
                parts = [pl.ds(0, main)]
                pick = lambda ref, part: ref.at[part, :]
            else:
                parts = [pl.ds(0, main), pl.ds(U, main)]
                pick = lambda ref, part: ref.at[:, part]
            few = [
                remote(pick(held, part), pick(goal, part), sem, R.w_r.at[peer, kind], dev)
                for part in parts
            ]
            full = remote(held, goal, sem, R.w_r.at[peer, kind], dev)
            if rest:
                pl.when(extra)(full.start)
                for cp in few:
                    pl.when(jnp.logical_not(extra))(cp.start)
            else:
                full.start()
            sent(held, kind, extra, sem)

    def pass_weights(classes, kind):
        for dz, dy in classes:
            p = kin(dz, dy, -1)
            ref = spots(p * 2 + c, None)[kind]
            arrived(ref, kind, has_extra, R.w_r.at[p, kind])
            remote(ref, ref, R.f_s.at[kind], R.f_r.at[kind], to(c=1 - c)).start()

    def wait_weights(kind):
        count = pl.ds(0, Q * LANES)
        ref = R.wdn.at[:, count] if kind else R.wup.at[count, :]
        go(remote(ref, ref, R.f_s.at[kind], R.f_r.at[kind], to(c=1 - c)), False).wait_recv()

    mid = (z == 1) | (z == 2)
    t0, t1 = jnp.where(z == 1, 0, 1), jnp.where(z == 2, 3, 2)
    far = jnp.where(z == 1, 0, 3)

    class ZGather:
        def __init__(self, src, dst, ss, rs):
            self.src, self.dst, self.ss, self.rs = src, dst, ss, rs
            self.pair = dst(pl.ds(2 * (1 - z // 2), 2))
            self.far = remote(self.pair, self.pair, ss(1), rs(1), to(z=far))

        def start(self):
            for t in (t0, t1):
                slot = jnp.where(t // 2 == z // 2, 0, 1)
                remote(self.src, self.dst(z), self.ss(0), self.rs(slot), to(z=t)).start()
            go(remote(self.pair, self.pair, self.ss(0), self.rs(1), to(z=t0)), False)

        def forward(self):
            @pl.when(mid)
            def _():
                self.far.wait_recv()
                self.far.start()

            drains.append((mid, self.far))

        def finish(self):
            one = self.dst(z)
            remote(one, one, self.ss(0), self.rs(0), to(z=t0)).wait_recv()
            pl.when(jnp.logical_not(mid))(self.far.wait_recv)

    loads = [
        pltpu.make_async_copy(src, dst, R.in_s.at[i])
        for i, (src, dst) in enumerate(
            (
                (R.zf_in, R.zf),
                (R.zb_in, R.zb),
                (R.val_in, R.val),
                (R.qry_in, R.qry),
                (R.og_in, R.og),
                (R.res_in, R.res),
            )
        )
    ]
    for cp in loads:
        cp.start()
    if rest:
        @pl.when(jnp.logical_not(has_extra))
        def _():
            R.wup[:, main:U] = jnp.zeros((D, LANES), BF16)
            R.wup[:, U + main :] = jnp.zeros((D, LANES), BF16)
            R.wdn[main:U, :] = jnp.zeros((LANES, D), BF16)

    edge = jnp.zeros((2 * f.most, 8, LANES), F32)
    R.er[:, 0:8, :] = edge
    R.er[:, 8 + 2 * Q :, :] = edge

    barrier = pltpu.get_barrier_semaphore()
    for k in range(1, Q):
        dev = {"sp": lax.rem(q + k, Q) * 2 + c, "tp": x}
        pl.semaphore_signal(barrier, inc=1, device_id=dev, device_id_type=MESH)
    pl.semaphore_signal(barrier, inc=1, device_id=to(c=1 - c), device_id_type=MESH)
    pl.semaphore_signal(barrier, inc=1, device_id=to(x=1 - x), device_id_type=MESH)
    pl.semaphore_wait(barrier, Q + 1)

    ccol = lane(c)
    O = f.piece
    own_out = pltpu.make_async_copy(
        R.out_w.at[pl.ds(pl.multiple_of(x * f.width, 16), f.width), :],
        R.outm.at[z, y, :, ccol],
        R.loc_s.at[0],
    )
    own_out.start()
    zg = []
    for i in range(OUT_PIECES):
        zg.append(
            ZGather(
                R.out_w.at[pl.ds(pl.multiple_of(x * f.width + i * O, 16), O), :],
                lambda k, i=i: R.outm.at[k, y, pl.ds(i * O, O), ccol],
                lambda j, i=i: R.oz_s.at[i, j],
                lambda j, i=i: R.oz_r.at[i, j],
            )
        )
        zg[-1].start()

    def out_y(i):
        src = R.outm.at[:, y, pl.ds(i * O, O), ccol]
        return remote(src, src, R.oy_s.at[i], R.oy_r.at[i], to(y=1 - y))

    def out_c(i):
        src = R.outm.at[:, :, pl.ds(i * O, O), ccol]
        return remote(src, src, R.oc_s.at[i], R.oc_r.at[i], to(c=1 - c))

    own_weights(0)
    send_weights([(0, 1)], 0)

    for cp in loads:
        cp.wait()
    L = f.length
    rows_i = lax.broadcasted_iota(jnp.int32, (L, L), 0)
    cols_i = lax.broadcasted_iota(jnp.int32, (L, L), 1)
    middle = L // 2
    extra = [jnp.transpose(R.extra[d]) for d in range(2)]
    for h in range(f.heads):
        at = slice(h * W, (h + 1) * W)
        values = R.val[:, at]
        logits = R.qry[:, at].astype(F32)
        queries = logits * jax.nn.sigmoid(logits)
        scores = jnp.zeros((L, L), F32)
        for d, z_ref in enumerate((R.zf, R.zb)):
            mask = rows_i >= cols_i if d == 0 else rows_i <= cols_i
            pre = z_ref[:, at].astype(F32)
            floor = R.floor[d : d + 1, at]
            span = 1.0 - floor
            logf = jnp.log(floor + span * jax.nn.sigmoid(pre)) + extra[d][:, h : h + 1]
            key = span * jax.nn.sigmoid(-pre)
            running = dot(jnp.where(mask, 1.0, 0.0), logf, ((1,), (0,)), lax.Precision.HIGHEST)
            last = L - 1 if d == 0 else 0
            total = running[last : last + 1]
            centred = running - running[middle : middle + 1]
            inner = dot(
                (queries * jnp.exp(centred)).astype(BF16),
                (key * jnp.exp(-centred)).astype(BF16),
                ((1,), (1,)),
            )
            scores += jnp.where(mask, inner, 0.0)
            R.carry[d, :, at] = (queries * jnp.exp(running)).astype(BF16)
            fresh = (key * jnp.exp(total - running)).astype(BF16)
            R.stb[h // 2, h % 2, d, :W] = dot(values, fresh, ((0,), (0,))).astype(BF16)
            R.stb[h // 2, h % 2, d, W:] = jnp.broadcast_to(jnp.exp(total), (PAD_ROWS, W)).astype(BF16)
        R.local[:, at] = dot(scores.astype(BF16), values, ((1,), (0,)))

    def state(ref, *at):
        return ref[at + (slice(0, W),)].astype(F32)

    def decay(ref, *at):
        return ref[at + (slice(W, W + 1),)].astype(F32)

    def put(ref, at, value, factor):
        ref[at + (slice(0, W),)] = value.astype(BF16)
        ref[at + (slice(W, W + PAD_ROWS),)] = jnp.broadcast_to(factor, (PAD_ROWS, W)).astype(BF16)

    def hop(i, src, dst, dev):
        return go(remote(src, dst, R.st_s.at[i], R.st_r.at[i], dev))

    out_ys, out_cs = {}, {}

    def out_second(i):
        zg[i].finish()
        out_ys[i] = go(out_y(i))

    def out_third(i):
        out_ys[i].wait_recv()
        out_cs[i] = go(out_c(i))

    step = hop(0, R.stb.at[1 - c], R.rc, to(c=1 - c))
    step.wait_recv()
    for hp in range(2):
        for d in range(2):
            ahead = c == d
            so, ao = state(R.stb, c, hp, d), decay(R.stb, c, hp, d)
            sp_, ap = state(R.rc, hp, d), decay(R.rc, hp, d)
            both = jnp.where(ahead, ap, ao) * jnp.where(ahead, so, sp_) + jnp.where(ahead, sp_, so)
            put(R.ct, (hp, d), both, ao * ap)
    step = hop(1, R.ct.at[1 - y], R.ry, to(y=1 - y))
    zg[0].forward()
    own_out.wait()
    step.wait_recv()
    for d in range(2):
        ahead = y == d
        so, ao = state(R.ct, y, d), decay(R.ct, y, d)
        sp_, ap = state(R.ry, d), decay(R.ry, d)
        both = jnp.where(ahead, ap, ao) * jnp.where(ahead, so, sp_) + jnp.where(ahead, sp_, so)
        put(R.pt, (d,), both, ao * ap)
    hops = []
    for k in range(1, 4):
        zt = lax.rem(z + k, 4)
        src = R.pt.at[jnp.where(zt > z, 0, 1)]
        remote(src, R.rz.at[z], R.sz_s.at[0], R.sz_r.at[0], to(z=zt)).start()
    three = R.rz.at[pl.ds(0, 3)]
    hops = [go(remote(three, three, R.sz_s.at[0], R.sz_r.at[0], to(y=1 - y)), False)]
    zg[1].forward()
    out_second(0)
    zg[2].forward()
    out_second(1)
    zg[3].forward()
    send_weights(STRAIGHT, 0)
    for h_ in hops:
        h_.wait_recv()

    def enter(d):
        def one(i, e):
            at = i if d == 0 else 3 - i
            return decay(R.rz, at) * e + state(R.rz, at)

        return lax.fori_loop(0, z if d == 0 else 3 - z, one, jnp.zeros((W, W), F32))

    for d in range(2):
        e = enter(d)
        so, ao = state(R.ct, y, d), decay(R.ct, y, d)
        sp_, ap = state(R.ry, d), decay(R.ry, d)
        R.ce[y, d] = jnp.where(y == d, e, ap * e + sp_).astype(BF16)
        R.yb[d] = jnp.where(y == d, ao * e + so, e).astype(BF16)
    step = hop(2, R.yb, R.ce.at[y], to(y=1 - y))
    out_second(2)
    out_second(3)
    step.wait_recv()
    for hp in range(2):
        for d in range(2):
            e = R.ce[hp, d].astype(F32)
            so, ao = state(R.stb, c, hp, d), decay(R.stb, c, hp, d)
            sp_, ap = state(R.rc, hp, d), decay(R.rc, hp, d)
            R.ent[c, hp, d] = jnp.where(c == d, e, ap * e + sp_).astype(BF16)
            R.cb[hp, d] = jnp.where(c == d, ao * e + so, e).astype(BF16)
    step = hop(3, R.cb, R.ent.at[c], to(c=1 - c))
    out_third(0)
    lend_weights([1, 3, 2], 0)
    step.wait_recv()

    for first, half in enumerate((1 - x, x)):
        at_rows = pl.ds(pl.multiple_of(half * H, H), H)
        for h in range(f.heads):
            at = slice(h * W, (h + 1) * W)
            total = R.local[at_rows, at]
            for d in range(2):
                total += dot(R.carry[d, at_rows, at], R.ent[h // 2, h % 2, d], ((1,), (1,)))
            mean = jnp.mean(total * total, axis=-1, keepdims=True)
            gate = R.og[at_rows, at].astype(F32)
            R.gb[first * H : (first + 1) * H, at] = (
                total * lax.rsqrt(mean + EPSILON) * R.hscale[...] * (gate * jax.nn.sigmoid(gate))
            ).astype(BF16)
    for i in range(1, OUT_PIECES):
        out_third(i)
    for i in range(OUT_PIECES):
        out_cs[i].wait_recv()

    width = g.c * LANES
    swaps = []
    for p in range(Q):
        at = slice(p * width, (p + 1) * width)
        total = dot(R.gb[...], R.outm[p // 2, p % 2], ((1,), (0,)))
        R.xb[:, at] = total[:H].astype(BF16)
        R.after[:, at] = R.res[:, at].astype(F32) + total[H:]
        if p % 2:
            i = p // 2
            two = pl.ds(2 * i * width, 2 * width)
            swaps.append(
                go(remote(R.xb.at[:, two], R.xr.at[:, two], R.xs_s.at[i], R.xs_r.at[i], to(x=1 - x)))
            )
    square = jnp.zeros((H, 1), F32)
    for i, swap in enumerate(swaps):
        at = slice(2 * i * width, 2 * (i + 1) * width)
        swap.wait_recv()
        if i == 1:
            relay_weights([1], 0)
        total = R.after[:, at] + R.xr[:, at].astype(F32)
        R.after[:, at] = total
        square += jnp.sum(total * total, axis=-1, keepdims=True)
    scale = lax.rsqrt(square / D + EPSILON)
    for p in range(Q):
        at = slice(p * width, (p + 1) * width)
        R.tok[z, y, x, :, at] = (R.after[:, at] * scale * R.pscale[:, at]).astype(BF16)

    n = len(f.gather)
    G = n // 2

    def cols(k):
        return slice(f.gather[k][0], sum(f.gather[k]))

    def cds(k):
        return pl.ds(*f.gather[k])

    ag = []
    for k in range(n):
        ag.append(
            ZGather(
                R.tok.at[z, y, x, :, cds(k)],
                lambda t, k=k: R.tok.at[t, y, x, :, cds(k)],
                lambda j, k=k: R.az_s.at[k, j],
                lambda j, k=k: R.az_r.at[k, j],
            )
        )

    def pair(t):
        return (t, t + G)

    spans = ((0, f.gather[G][0]), (f.gather[G][0], D - f.gather[G][0]))

    def second_own(color):
        src = R.tok.at[z, y, x, :, pl.ds(*spans[color])]
        dev = to(y=1 - y) if color else to(x=1 - x)
        return remote(src, src, R.ao_s.at[color], R.ao_r.at[color], dev)

    def second(k):
        dev = to(x=1 - x) if k < G else to(y=1 - y)
        half = z // 2
        for zs in (pl.ds(4 * half + 1 - z, 1), pl.ds(2 * (1 - half), 2)):
            src = R.tok.at[zs, y, x, :, cds(k)]
            remote(src, src, R.a2_s.at[k], R.a2_r.at[k], dev).start()
        all3 = R.tok.at[pl.ds(0, 3), y, x, :, cds(k)]
        return go(remote(all3, all3, R.a2_s.at[k], R.a2_r.at[k], dev), False)

    def third_own(color, piece):
        first, size = spans[color]
        less = size // (2 * LANES) * LANES
        at = pl.ds(first + piece * less, size - less if piece else less)
        if color:
            src, dev = R.tok.at[z, :, x, :, at], to(x=1 - x)
        else:
            src, dev = R.tok.at[z, y, :, :, at], to(y=1 - y)
        return remote(src, src, R.at_s.at[color, piece], R.at_r.at[color, piece], dev)

    def third(k):
        half = z // 2

        def shards(zs):
            if k < G:
                return R.tok.at[zs, y, :, :, cds(k)]
            return R.tok.at[zs, :, x, :, cds(k)]

        dev = to(y=1 - y) if k < G else to(x=1 - x)
        for zs in (pl.ds(4 * half + 1 - z, 1), pl.ds(2 * (1 - half), 2)):
            remote(shards(zs), shards(zs), R.a3_s.at[k], R.a3_r.at[k], dev).start()
        all3 = shards(pl.ds(0, 3))
        return go(remote(all3, all3, R.a3_s.at[k], R.a3_r.at[k], dev), False)

    def up(t, first):
        tall = g.y * g.x * H

        def body(i, _):
            at = pl.ds(pl.multiple_of(i * tall, tall), tall)
            value = 0.0
            for k in pair(t):
                rows = R.tok[i, :, :, :, cols(k)].reshape(tall, f.gather[k][1])
                value += dot(rows, R.wup[cols(k), :], ((1,), (0,)))
            R.acc[at, :] = value if first else R.acc[at, :] + value
            return 0

        lax.fori_loop(0, g.z, body, 0, unroll=True)

    for t in range(G):
        for k in pair(t):
            ag[k].start()
    own_weights(1)
    pass_weights(NEAR + STRAIGHT, 0)
    own_second = [go(second_own(color)) for color in range(2)]
    own_third = []
    flying = {}
    for t in range(G + 3):
        if t < G:
            for k in pair(t):
                ag[k].forward()
            if t == G - 2:
                relay_weights([3, 2], 0)
        if t in (1, 2):
            for color in (1, 0):
                if t == 1:
                    own_second[color].wait_recv()
                own_third.append(go(third_own(color, t - 1)))
        if 0 <= t - 1 < G:
            for k in pair(t - 1):
                ag[k].finish()
                flying[2, k] = second(k)
        if t == LEND:
            lend_weights([1, 3, 2], 1)
            send_weights([(0, 1)], 1)
        if 0 <= t - 3 < G:
            for k in pair(t - 3):
                flying[2, k].wait_recv()
                flying[3, k] = third(k)
        if t == G - 1:
            send_weights(STRAIGHT, 1)
        if t == G:
            relay_weights([1, 3, 2], 1)
    pass_weights(CROSS, 0)
    wait_weights(0)
    for t in range(G):
        if t == G - 1:
            pass_weights(NEAR + STRAIGHT, 1)
        for cp in own_third if t == 0 else ():
            cp.wait_recv()
        for k in pair(t):
            flying[3, k].wait_recv()
        up(t, t == 0)

    for i in range(Q):
        for e, row in enumerate((i * L, (i + 1) * L - 1)):
            value = R.acc[row : row + 1, :].astype(BF16).astype(F32)
            for b in range(2 * f.most):
                R.ed[b, 2 * i + e : 2 * i + e + 1, :] = value[:, b * LANES : (b + 1) * LANES]
    edges = go(
        remote(R.ed, R.er.at[:, pl.ds(8, 2 * Q), :], R.ed_s.at[0], R.ed_r.at[0], to(c=1 - c))
    )
    pass_weights(CROSS, 1)
    edges.wait_recv()
    top = lax.broadcasted_iota(jnp.int32, (L, LANES), 0)

    def conv(i, _):
        at = pl.ds(pl.multiple_of(i * L, L), L)
        for b in range(f.most):
            def branch(ref, off):
                col = slice(off + b * LANES, off + (b + 1) * LANES)
                tap = ref[:, pl.ds(pl.multiple_of((mine + b) * LANES, LANES), LANES)]
                value = R.acc[at, col].astype(BF16).astype(F32)
                before = R.er[off // LANES + b, pl.ds(7 + 2 * (i + c), 1), :]
                behind = R.er[off // LANES + b, pl.ds(8 + 2 * (i + c), 1), :]
                above = jnp.where(top == 0, before, pltpu.roll(value, 1, 0))
                below = jnp.where(top == L - 1, behind, pltpu.roll(value, L - 1, 0))
                return above * tap[0:1] + value * tap[1:2] + below * tap[2:3]

            gate = branch(R.gtaps, 0)
            value = branch(R.vtaps, U)
            R.hid[at, b * LANES : (b + 1) * LANES] = (
                gate * jax.nn.sigmoid(gate) * value
            ).astype(BF16)
        return 0

    lax.fori_loop(0, Q, conv, 0, unroll=True)
    wait_weights(1)

    n = len(f.reduce)
    G = n // 2

    def cols(k):
        return slice(f.reduce[k][0], sum(f.reduce[k]))

    def cds(k):
        return pl.ds(*f.reduce[k])

    def pair(t):
        return (t, t + G)

    def down(k):
        tall = g.y * g.x * H

        def body(i, _):
            at = pl.ds(pl.multiple_of(i * tall, tall), tall)
            value = dot(R.hid[at, :], R.wdn[:, k], ((1,), (0,)))
            R.part[i, :, :, :, k] = value.astype(BF16).reshape(g.y, g.x, H, k.stop - k.start)
            return 0

        lax.fori_loop(0, g.z, body, 0, unroll=True)

    half = z // 2
    others = (pl.ds(4 * half + 1 - z, 1), pl.ds(2 * (1 - half), 2))

    def ds(at):
        return pl.ds(at.start, at.stop - at.start)

    def first_part(zs, color, at):
        if color == 0:
            return R.part.at[zs, 1 - y, :, :, at], to(y=1 - y)
        return R.part.at[zs, :, 1 - x, :, at], to(x=1 - x)

    def second_part(zs, color, at):
        if color == 0:
            return R.part.at[zs, y, 1 - x, :, at], to(x=1 - x)
        return R.part.at[zs, 1 - y, x, :, at], to(y=1 - y)

    def first_sum(k):
        for zs in others:
            src, dev = first_part(zs, k // G, cds(k))
            remote(src, R.r1.at[zs, :, :, cds(k)], R.r1_s.at[k], R.r1_r.at[k], dev).start()
        all3 = R.r1.at[pl.ds(0, 3), :, :, cds(k)]
        return go(remote(all3, all3, R.r1_s.at[k], R.r1_r.at[k], dev), False)

    def second_sum(k):
        for zs in others:
            src, dev = second_part(zs, k // G, cds(k))
            remote(src, R.r2.at[zs, :, cds(k)], R.r2_s.at[k], R.r2_r.at[k], dev).start()
        all3 = R.r2.at[pl.ds(0, 3), :, cds(k)]
        return go(remote(all3, all3, R.r2_s.at[k], R.r2_r.at[k], dev), False)

    def add_one(zi, j, color, at):
        where = ((zi, y, j) if color == 0 else (zi, j, x)) + (slice(None), at)
        R.part[where] = (R.part[where].astype(F32) + R.r1[zi, j, :, at].astype(F32)).astype(BF16)

    def add_first(k):
        def body(i, _):
            add_one(lax.rem(z + 1 + i // 2, 4), lax.rem(i, 2), k // G, cols(k))
            return 0

        lax.fori_loop(0, 2 * (g.z - 1), body, 0)

    def add_second(k):
        def body(i, _):
            zi = lax.rem(z + 1 + i, 4)
            at = (zi, y, x, slice(None), cols(k))
            R.part[at] = (R.part[at].astype(F32) + R.r2[zi, :, cols(k)].astype(F32)).astype(BF16)
            return 0

        lax.fori_loop(0, g.z - 1, body, 0)

    ends = (0, f.reduce[G][0], D - 2 * f.side)
    mine_sums = {}

    def own_span(color, piece):
        first, size = ends[color], ends[color + 1] - ends[color]
        less = -(-size // (2 * LANES)) * LANES
        return slice(first + less, first + size) if piece else slice(first, first + less)

    def own_first(piece):
        for color in range(2):
            at = ds(own_span(color, piece))
            src, dev = first_part(z, color, at)
            dst = R.r1.at[z, :, :, at]
            sems = R.o1_s.at[color, piece], R.o1_r.at[color, piece]
            mine_sums[1, color, piece] = go(remote(src, dst, *sems, dev))

    def own_next(piece):
        for color in range(2):
            span = own_span(color, piece)
            mine_sums[1, color, piece].wait_recv()
            for j in range(2):
                add_one(z, j, color, span)
            src, dev = second_part(z, color, ds(span))
            dst = R.r2.at[z, :, ds(span)]
            sems = R.o2_s.at[color, piece], R.o2_r.at[color, piece]
            mine_sums[2, color, piece] = go(remote(src, dst, *sems, dev))

    def own_last(piece):
        for color in range(2):
            at = own_span(color, piece)
            mine_sums[2, color, piece].wait_recv()
            total = R.after[:, at] + R.part[z, y, x, :, at].astype(F32) + R.r2[z, :, at].astype(F32)
            for j in range(3):
                total += R.r3[j, :, at].astype(F32)
            R.out[:, at] = total.astype(BF16)

    def last_sums(k):
        for j in range(1, 4):
            zt = lax.rem(z + j, 4)
            src = R.part.at[zt, y, x, :, cds(k)]
            remote(src, R.r3.at[j - 1, :, cds(k)], R.r3_s.at[k], R.r3_r.at[k], to(z=zt)).start()
        all3 = R.r3.at[:, :, cds(k)]
        return go(remote(all3, all3, R.r3_s.at[k], R.r3_r.at[k], to(y=1 - y)), False)

    def stage1(t):
        for k in pair(t):
            flying[4, k] = first_sum(k)

    def stage2(t):
        for k in pair(t):
            flying[4, k].wait_recv()
            add_first(k)
            flying[5, k] = second_sum(k)

    def stage3(t):
        for k in pair(t):
            flying[5, k].wait_recv()
            add_second(k)
            flying[6, k] = last_sums(k)

    V = f.side
    both = slice(D - 2 * V, D)
    one, two = slice(D - 2 * V, D - V), slice(D - V, D)

    side = {}

    def side1():
        for j in range(1, 4):
            zt = lax.rem(z + j, 4)
            src = R.part.at[zt, :, :, :, ds(both)]
            remote(src, R.c1.at[j - 1], R.c1_s.at[0], R.c1_r.at[0], to(z=zt)).start()
        side[1] = go(remote(R.c1, R.c1, R.c1_s.at[0], R.c1_r.at[0], to(y=1 - y)), False)

    def side2():
        side[1].wait_recv()
        for i in range(2 * g.y):
            at = (z, i // 2, i % 2, slice(None), both)
            total = R.part[at].astype(F32)
            for j in range(3):
                total += R.c1[j, i // 2, i % 2].astype(F32)
            R.part[at] = total.astype(BF16)
        src = R.part.at[z, :, 1 - x, :, ds(one)]
        side[2, 0] = go(remote(src, R.c2.at[0], R.c2_s.at[0], R.c2_r.at[0], to(x=1 - x)))
        src = R.part.at[z, 1 - y, :, :, ds(two)]
        side[2, 1] = go(remote(src, R.c2.at[1], R.c2_s.at[1], R.c2_r.at[1], to(y=1 - y)))

    def side3():
        side[2, 0].wait_recv()
        for i in range(2):
            at = (z, i, x, slice(None), one)
            R.part[at] = (R.part[at].astype(F32) + R.c2[0, i].astype(F32)).astype(BF16)
        src = R.part.at[z, 1 - y, x, :, ds(one)]
        side[3, 0] = go(remote(src, R.c3.at[0], R.c3_s.at[0], R.c3_r.at[0], to(y=1 - y)))
        side[2, 1].wait_recv()
        for i in range(2):
            at = (z, y, i, slice(None), two)
            R.part[at] = (R.part[at].astype(F32) + R.c2[1, i].astype(F32)).astype(BF16)
        src = R.part.at[z, y, 1 - x, :, ds(two)]
        side[3, 1] = go(remote(src, R.c3.at[1], R.c3_s.at[1], R.c3_r.at[1], to(x=1 - x)))

    def side4():
        for i, at in enumerate((one, two)):
            side[3, i].wait_recv()
            total = R.after[:, at] + R.part[z, y, x, :, at].astype(F32) + R.c3[i].astype(F32)
            R.out[:, at] = total.astype(BF16)

    for t in range(G):
        for k in pair(t):
            down(cols(k))
            if t < 2:
                flying[4, k] = first_sum(k)
        if t == 0:
            down(both)
            side1()
    for t in range(G + 1):
        if t < G:
            stage2(t)
        if t + 2 < G:
            stage1(t + 2)
        if t == G - 2:
            own_first(0)
        if t == G - 1:
            own_first(1)
        if t == 1:
            side2()
        if 0 <= t - 1 < G:
            stage3(t - 1)
        if t == 3:
            side3()
    own_next(0)
    own_next(1)
    side4()
    for t in range(G):
        for k in pair(t):
            flying[6, k].wait_recv()
    own_last(0)
    own_last(1)
    for cond, cp in drains:
        if cond is None:
            cp.wait_send()
        else:
            pl.when(cond)(cp.wait_send)


def fused(grid, f, args):
    scratch = f.scratch()
    vmem = pl.BlockSpec(memory_space=pltpu.VMEM)
    anyw = pl.BlockSpec(memory_space=pl.ANY)
    return pl.pallas_call(
        functools.partial(fused_kernel, f, list(scratch)),
        out_shape=jax.ShapeDtypeStruct((f.rows, f.depth), BF16),
        in_specs=[anyw] * 5 + [vmem] * 3 + [anyw] + [vmem] * 3 + [anyw] * 4,
        out_specs=vmem,
        scratch_shapes=list(scratch.values()),
        compiler_params=pltpu.CompilerParams(
            collective_id=next(grid.ids), has_side_effects=True, vmem_limit_bytes=60000000
        ),
    )(*args)


def on_device(
    grid,
    residual,
    forget_forward,
    forget_backward,
    value_written,
    query_logits,
    output_gate_logits,
    forget_minimum,
    extra_log_rate,
    head_norm_scale,
    output_matrix,
    prenorm_scale,
    gate_up_matrix,
    value_up_matrix,
    gate_taps,
    value_taps,
    down_matrix,
):
    shape = (
        value_written.shape[1] // HEAD_WIDTH,
        value_written.shape[0],
        gate_up_matrix.shape[0] * grid.sp,
        gate_up_matrix.shape[1],
        value_written.shape[1],
    )
    if Fused.fits(grid, *shape, output_matrix.shape[1] * grid.sp):
        return fused(
            grid,
            Fused(grid, *shape),
            (
                forget_forward,
                forget_backward,
                value_written,
                query_logits,
                output_gate_logits,
                forget_minimum,
                extra_log_rate.transpose(0, 2, 1),
                head_norm_scale[None],
                residual,
                prenorm_scale[None],
                gate_taps,
                value_taps,
                output_matrix,
                gate_up_matrix,
                value_up_matrix,
                down_matrix,
            ),
        )
    sp, tp = grid.sp, grid.x
    length, width = value_written.shape
    heads = width // HEAD_WIDTH
    depth, units = gate_up_matrix.shape
    unit = units // sp
    me = lax.axis_index("sp")

    out_full = lax.all_gather(output_matrix, "sp", axis=1, tiled=True)

    def cut(w):
        return w.reshape(depth, sp, unit).transpose(1, 0, 2)

    up = jnp.concatenate([cut(gate_up_matrix), cut(value_up_matrix)], axis=2)
    down = down_matrix.reshape(sp, unit, down_matrix.shape[1])
    up, down = exchange(grid, [(up, "sp"), (down, "sp")], True)
    up = up.reshape(sp * depth, 2 * unit)
    down = down.transpose(1, 0, 2).reshape(unit, -1)

    local, carry, state, decay = pl.pallas_call(
        functools.partial(local_kernel, heads),
        out_shape=(
            jax.ShapeDtypeStruct((length, width), F32),
            jax.ShapeDtypeStruct((2, length, width), BF16),
            jax.ShapeDtypeStruct((2, heads, HEAD_WIDTH, HEAD_WIDTH), BF16),
            jax.ShapeDtypeStruct((2, heads, DECAY_ROWS, HEAD_WIDTH), BF16),
        ),
    )(forget_forward, forget_backward, value_written, query_logits, forget_minimum, extra_log_rate)

    rows = 2 * heads * HEAD_WIDTH // sp
    decays = jnp.repeat(
        decay.reshape(2 * heads, DECAY_ROWS, HEAD_WIDTH), sp // (2 * heads), axis=0
    )
    message = jnp.concatenate([state.reshape(sp, rows, HEAD_WIDTH), decays], axis=1)
    (got,) = exchange(grid, [(message, "sp")], True)
    prefix = pl.pallas_call(
        functools.partial(prefix_kernel, rows),
        out_shape=jax.ShapeDtypeStruct((sp, rows, HEAD_WIDTH), BF16),
    )(got)
    (entering,) = exchange(grid, [(prefix, "sp")], True)
    gated = pl.pallas_call(
        functools.partial(finish_kernel, heads),
        out_shape=jax.ShapeDtypeStruct((length, width), BF16),
    )(
        local,
        carry,
        entering.reshape(2, heads, HEAD_WIDTH, HEAD_WIDTH),
        output_gate_logits,
        head_norm_scale[None],
    )
    (swapped,) = exchange(grid, [(gated.reshape(tp, length // tp, width), "x")], True)
    token_rows = swapped.transpose(1, 0, 2).reshape(length // tp, tp * width)
    mixed = jnp.dot(token_rows, out_full, preferred_element_type=F32)
    own_after = residual.astype(F32) + mixed
    mean = jnp.mean(own_after * own_after, axis=-1, keepdims=True)
    normed = (own_after * lax.rsqrt(mean + EPSILON) * prenorm_scale).astype(BF16)
    everyone = gather(grid, normed)
    tokens = everyone.reshape(-1, normed.shape[1])
    upward = jnp.dot(tokens, up, preferred_element_type=F32).astype(BF16)
    padded = jnp.pad(upward, ((1, 1), (0, 0)))
    taps = jnp.concatenate(
        [
            lax.dynamic_slice_in_dim(gate_taps, me * unit, unit, 1),
            lax.dynamic_slice_in_dim(value_taps, me * unit, unit, 1),
        ],
        axis=1,
    )
    count = tokens.shape[0]
    conv = padded[:count] * taps[0] + padded[1 : count + 1] * taps[1] + padded[2:] * taps[2]
    hidden = (jax.nn.silu(conv[:, :unit]) * conv[:, unit:]).astype(BF16)
    parts = hidden.reshape(everyone.shape[:-1] + (unit,))
    half = down.shape[1] // 2

    def project(order, weights):
        moved = parts.transpose(*order, 4, 5)
        product = jnp.dot(moved.reshape(-1, unit), weights, preferred_element_type=F32)
        return product.astype(BF16).reshape(moved.shape[:-1] + (weights.shape[1],))

    down_sum = reduce_scatter(
        grid, project((2, 3, 1, 0), down[:, :half]), project((2, 1, 3, 0), down[:, half:])
    )
    return (own_after + down_sum).astype(BF16)


def solution(mesh):
    return jax.shard_map(
        functools.partial(on_device, Grid(mesh)),
        mesh=mesh,
        in_specs=(
            P(("sp", "tp"), None),
            P("sp", "tp"),
            P("sp", "tp"),
            P("sp", "tp"),
            P("sp", "tp"),
            P("sp", "tp"),
            P(None, "tp"),
            P(None, "sp", "tp"),
            P(),
            P(None, "sp"),
            P(),
            P("sp", "tp"),
            P("sp", "tp"),
            P(None, "tp"),
            P(None, "tp"),
            P("tp", "sp"),
        ),
        out_specs=P(("sp", "tp"), None),
        check_vma=False,
    )
```
